256 devices in a mesh: sp: 32 (over z, y), tp: 8 (over x, core).
Axes of the slice: x: 4, y: 4, z: 8, core: 2. Of those that a mesh axis runs over, the one named last changes fastest.
Arguments:
- tokens: bfloat16 [4, 16384, 2048], P(None, ('sp', 'tp')), may hold values from -6 to 6
- in_gain: float32 [2048], replicated, may hold values from 0.1 to 1.9
- query_weight: bfloat16 [2048, 1024], P(None, 'tp'), may hold values from -0.125 to 0.125
- key_weight: bfloat16 [2048, 1024], P(None, 'tp'), may hold values from -0.125 to 0.125
- value_weight: bfloat16 [2048, 1024], P(None, 'tp'), may hold values from -0.125 to 0.125
- gate_weight: bfloat16 [2048, 1024], P(None, 'tp'), may hold values from -0.125 to 0.125
- log_decay: float32 [8], P('tp'), may hold values from -0.034 to 0, as said below
- norm_gain: float32 [1024], P('tp'), may hold values from 0.1 to 1.9
- out_weight: bfloat16 [1024, 2048], replicated, may hold values from -0.1875 to 0.1875
- post_gain: float32 [2048], replicated, may hold values from 0.1 to 1.9
Outputs:
- mixed: bfloat16 [4, 16384, 2048], P(None, ('sp', 'tp'))
The draws below stay inside these ranges and needn't reach their ends.
Inputs may be any that keep to these rules, and one draw needn't show every extreme that they name: `log_decay`: every entry is negative; some heads keep a tenth or more of their memory over 16384 positions, others lose most of it within 30 to 100 positions.
All inputs are finite; a program needn't handle non-finite values.
Results may differ from the reference program's by a relative error of at most 0.015.
Values may be sent and summed in bfloat16 or wider, within the bound.
A program may use at most 64 MiB of HBM per device.

```python
import math
import jax
import jax.numpy as jnp
from jax import lax

D = 2048
HEADS = 8
HEAD_DIM = 128
BLOCK = 128
SEQS = 4
RET_WIDTH = 1024
SEQLEN = 16384


def draw_log_decay(key, part):
    head_order = jax.random.permutation(jax.random.fold_in(key, 11), HEADS)
    slow_heads = head_order < HEADS // 2
    uniform_draw = jax.random.uniform(jax.random.fold_in(key, 12), (HEADS,), jnp.float32)
    slow_rate = math.log(10.0) / SEQLEN * (0.1 + 0.9 * uniform_draw)
    fast_rate = jnp.exp(math.log(1.0 / 100.0) + uniform_draw * (math.log(1.0 / 30.0) - math.log(1.0 / 100.0)))
    return -jnp.where(slow_heads, slow_rate, fast_rate).astype(jnp.float32)


def level_of(stream_key, dims, pieces, smallest, high):
    level = 1.0
    for position, parts in pieces:
        steps = jax.random.uniform(jax.random.fold_in(jax.random.fold_in(stream_key, 6), position), (parts,), jnp.float32, smallest / len(pieces), high / len(pieces))
        level = level * jnp.repeat(jnp.exp(steps), dims[position] // parts).reshape((-1,) + (1,) * (len(dims) - 1 - position))
    return level


def noise(own_key, shape, scale, reach, split=(), kind=jnp.bfloat16):
    level = level_of(own_key, shape, split, -0.22, 0.18) if split else 1.0
    values = jax.random.normal(own_key, shape, jnp.float32) * scale * level
    return jnp.minimum(jnp.maximum(values, -reach), reach).astype(kind)


def setup_inputs(seed: int = 0) -> dict:
    keys = jax.random.split(jax.random.key(seed), 11)
    return {
        "tokens": noise(keys[0], (SEQS, SEQLEN, D), 1.0, 6.0, ((1, 256),)),
        "in_gain": jnp.clip(1.0 + 0.18 * jax.random.normal(keys[1], (D,), jnp.float32), 0.1, 1.9),
        "query_weight": noise(keys[2], (D, RET_WIDTH), D ** -0.5, 0.125, ((1, 8),)),
        "key_weight": noise(keys[3], (D, RET_WIDTH), D ** -0.5, 0.125, ((1, 8),)),
        "value_weight": noise(keys[4], (D, RET_WIDTH), D ** -0.5, 0.125, ((1, 8),)),
        "gate_weight": noise(keys[5], (D, RET_WIDTH), D ** -0.5, 0.125, ((1, 8),)),
        "log_decay": draw_log_decay(jax.random.fold_in(keys[10], 71), 0),
        "norm_gain": jnp.clip(1.0 + 0.18 * jax.random.normal(keys[7], (RET_WIDTH,), jnp.float32), 0.1, 1.9),
        "out_weight": noise(keys[8], (RET_WIDTH, D), RET_WIDTH ** -0.5, 0.1875),
        "post_gain": jnp.clip(1.0 + 0.18 * jax.random.normal(keys[9], (D,), jnp.float32), 0.1, 1.9),
    }


rms_eps = 1e-06
group_eps = 1e-05
rope_base = 10000.0
highest = lax.Precision.HIGHEST

def rotate(values, positions):
    half_dim = values.shape[-1] // 2
    inverse = rope_base ** (-jnp.arange(half_dim, dtype=jnp.float32) / half_dim)
    angles = positions.astype(jnp.float32)[:, None] * inverse[None, :]
    cosine = jnp.cos(angles)
    sine_part = jnp.sin(angles)
    first_half = values[..., :half_dim].astype(jnp.float32)
    second = values[..., half_dim:].astype(jnp.float32)
    return jnp.concatenate([first_half * cosine - second * sine_part, first_half * sine_part + second * cosine], axis=-1)

def retain(queries, key_rows, values, log_decay):
    seq_count, head_count, length, head_width = queries.shape
    block_count = length // BLOCK
    offsets = jnp.arange(BLOCK, dtype=jnp.float32)
    distance = offsets[:, None] - offsets[None, :]
    rate_col = log_decay[:, None, None]
    inside = jnp.where(distance >= 0, jnp.exp(rate_col * jnp.maximum(distance, 0.0)), 0.0)
    query_scale = jnp.exp(log_decay[:, None] * (offsets + 1.0))[..., None]
    key_scale = jnp.exp(log_decay[:, None] * (BLOCK - 1.0 - offsets))[..., None]
    block_decay = jnp.exp(log_decay * BLOCK)[:, None, None]

    def to_blocks(arr):
        return arr.reshape(seq_count, head_count, block_count, BLOCK, arr.shape[-1]).transpose(2, 0, 1, 3, 4)

    def advance(memory, inputs):
        q_block, k_block, v_block = inputs
        qf = q_block.astype(jnp.float32)
        kf = k_block.astype(jnp.float32)
        vf = v_block.astype(jnp.float32)
        scores = jnp.einsum('shqd,shkd->shqk', qf, kf, precision=highest)
        weights = (scores * inside).astype(jnp.bfloat16)
        within = jnp.einsum('shqk,shkv->shqv', weights.astype(jnp.float32), vf, precision=highest)
        carried = jnp.einsum('shqd,shdv->shqv', qf * query_scale, memory, precision=highest)
        k_scaled = (kf * key_scale).astype(jnp.bfloat16)
        memory = memory * block_decay + jnp.einsum('shkd,shkv->shdv', k_scaled.astype(jnp.float32), vf, precision=highest)
        return (memory, within + carried)
    start_memory = jnp.zeros((seq_count, head_count, head_width, values.shape[-1]), jnp.float32)
    outputs = lax.scan(advance, start_memory, (to_blocks(queries), to_blocks(key_rows), to_blocks(values)))[1]
    return outputs.transpose(1, 2, 0, 3, 4).reshape(seq_count, head_count, length, values.shape[-1])

def reference(tokens, in_gain, query_weight, key_weight, value_weight, gate_weight, log_decay, norm_gain, out_weight, post_gain):
    seq_count, length, model_width = tokens.shape
    tok_f32 = tokens.astype(jnp.float32)
    normed = (tok_f32 * lax.rsqrt(lax.optimization_barrier(jnp.mean(tok_f32 * tok_f32, axis=-1, keepdims=True)) + rms_eps) * in_gain).astype(jnp.bfloat16)
    flat_rows = normed.reshape(seq_count * length, model_width)

    def project(weight_mat):
        result = jnp.dot(flat_rows, weight_mat, preferred_element_type=jnp.float32).astype(jnp.bfloat16)
        return result.reshape(seq_count, length, HEADS, HEAD_DIM).transpose(0, 2, 1, 3)
    positions = jnp.arange(length, dtype=jnp.int32)
    queries = rotate(project(query_weight), positions).astype(jnp.bfloat16)
    key_rows = (rotate(project(key_weight), positions) * HEAD_DIM ** (-0.5)).astype(jnp.bfloat16)
    values = project(value_weight)
    gating = jnp.dot(flat_rows, gate_weight, preferred_element_type=jnp.float32).astype(jnp.bfloat16)
    gating = gating.reshape(seq_count, length, RET_WIDTH)
    retained = retain(queries, key_rows, values, log_decay)
    center = lax.optimization_barrier(jnp.mean(retained, axis=-1, keepdims=True))
    spread = lax.optimization_barrier(jnp.mean(jnp.square(retained - center), axis=-1, keepdims=True))
    normal = ((retained - center) * lax.rsqrt(spread + group_eps)).transpose(0, 2, 1, 3).reshape(seq_count, length, RET_WIDTH)
    gated = (normal * norm_gain * jax.nn.silu(gating.astype(jnp.float32))).astype(jnp.bfloat16)
    premix = jnp.dot(gated.reshape(seq_count * length, RET_WIDTH), out_weight, preferred_element_type=jnp.float32)
    mixed = premix * lax.rsqrt(lax.optimization_barrier(jnp.mean(premix * premix, axis=-1, keepdims=True)) + rms_eps) * post_gain
    return mixed.astype(jnp.bfloat16).reshape(seq_count, length, model_width)
```

```python
import functools

import jax
import jax.numpy as jnp
import numpy as np
from jax import lax
from jax.experimental import pallas as pl
from jax.experimental.pallas import tpu as pltpu
from jax.sharding import PartitionSpec as P

MESH = pl.DeviceIdType.MESH
F32 = jnp.float32
BF16 = jnp.bfloat16
HD = 128
BLOCK = 128
NY = 4
RMS_EPS = 1e-06
GROUP_EPS = 1e-05
ROPE_BASE = 10000.0


def rotary_tables(blocks):
    half = HD // 2
    rate = ROPE_BASE ** (-np.arange(half, dtype=np.float64) / half)
    rate = np.concatenate([rate, rate])
    inside = np.arange(BLOCK, dtype=np.float64)[:, None] * rate
    starts = BLOCK * np.arange(blocks, dtype=np.float64)[:, None] * rate
    tables = (np.cos(inside), np.sin(inside), np.cos(starts), np.sin(starts))
    return [t.astype(np.float32) for t in tables]


def kernel(
    nz, ny, tok_hbm, gain, wq, wk, wv, wg, ld_ref, ng, ow, pg, cin, sin_, cbl, sbl, out_ref,
    raw, tok, w, oww, ctab, stab, dmat, qsc, ksc, qs, acc, gs, smat, esend, ybuf, zsnd, zbuf, msnd, mbuf,
    gsend, gat, osc, lsem, xs, xr, rs, rr, ps, pr, ys, yr, zs, zr, ms, mr, as_, ar,
):
    nseq, rows, width = raw.shape
    ntp = 8
    nchip = ntp // 2
    hr = rows // 2
    qr = HD // ny
    sp = lax.axis_index("sp")
    me = lax.axis_index("tp")
    z, y = sp // ny, sp % ny
    chip, core = me // 2, me % 2
    partner = chip * 2 + 1 - core
    left_chip, right_chip, far_chip = (chip + 3) % nchip, (chip + 1) % nchip, (chip + 2) % nchip
    left, right, far = left_chip * 2 + core, right_chip * 2 + core, far_chip * 2 + core

    barrier = pltpu.get_barrier_semaphore()
    peers = [(sp, (me + k) % ntp) for k in range(1, ntp)]
    peers += [(z * ny + (y + k) % ny, me) for k in range(1, ny)]
    peers += [((z + k) % nz * ny + y, me) for k in range(1, nz)]
    for dev in peers:
        pl.semaphore_signal(barrier, inc=1, device_id=dev, device_id_type=MESH)

    loads = [pltpu.make_async_copy(tok_hbm, raw, lsem.at[0])]
    for j, src in enumerate((wq, wk, wv, wg)):
        loads.append(pltpu.make_async_copy(src, w.at[:, j * HD:(j + 1) * HD], lsem.at[1 + j]))
    loads.append(pltpu.make_async_copy(ow, oww, lsem.at[5]))
    for load in loads:
        load.start()

    def remote(src, dst, send, recv, dev):
        return pltpu.make_async_remote_copy(
            src_ref=src, dst_ref=dst, send_sem=send, recv_sem=recv, device_id=dev, device_id_type=MESH
        )

    def piece(s, d, lo, n):
        return tok.at[s, pl.ds(pl.multiple_of(d * rows + lo, hr), n), :]

    halves = (0, hr, hr, 0)

    def own_send(s, i):
        ref = piece(s, me, halves[i], hr)
        return remote(ref, ref, xs.at[s, i], xr.at[s, i], (sp, (right, right, left, left)[i]))

    def own_recv(s, i):
        ref = piece(s, (left, left, right, right)[i], halves[i], hr)
        return remote(ref, ref, xs.at[s, i], xr.at[s, i], (sp, right))

    def relay_send(s, i):
        ref = piece(s, (left, right)[i], i * hr, hr)
        return remote(ref, ref, rs.at[s, i], rr.at[s, i], (sp, (right, left)[i]))

    def relay_recv(s, i):
        ref = piece(s, far, i * hr, hr)
        return remote(ref, ref, rs.at[s, i], rr.at[s, i], (sp, right))

    same = (me, left, right, far)
    other = tuple(chip_ * 2 + 1 - core for chip_ in (chip, left_chip, right_chip, far_chip))

    def pair_send(s, i):
        ref = piece(s, same[i], 0, rows)
        return remote(ref, ref, ps.at[s, i], pr.at[s, i], (sp, partner))

    def pair_recv(s, i):
        ref = piece(s, other[i], 0, rows)
        return remote(ref, ref, ps.at[s, i], pr.at[s, i], (sp, partner))

    def ycopy(s, to):
        src = esend.at[s, pl.ds(pl.multiple_of(to * qr, qr), qr), :]
        return remote(src, ybuf.at[s, y], ys.at[s, to], yr.at[s, y], (z * ny + to, me))

    def yrecv(s, frm):
        ref = ybuf.at[s, frm]
        return remote(ref, ref, ys.at[s, frm], yr.at[s, frm], (z * ny + frm, me))

    def zcopy(s, to):
        return remote(zsnd.at[s], zbuf.at[s, z], zs.at[s, to], zr.at[s, z], (to * ny + y, me))

    def zrecv(s, frm):
        ref = zbuf.at[s, frm]
        return remote(ref, ref, zs.at[s, frm], zr.at[s, frm], (frm * ny + y, me))

    def mcopy(s, to):
        dst = mbuf.at[s, pl.ds(pl.multiple_of(y * qr, qr), qr), :]
        return remote(msnd.at[s, to], dst, ms.at[s, to], mr.at[s, y], (z * ny + to, me))

    def mrecv(s, frm):
        ref = mbuf.at[s, pl.ds(pl.multiple_of(frm * qr, qr), qr), :]
        return remote(ref, ref, ms.at[s, frm], mr.at[s, frm], (z * ny + frm, me))

    def acopy(s, to):
        src = gsend.at[s, pl.ds(pl.multiple_of(to * rows, rows), rows), :]
        dst = gat.at[s, :, pl.ds(pl.multiple_of(me * HD, HD), HD)]
        return remote(src, dst, as_.at[s, to], ar.at[s, me], (sp, to))

    def arecv(s, frm):
        ref = gat.at[s, :, pl.ds(pl.multiple_of(frm * HD, HD), HD)]
        return remote(ref, ref, as_.at[s, frm], ar.at[s, frm], (sp, frm))

    ld = ld_ref[0]
    i_col = lax.broadcasted_iota(jnp.int32, (BLOCK, HD), 0).astype(F32)
    i_row = lax.broadcasted_iota(jnp.int32, (BLOCK, HD), 1).astype(F32)
    dist = i_col - i_row
    dmat[...] = jnp.where(dist >= 0, jnp.exp(ld * jnp.maximum(dist, 0.0)), 0.0)
    qsc[...] = jnp.exp(ld * (i_col + 1.0))
    ksc[...] = jnp.exp(ld * (BLOCK - 1.0 - i_col))
    sign = jnp.where(i_row < HD // 2, -1.0, 1.0)

    def decay(count):
        return jnp.exp(jnp.full((1, HD), ld * count, F32))

    @pl.loop(0, nchip)
    def _(b):
        block = sp * nchip + b
        cb = cbl[pl.ds(block, 1), :]
        sb = sbl[pl.ds(block, 1), :]
        ctab[b] = cin[...] * cb - sin_[...] * sb
        stab[b] = (sin_[...] * cb + cin[...] * sb) * sign

    loads[0].wait()
    part = 16

    @pl.loop(0, nseq * (rows // part))
    def _(t):
        s, c = t // (rows // part), t % (rows // part)
        v = raw[s, pl.ds(pl.multiple_of(c * part, part), part), :].astype(F32)
        scale = lax.rsqrt(jnp.mean(v * v, axis=-1, keepdims=True) + RMS_EPS)
        at = pl.multiple_of(me * rows + c * part, part)
        tok[s, pl.ds(at, part), :] = (v * scale * gain[...]).astype(BF16)

    pl.semaphore_wait(barrier, len(peers))

    def start_own(s):
        for i in (0, 2, 1, 3):
            own_send(s, i).start()
        pair_send(s, 0).start()

    start_own(0)
    for load in loads[1:]:
        load.wait()

    def rotate(u, b):
        return u * ctab[b] + pltpu.roll(u, HD // 2, 1) * stab[b]

    def block_work(s, b):
        at = pl.ds(pl.multiple_of(b * BLOCK, BLOCK), BLOCK)
        proj = jnp.dot(tok[s, at, :], w[...], preferred_element_type=F32).astype(BF16)
        q = rotate(proj[:, :HD].astype(F32), b).astype(BF16)
        k = (rotate(proj[:, HD:2 * HD].astype(F32), b) * HD ** -0.5).astype(BF16)
        v = proj[:, 2 * HD:3 * HD]
        g = proj[:, 3 * HD:].astype(F32)
        scores = lax.dot_general(q, k, (((1,), (1,)), ((), ())), preferred_element_type=F32)
        weights = (scores * dmat[...]).astype(BF16)
        acc[s, at, :] = jnp.dot(weights, v, preferred_element_type=F32)
        qs[s, at, :] = (q.astype(F32) * qsc[...]).astype(BF16)
        ks = (k.astype(F32) * ksc[...]).astype(BF16)
        smat[b] = lax.dot_general(ks, v, (((0,), (0,)), ((), ())), preferred_element_type=F32)
        gs[s, at, :] = ng[...] * (g * jax.nn.sigmoid(g))

    def state_out(s):
        step = decay(float(BLOCK))
        prefix = smat[0]
        befores = []
        for b in range(1, nchip):
            befores.append(prefix.astype(BF16))
            prefix = prefix * step + smat[b]
        esend[s] = prefix.astype(BF16)
        ybuf[s, y] = esend[s, pl.ds(pl.multiple_of(y * qr, qr), qr), :]
        for k in range(1, ny):
            ycopy(s, (y + k) % ny).start()
        for b in range(1, nchip):
            at = pl.ds(b * BLOCK, BLOCK)
            acc[s, at, :] += jnp.dot(qs[s, at, :], befores[b - 1], preferred_element_type=F32)

    def state_row(s):
        for k in range(1, ny):
            yrecv(s, (y + k) % ny).wait_recv()
        span = decay(float(BLOCK * nchip))
        total = ybuf[s, 0].astype(F32)
        for k in range(1, ny):
            total = total * span + ybuf[s, k].astype(F32)
        zsnd[s] = total.astype(BF16)

        @pl.loop(z + 1, nz)
        def _(to):
            zcopy(s, to).start()

    def state_back(s):
        span = decay(float(BLOCK * nchip))
        row_span = decay(float(BLOCK * nchip * ny))

        def add(frm, total):
            zrecv(s, frm).wait_recv()
            return total * row_span + zbuf[s, frm].astype(F32)

        carried = lax.fori_loop(0, z, add, jnp.zeros((qr, HD), F32))
        for k in range(ny):
            msnd[s, k] = carried.astype(BF16)
            if k < ny - 1:
                carried = carried * span + ybuf[s, k].astype(F32)
        mbuf[s, pl.ds(pl.multiple_of(y * qr, qr), qr), :] = msnd[s, y]
        for k in range(1, ny):
            mcopy(s, (y + k) % ny).start()

    def read_out(s):
        for k in range(1, ny):
            mrecv(s, (y + k) % ny).wait_recv()
        memory = mbuf[s]
        for b in range(nchip):
            at = pl.ds(b * BLOCK, BLOCK)
            kept = jnp.dot(qs[s, at, :], memory, preferred_element_type=F32)
            kept = acc[s, at, :] + kept * decay(float(BLOCK * b))
            kept = kept - jnp.mean(kept, axis=-1, keepdims=True)
            spread = jnp.mean(kept * kept, axis=-1, keepdims=True)
            gsend[s, at, :] = (kept * lax.rsqrt(spread + GROUP_EPS) * gs[s, at, :]).astype(BF16)
        for k in range(1, ntp):
            acopy(s, (me + k) % ntp).start()
        own = gsend[s, pl.ds(pl.multiple_of(me * rows, rows), rows), :]
        gat[s, :, pl.ds(pl.multiple_of(me * HD, HD), HD)] = own

    def mix(s):
        for k in range(1, ntp):
            arecv(s, (me + k) % ntp).wait_recv()
        osc[...] = jnp.dot(gat[s], oww[...], preferred_element_type=F32)

        @pl.loop(0, rows // part)
        def _(c):
            at = pl.ds(pl.multiple_of(c * part, part), part)
            v = osc[at, :]
            scale = lax.rsqrt(jnp.mean(v * v, axis=-1, keepdims=True) + RMS_EPS)
            out_ref[s, at, :] = (v * scale * pg[...]).astype(BF16)

    @pl.loop(0, nseq + 2)
    def _(t):
        tokens_left = t < nseq
        scanning = (t >= 1) & (t <= nseq)
        reading = t >= 2

        @pl.when(tokens_left)
        def _():
            own_recv(t, 0).wait_recv()
            relay_send(t, 0).start()
            own_recv(t, 2).wait_recv()
            relay_send(t, 1).start()

            @pl.when(t + 1 < nseq)
            def _():
                start_own(t + 1)

        @pl.when(reading)
        def _():
            read_out(t - 2)

        @pl.when(tokens_left)
        def _():
            pair_recv(t, 0).wait_recv()
            block_work(t, chip)

        @pl.when(scanning)
        def _():
            state_row(t - 1)

        @pl.when(tokens_left)
        def _():
            own_recv(t, 1).wait_recv()
            pair_send(t, 1).start()
            own_recv(t, 3).wait_recv()
            pair_send(t, 2).start()
            pair_recv(t, 1).wait_recv()
            block_work(t, left_chip)
            pair_recv(t, 2).wait_recv()
            block_work(t, right_chip)

        @pl.when(reading)
        def _():
            mix(t - 2)

        @pl.when(scanning)
        def _():
            state_back(t - 1)

        @pl.when(tokens_left)
        def _():
            relay_recv(t, 0).wait_recv()
            relay_recv(t, 1).wait_recv()
            pair_send(t, 3).start()
            pair_recv(t, 3).wait_recv()
            block_work(t, far_chip)
            state_out(t)

    @pl.loop(0, nseq)
    def _(s):
        for i in range(4):
            own_send(s, i).wait_send()
            pair_send(s, i).wait_send()
        for i in range(2):
            relay_send(s, i).wait_send()
        for k in range(1, ny):
            ycopy(s, (y + k) % ny).wait_send()
            mcopy(s, (y + k) % ny).wait_send()
        for k in range(1, ntp):
            acopy(s, (me + k) % ntp).wait_send()

        @pl.loop(z + 1, nz)
        def _(to):
            zcopy(s, to).wait_send()


def body(nz, ny, tokens, in_gain, wq, wk, wv, wg, log_decay, norm_gain, out_weight, post_gain):
    nseq, rows, width = tokens.shape
    ntp = 8
    stretch = rows * ntp
    tables = [jnp.asarray(t) for t in rotary_tables(nz * ny * stretch // BLOCK)]
    qr = HD // ny
    vmem, hbm, smem = (pl.BlockSpec(memory_space=m) for m in (pltpu.VMEM, pl.ANY, pltpu.SMEM))
    dma = pltpu.SemaphoreType.DMA
    scratch = [
        pltpu.VMEM((nseq, rows, width), BF16),
        pltpu.VMEM((nseq, stretch, width), BF16),
        pltpu.VMEM((width, 4 * HD), BF16),
        pltpu.VMEM(out_weight.shape, BF16),
        pltpu.VMEM((stretch // BLOCK, BLOCK, HD), F32),
        pltpu.VMEM((stretch // BLOCK, BLOCK, HD), F32),
        pltpu.VMEM((BLOCK, HD), F32),
        pltpu.VMEM((BLOCK, HD), F32),
        pltpu.VMEM((BLOCK, HD), F32),
        pltpu.VMEM((nseq, stretch, HD), BF16),
        pltpu.VMEM((nseq, stretch, HD), F32),
        pltpu.VMEM((nseq, stretch, HD), F32),
        pltpu.VMEM((stretch // BLOCK, HD, HD), F32),
        pltpu.VMEM((nseq, HD, HD), BF16),
        pltpu.VMEM((nseq, ny, qr, HD), BF16),
        pltpu.VMEM((nseq, qr, HD), BF16),
        pltpu.VMEM((nseq, nz, qr, HD), BF16),
        pltpu.VMEM((nseq, ny, qr, HD), BF16),
        pltpu.VMEM((nseq, HD, HD), BF16),
        pltpu.VMEM((nseq, stretch, HD), BF16),
        pltpu.VMEM((nseq, rows, ntp * HD), BF16),
        pltpu.VMEM((rows, width), F32),
        dma((6,)),
        dma((nseq, 4)), dma((nseq, 4)), dma((nseq, 2)), dma((nseq, 2)), dma((nseq, 4)), dma((nseq, 4)),
        dma((nseq, ny)), dma((nseq, ny)), dma((nseq, nz)), dma((nseq, nz)), dma((nseq, ny)), dma((nseq, ny)),
        dma((nseq, ntp)), dma((nseq, ntp)),
    ]
    return pl.pallas_call(
        functools.partial(kernel, nz, ny),
        out_shape=jax.ShapeDtypeStruct(tokens.shape, BF16),
        in_specs=[hbm, vmem, hbm, hbm, hbm, hbm, smem, vmem, hbm, vmem, vmem, vmem, vmem, vmem],
        out_specs=vmem,
        scratch_shapes=scratch,
        name="retention",
        compiler_params=pltpu.CompilerParams(
            collective_id=0, has_side_effects=True, vmem_limit_bytes=60 * 1024 * 1024
        ),
    )(
        tokens, in_gain.reshape(1, -1), wq, wk, wv, wg, log_decay, norm_gain.reshape(1, -1), out_weight,
        post_gain.reshape(1, -1), *tables,
    )


def solution(mesh):
    both = ("sp", "tp")
    nz = mesh.shape["sp"] // NY
    return jax.shard_map(
        functools.partial(body, nz, NY),
        mesh=mesh,
        in_specs=(
            P(None, both, None), P(), P(None, "tp"), P(None, "tp"), P(None, "tp"), P(None, "tp"), P("tp"), P("tp"),
            P(), P(),
        ),
        out_specs=P(None, both, None),
        check_vma=False,
    )
```

```python
import functools

import jax
import jax.numpy as jnp
import numpy as np
from jax import lax
from jax.experimental import pallas as pl
from jax.experimental.pallas import tpu as pltpu
from jax.sharding import PartitionSpec as P

MESH = pl.DeviceIdType.MESH
F32 = jnp.float32
BF16 = jnp.bfloat16
HD = 128
BLOCK = 128
NY = 4
RMS_EPS = 1e-06
GROUP_EPS = 1e-05
ROPE_BASE = 10000.0


def rotary_tables(blocks):
    half = HD // 2
    rate = ROPE_BASE ** (-np.arange(half, dtype=np.float64) / half)
    rate = np.concatenate([rate, rate])
    inside = np.arange(BLOCK, dtype=np.float64)[:, None] * rate
    starts = BLOCK * np.arange(blocks, dtype=np.float64)[:, None] * rate
    tables = (np.cos(inside), np.sin(inside), np.cos(starts), np.sin(starts))
    return [t.astype(np.float32) for t in tables]


def kernel(
    nz, ny, tok_hbm, gain_hbm, wq, wk, wv, wg, ld_ref, ng_hbm, ow, pg_hbm, tab_hbm, out_ref,
    raw, tok, w, oww, gain, pg, tabs, crow, ctab, stab, dmat, qsc, ksc, qs, acc, gs, smat, esend, ybuf, zsnd, zbuf,
    msnd, mbuf, gsend, gat, osc, lsem, xs, xr, ps, pr, wxs, wxr, wfs, wfr, cs, cr, ys, yr, zs, zr, ms, mr, as_, ar,
    ready_a, ready_b,
):
    nseq, rows, width = raw.shape
    ntp = 8
    nchip = ntp // 2
    blocks = 2
    span = blocks * BLOCK
    qr = HD // ny
    quarter = width // 4
    chunk = quarter // 4
    sp = lax.axis_index("sp")
    me = lax.axis_index("tp")
    z, y = sp // ny, sp % ny
    chip, core = me // 2, me % 2
    partner = chip * 2 + 1 - core
    half, dl = chip // 2, me % 4
    mine, theirs = chip % 2, 1 - chip % 2
    pair_same = (half * 2 + theirs) * 2 + core
    pair_other = (half * 2 + theirs) * 2 + 1 - core
    mate = (nchip - 1 - chip) * 2 + core

    def at(zz, yy):
        return (zz + nz) % nz * ny + (yy + ny) % ny

    barrier = pltpu.get_barrier_semaphore()
    near = [(at(z, y + k), me) for k in range(1, ny)] + [(at(z - 1, y), me), (at(z + 1, y), me), (sp, mate)]
    peers = [(sp, partner), (sp, pair_same), (sp, pair_other)] + near
    for dev in peers:
        pl.semaphore_signal(barrier, inc=1, device_id=dev, device_id_type=MESH)

    raw_loads = [pltpu.make_async_copy(tok_hbm.at[s], raw.at[s], lsem.at[s]) for s in range(nseq)]
    gain_load = pltpu.make_async_copy(gain_hbm, gain, lsem.at[4])
    tab_load = pltpu.make_async_copy(tab_hbm, tabs, lsem.at[5])
    ng_load = pltpu.make_async_copy(ng_hbm, crow.at[0, pl.ds(0, 1)], lsem.at[6])
    pg_load = pltpu.make_async_copy(pg_hbm, pg, lsem.at[7])
    w_load = pltpu.make_async_copy(w.at[0], w.at[0], lsem.at[8])
    ow_load = pltpu.make_async_copy(oww, oww, lsem.at[9])
    gain_load.start()
    for load in raw_loads:
        load.start()
    ng_load.start()
    for j, src in enumerate((wq, wk, wv, wg)):
        pltpu.make_async_copy(src, w.at[0, :, j * HD:(j + 1) * HD], lsem.at[8]).start()
    tab_load.start()
    pg_load.start()
    for d in range(4):
        first = half * 4 + d
        second = (nchip - 1 - first // 2) * 2 + d % 2
        for i, h in enumerate((first, second)):
            src = ow.at[pl.ds(pl.multiple_of(h * HD, HD), HD), :]
            pltpu.make_async_copy(src, oww.at[(2 * d + i) * HD:(2 * d + i + 1) * HD, :], lsem.at[9]).start()

    def remote(src, dst, send, recv, dev):
        return pltpu.make_async_remote_copy(
            src_ref=src, dst_ref=dst, send_sem=send, recv_sem=recv, device_id=dev, device_id_type=MESH
        )

    def part_of(s, d):
        return tok.at[s, pl.ds(pl.multiple_of(d * rows, rows), rows), :]

    def own_send(s):
        ref = part_of(s, dl)
        return remote(ref, ref, xs.at[0], xr.at[s], (sp, pair_same))

    def own_recv(s):
        ref = part_of(s, theirs * 2 + core)
        return remote(ref, ref, xs.at[0], xr.at[s], (sp, pair_same))

    def pass_send(s, i):
        ref = part_of(s, (mine, theirs)[i] * 2 + core)
        return remote(ref, ref, ps.at[0], pr.at[s, i], (sp, partner))

    def pass_recv(s, i):
        ref = part_of(s, (mine, theirs)[i] * 2 + 1 - core)
        return remote(ref, ref, ps.at[0], pr.at[s, i], (sp, partner))

    my_quarter = (y % 2) * 2 + z % 2

    def w_rows(k, j):
        return w.at[k, pl.ds(pl.multiple_of(my_quarter * quarter + j * chunk, chunk), chunk), :]

    def w_send(j):
        return remote(w_rows(0, j), w_rows(1, j), wxs.at[0], wxr.at[j], (sp, mate))

    def w_recv(j):
        return remote(w_rows(1, j), w_rows(1, j), wxs.at[0], wxr.at[j], (sp, mate))

    def w_forward(j):
        w_recv(j).wait_recv()
        yy, zz = y + (1, 1, -1, -1)[j], z + (1, -1, 1, -1)[j]
        for dev in (at(z, yy), at(zz, y), at(zz, yy)):
            remote(w_rows(1, j), w_rows(1, j), wfs.at[0], wfr.at[0], (dev, me)).start()

    def w_rest(rows_):
        ref = w.at[1, 0:rows_, :]
        return remote(ref, ref, wfs.at[0], wfr.at[0], (sp, partner))

    def c_send():
        return remote(crow.at[0], crow.at[1], cs.at[0], cr.at[0], (sp, mate))

    def ycopy(s, k, to):
        src = esend.at[s, k, pl.ds(pl.multiple_of(to * qr, qr), qr), :]
        return remote(src, ybuf.at[s, y * 2 + half], ys.at[0], yr.at[s], (at(z, to), (me, mate)[k]))

    def zcopy(s, to):
        return remote(zsnd.at[s], zbuf.at[s, z], zs.at[to], zr.at[s, z], (to * ny + y, me))

    def zrecv(s, frm):
        ref = zbuf.at[s, frm]
        return remote(ref, ref, zs.at[frm], zr.at[s, frm], (frm * ny + y, me))

    def mcopy(s, k, to):
        src = msnd.at[s, to * 2 + (half, 1 - half)[k]]
        dst = mbuf.at[s, k, pl.ds(pl.multiple_of(y * qr, qr), qr), :]
        return remote(src, dst, ms.at[0], mr.at[s], (at(z, to), (me, mate)[k]))

    def acopy(s, to):
        src = gsend.at[s, pl.ds(pl.multiple_of(to * rows, rows), rows), :]
        dst = gat.at[s, :, pl.ds(pl.multiple_of(dl * 2 * HD, 2 * HD), 2 * HD)]
        return remote(src, dst, as_.at[0], ar.at[s], (sp, half * 4 + to))

    def whole(ref, send, recv):
        return remote(ref, ref, send, recv, (sp, partner))

    part = 16

    def norm_own(s):
        raw_loads[s].wait()

        @pl.loop(0, rows // part)
        def _(c):
            v = raw[s, pl.ds(pl.multiple_of(c * part, part), part), :].astype(F32)
            scale = lax.rsqrt(jnp.mean(v * v, axis=-1, keepdims=True) + RMS_EPS)
            at_ = pl.multiple_of(dl * rows + c * part, part)
            tok[s, pl.ds(at_, part), :] = (v * scale * gain[...]).astype(BF16)

    gain_load.wait()
    norm_own(0)
    ng_load.wait()
    crow[0, pl.ds(1, 7), :] = jnp.full((7, HD), ld_ref[0], F32)

    pl.semaphore_wait(barrier, len(peers))
    own_send(0).start()
    pass_send(0, 0).start()
    for dev in near:
        pl.semaphore_signal(ready_a, inc=1, device_id=dev, device_id_type=MESH)
    w_load.wait()
    for j in range(4):
        w_send(j).start()
    c_send().start()
    for s in range(1, nseq):
        norm_own(s)
        if s == 1:
            own_send(s).start()
        pass_send(s, 0).start()

    i_col = lax.broadcasted_iota(jnp.int32, (BLOCK, HD), 0).astype(F32)
    i_row = lax.broadcasted_iota(jnp.int32, (BLOCK, HD), 1).astype(F32)

    def decay(k, count):
        return jnp.exp(crow[k, pl.ds(1, 1), :] * count)

    def head_tables(k):
        ld = crow[k, pl.ds(1, 1), :]
        dist = i_col - i_row
        dmat[k] = jnp.where(dist >= 0, jnp.exp(ld * jnp.maximum(dist, 0.0)), 0.0)
        qsc[k] = jnp.exp(ld * (i_col + 1.0))
        ksc[k] = jnp.exp(ld * (BLOCK - 1.0 - i_col))

    head_tables(0)
    tab_load.wait()
    sign = jnp.where(i_row < HD // 2, -1.0, 1.0)
    for b in range(blocks):
        start = sp * nchip + half * blocks + b
        cb = tabs[2, pl.ds(start, 1), :]
        sb = tabs[3, pl.ds(start, 1), :]
        ctab[b] = tabs[0] * cb - tabs[1] * sb
        stab[b] = (tabs[1] * cb + tabs[0] * sb) * sign

    def rotate(u, b):
        return u * ctab[b] + pltpu.roll(u, HD // 2, 1) * stab[b]

    def work(s, k, b0, nb):
        proj = jnp.dot(
            tok[s, pl.ds(pl.multiple_of(b0 * BLOCK, BLOCK), nb * BLOCK), :], w[k], preferred_element_type=F32
        ).astype(BF16)
        for i in range(nb):
            b = b0 + i
            here = pl.ds(pl.multiple_of(b * BLOCK, BLOCK), BLOCK)
            p = proj[i * BLOCK:(i + 1) * BLOCK]
            q = rotate(p[:, :HD].astype(F32), b).astype(BF16)
            kk = (rotate(p[:, HD:2 * HD].astype(F32), b) * HD ** -0.5).astype(BF16)
            v = p[:, 2 * HD:3 * HD]
            g = p[:, 3 * HD:].astype(F32)
            scores = lax.dot_general(q, kk, (((1,), (1,)), ((), ())), preferred_element_type=F32)
            weights = (scores * dmat[k]).astype(BF16)
            acc[s, k, here, :] = jnp.dot(weights, v, preferred_element_type=F32)
            qs[s, k, here, :] = (q.astype(F32) * qsc[k]).astype(BF16)
            ks = (kk.astype(F32) * ksc[k]).astype(BF16)
            smat[s, k, b] = lax.dot_general(ks, v, (((0,), (0,)), ((), ())), preferred_element_type=F32)
            gs[s, k, here, :] = crow[k, pl.ds(0, 1), :] * (g * jax.nn.sigmoid(g))

    def state_out(s):
        for k in range(2):
            esend[s, k] = (smat[s, k, 0] * decay(k, float(BLOCK)) + smat[s, k, 1]).astype(BF16)
        ybuf[s, y * 2 + half] = esend[s, 0, pl.ds(pl.multiple_of(y * qr, qr), qr), :]
        for to in range(ny):
            ycopy(s, 1, (y + to) % ny).start()
            if to:
                ycopy(s, 0, (y + to) % ny).start()
        for k in range(2):
            here = pl.ds(BLOCK, BLOCK)
            acc[s, k, here, :] += jnp.dot(
                qs[s, k, here, :], smat[s, k, 0].astype(BF16), preferred_element_type=F32
            )

    def state_row(s):
        whole(ybuf.at[s, pl.ds(0, 2 * ny - 1)], ys.at[0], yr.at[s]).wait_recv()
        step = decay(0, float(span))
        total = ybuf[s, 0].astype(F32)
        for k in range(1, 2 * ny):
            total = total * step + ybuf[s, k].astype(F32)
        zsnd[s] = total.astype(BF16)

        @pl.loop(z + 1, nz)
        def _(to):
            zcopy(s, to).start()

    def state_back(s):
        step = decay(0, float(span))
        row_step = decay(0, float(span * 2 * ny))

        def add(frm, total):
            zrecv(s, frm).wait_recv()
            return total * row_step + zbuf[s, frm].astype(F32)

        carried = lax.fori_loop(0, z, add, jnp.zeros((qr, HD), F32))
        for k in range(2 * ny):
            msnd[s, k] = carried.astype(BF16)
            if k < 2 * ny - 1:
                carried = carried * step + ybuf[s, k].astype(F32)
        mbuf[s, 0, pl.ds(pl.multiple_of(y * qr, qr), qr), :] = msnd[s, y * 2 + half]
        for to in range(ny):
            mcopy(s, 1, (y + to) % ny).start()
            if to:
                mcopy(s, 0, (y + to) % ny).start()

    def read_out(s):
        whole(ybuf.at[s, pl.ds(0, 2 * ny - 1)], ms.at[0], mr.at[s]).wait_recv()
        for k in range(2):
            memory = mbuf[s, k]
            for b in range(blocks):
                here = pl.ds(b * BLOCK, BLOCK)
                kept = jnp.dot(qs[s, k, here, :], memory, preferred_element_type=F32)
                kept = acc[s, k, here, :] + kept * decay(k, float(BLOCK * b))
                kept = kept - jnp.mean(kept, axis=-1, keepdims=True)
                spread = jnp.mean(kept * kept, axis=-1, keepdims=True)
                kept = kept * lax.rsqrt(spread + GROUP_EPS) * gs[s, k, here, :]
                gsend[s, here, k * HD:(k + 1) * HD] = kept.astype(BF16)
        for k in range(1, 4):
            acopy(s, (dl + k) % 4).start()
        own = gsend[s, pl.ds(pl.multiple_of(dl * rows, rows), rows), :]
        gat[s, :, pl.ds(pl.multiple_of(dl * 2 * HD, 2 * HD), 2 * HD)] = own

    def mix(s):
        whole(gat.at[s, :, 0:6 * HD], as_.at[0], ar.at[s]).wait_recv()
        osc[...] = jnp.dot(gat[s], oww[...], preferred_element_type=F32)

        @pl.loop(0, rows // part)
        def _(c):
            here = pl.ds(pl.multiple_of(c * part, part), part)
            v = osc[here, :]
            scale = lax.rsqrt(jnp.mean(v * v, axis=-1, keepdims=True) + RMS_EPS)
            out_ref[s, here, :] = (v * scale * pg[...]).astype(BF16)

    @pl.loop(0, nseq)
    def _(s):
        pass_recv(s, 0).wait_recv()
        work(s, 0, mine, 1)

    pl.semaphore_wait(ready_a, len(near))
    for dev in ((at(z - 2, y), me), (at(z + 2, y), me)):
        pl.semaphore_signal(ready_b, inc=1, device_id=dev, device_id_type=MESH)
    w_forward(0)
    for s in range(2):
        own_recv(s).wait_recv()
        pass_send(s, 1).start()
        own_send(s + 2).start()
        w_forward(1 + 2 * s)
        pass_recv(s, 1).wait_recv()
        work(s, 0, theirs, 1)
        if s == 0:
            w_forward(2)
    whole(crow.at[1], cs.at[0], cr.at[0]).wait_recv()
    head_tables(1)
    w_rest(3 * quarter).wait_recv()

    @pl.loop(0, 2)
    def _(s):
        work(s, 1, 0, 2)
        state_out(s)

    own_recv(2).wait_recv()
    pass_send(2, 1).start()
    pass_recv(2, 1).wait_recv()
    work(2, 0, theirs, 1)
    work(2, 1, 0, 2)
    state_out(2)
    work(3, 1, mine, 1)
    pl.semaphore_wait(ready_b, 2)
    state_row(0)
    state_row(1)
    own_recv(3).wait_recv()
    pass_send(3, 1).start()
    pass_recv(3, 1).wait_recv()
    work(3, 0, theirs, 1)
    work(3, 1, theirs, 1)
    state_out(3)
    state_row(2)
    state_row(3)
    state_back(0)
    state_back(1)
    state_back(2)
    read_out(0)
    read_out(1)
    state_back(3)
    ow_load.wait()
    pg_load.wait()
    read_out(2)
    mix(0)
    mix(1)
    read_out(3)
    mix(2)
    mix(3)

    whole(raw, xs.at[0], xr.at[0]).wait_send()
    whole(tok.at[:, 0:2 * rows, :], ps.at[0], pr.at[0, 0]).wait_send()
    whole(w.at[1, 0:quarter, :], wxs.at[0], wxr.at[0]).wait_send()
    w_rest(3 * quarter).wait_send()
    whole(crow.at[0], cs.at[0], cr.at[0]).wait_send()
    whole(ybuf.at[:, pl.ds(0, 2 * ny - 1)], ys.at[0], yr.at[0]).wait_send()
    whole(ybuf.at[:, pl.ds(0, 2 * ny - 1)], ms.at[0], mr.at[0]).wait_send()
    whole(gat.at[:, :, 0:6 * HD], as_.at[0], ar.at[0]).wait_send()

    @pl.loop(z + 1, nz)
    def _(to):
        whole(zsnd, zs.at[to], zr.at[0, to]).wait_send()


def body(nz, ny, tokens, in_gain, wq, wk, wv, wg, log_decay, norm_gain, out_weight, post_gain):
    nseq, rows, width = tokens.shape
    ntp = 8
    stretch = rows * ntp
    half = stretch // 2
    tables = jnp.asarray(np.stack(rotary_tables(BLOCK)))
    qr = HD // ny
    vmem, hbm, smem = (pl.BlockSpec(memory_space=m) for m in (pltpu.VMEM, pl.ANY, pltpu.SMEM))
    dma = pltpu.SemaphoreType.DMA
    signal = pltpu.SemaphoreType.REGULAR
    scratch = [
        pltpu.VMEM((nseq, rows, width), BF16),
        pltpu.VMEM((nseq, half, width), BF16),
        pltpu.VMEM((2, width, 4 * HD), BF16),
        pltpu.VMEM(out_weight.shape, BF16),
        pltpu.VMEM((1, width), F32),
        pltpu.VMEM((1, width), F32),
        pltpu.VMEM(tables.shape, F32),
        pltpu.VMEM((2, 8, HD), F32),
        pltpu.VMEM((2, BLOCK, HD), F32),
        pltpu.VMEM((2, BLOCK, HD), F32),
        pltpu.VMEM((2, BLOCK, HD), F32),
        pltpu.VMEM((2, BLOCK, HD), F32),
        pltpu.VMEM((2, BLOCK, HD), F32),
        pltpu.VMEM((nseq, 2, half, HD), BF16),
        pltpu.VMEM((nseq, 2, half, HD), F32),
        pltpu.VMEM((nseq, 2, half, HD), F32),
        pltpu.VMEM((nseq, 2, 2, HD, HD), F32),
        pltpu.VMEM((nseq, 2, HD, HD), BF16),
        pltpu.VMEM((nseq, 2 * ny, qr, HD), BF16),
        pltpu.VMEM((nseq, qr, HD), BF16),
        pltpu.VMEM((nseq, nz, qr, HD), BF16),
        pltpu.VMEM((nseq, 2 * ny, qr, HD), BF16),
        pltpu.VMEM((nseq, 2, HD, HD), BF16),
        pltpu.VMEM((nseq, half, 2 * HD), BF16),
        pltpu.VMEM((nseq, rows, ntp * HD), BF16),
        pltpu.VMEM((rows, width), F32),
        dma((10,)),
        dma((1,)), dma((nseq,)), dma((1,)), dma((nseq, 2)), dma((1,)), dma((4,)), dma((1,)), dma((1,)),
        dma((1,)), dma((1,)), dma((1,)), dma((nseq,)), dma((nz,)), dma((nseq, nz)), dma((1,)), dma((nseq,)),
        dma((1,)), dma((nseq,)), signal, signal,
    ]
    return pl.pallas_call(
        functools.partial(kernel, nz, ny),
        out_shape=jax.ShapeDtypeStruct(tokens.shape, BF16),
        in_specs=[hbm] * 6 + [smem] + [hbm] * 4,
        out_specs=vmem,
        scratch_shapes=scratch,
        name="retention",
        compiler_params=pltpu.CompilerParams(
            collective_id=0, has_side_effects=True, vmem_limit_bytes=60 * 1024 * 1024
        ),
    )(
        tokens, in_gain.reshape(1, -1), wq, wk, wv, wg, log_decay, norm_gain.reshape(1, -1), out_weight,
        post_gain.reshape(1, -1), tables,
    )


def solution(mesh):
    both = ("sp", "tp")
    nz = mesh.shape["sp"] // NY
    return jax.shard_map(
        functools.partial(body, nz, NY),
        mesh=mesh,
        in_specs=(
            P(None, both, None), P(), P(None, "tp"), P(None, "tp"), P(None, "tp"), P(None, "tp"), P("tp"), P("tp"),
            P(), P(),
        ),
        out_specs=P(None, both, None),
        check_vma=False,
    )
```

```python
import functools

import jax
import jax.numpy as jnp
import numpy as np
from jax import lax
from jax.experimental import pallas as pl
from jax.experimental.pallas import tpu as pltpu
from jax.sharding import PartitionSpec as P

MESH = pl.DeviceIdType.MESH
F32 = jnp.float32
BF16 = jnp.bfloat16
HD = 128
BLOCK = 128
NY = 4
RMS_EPS = 1e-06
GROUP_EPS = 1e-05
ROPE_BASE = 10000.0


def rotary_tables(blocks):
    half = HD // 2
    rate = ROPE_BASE ** (-np.arange(half, dtype=np.float64) / half)
    rate = np.concatenate([rate, rate])
    inside = np.arange(BLOCK, dtype=np.float64)[:, None] * rate
    starts = BLOCK * np.arange(blocks, dtype=np.float64)[:, None] * rate
    tables = (np.cos(inside), np.sin(inside), np.cos(starts), np.sin(starts))
    return [t.astype(np.float32) for t in tables]


def kernel(
    nz, ny, tok_hbm, gain_hbm, wq, wk, wv, wg, ld_ref, ng_hbm, ow, pg_hbm, tab_hbm, out_ref,
    raw, tok, w, oww, gain, pg, tabs, crow, ctab, stab, dmat, qsc, ksc, kbuf, vbuf, qs, acc, gs, smat, esend, ybuf,
    zsnd, zbuf, msnd, mbuf, gsend, gat, osc, lsem, xs, xr, ps, pr, wxs, wxr, wfs, wfr, cs, cr, ys, yr, zs, zr, ms, mr, as_, ar,
    ready_a, ready_b,
):
    nseq, rows, width = raw.shape
    ntp = 8
    nchip = ntp // 2
    blocks = 2
    span = blocks * BLOCK
    qr = HD // ny
    quarter = width // 4
    chunk = quarter // 4
    sp = lax.axis_index("sp")
    me = lax.axis_index("tp")
    z, y = sp // ny, sp % ny
    chip, core = me // 2, me % 2
    partner = chip * 2 + 1 - core
    half, dl = chip // 2, me % 4
    mine, theirs = chip % 2, 1 - chip % 2
    pair_same = (half * 2 + theirs) * 2 + core
    pair_other = (half * 2 + theirs) * 2 + 1 - core
    mate = (nchip - 1 - chip) * 2 + core

    def at(zz, yy):
        return (zz + nz) % nz * ny + (yy + ny) % ny

    barrier = pltpu.get_barrier_semaphore()
    near = [(at(z, y + k), me) for k in range(1, ny)] + [(at(z - 1, y), me), (at(z + 1, y), me), (sp, mate)]
    peers = [(sp, partner), (sp, pair_same), (sp, pair_other)] + near
    for dev in peers:
        pl.semaphore_signal(barrier, inc=1, device_id=dev, device_id_type=MESH)

    raw_loads = [pltpu.make_async_copy(tok_hbm.at[s], raw.at[s], lsem.at[s]) for s in range(nseq)]
    gain_load = pltpu.make_async_copy(gain_hbm, gain, lsem.at[4])
    tab_load = pltpu.make_async_copy(tab_hbm, tabs, lsem.at[5])
    ng_load = pltpu.make_async_copy(ng_hbm, crow.at[0, pl.ds(0, 1)], lsem.at[6])
    pg_load = pltpu.make_async_copy(pg_hbm, pg, lsem.at[7])
    w_loads = [pltpu.make_async_copy(w.at[0, c], w.at[0, c], lsem.at[8 + c]) for c in range(2)]
    ow_load = pltpu.make_async_copy(oww, oww, lsem.at[10])
    gain_load.start()
    for load in raw_loads:
        load.start()
    ng_load.start()
    for j, src in enumerate((wk, wv, wq, wg)):
        cols = j % 2 * HD
        pltpu.make_async_copy(src, w.at[0, j // 2, :, cols:cols + HD], lsem.at[8 + j // 2]).start()
    tab_load.start()
    pg_load.start()
    for d in range(4):
        first = half * 4 + d
        second = (nchip - 1 - first // 2) * 2 + d % 2
        for i, h in enumerate((first, second)):
            src = ow.at[pl.ds(pl.multiple_of(h * HD, HD), HD), :]
            pltpu.make_async_copy(src, oww.at[(2 * d + i) * HD:(2 * d + i + 1) * HD, :], lsem.at[10]).start()

    def remote(src, dst, send, recv, dev):
        return pltpu.make_async_remote_copy(
            src_ref=src, dst_ref=dst, send_sem=send, recv_sem=recv, device_id=dev, device_id_type=MESH
        )

    def part_of(s, d):
        return tok.at[s, pl.ds(pl.multiple_of(d * rows, rows), rows), :]

    def own_send(s):
        ref = part_of(s, dl)
        return remote(ref, ref, xs.at[0], xr.at[s], (sp, pair_same))

    def own_recv(s):
        ref = part_of(s, theirs * 2 + core)
        return remote(ref, ref, xs.at[0], xr.at[s], (sp, pair_same))

    def pass_send(s, i):
        ref = part_of(s, (mine, theirs)[i] * 2 + core)
        return remote(ref, ref, ps.at[0], pr.at[s, i], (sp, partner))

    def pass_recv(s, i):
        ref = part_of(s, (mine, theirs)[i] * 2 + 1 - core)
        return remote(ref, ref, ps.at[0], pr.at[s, i], (sp, partner))

    my_quarter = (y % 2) * 2 + z % 2

    def w_rows(k, j):
        at_ = pl.multiple_of(my_quarter * quarter + j % 4 * chunk, chunk)
        return w.at[k, j // 4, pl.ds(at_, chunk), :]

    def w_send(j):
        return remote(w_rows(0, j), w_rows(1, j), wxs.at[0], wxr.at[j], (sp, mate))

    def w_recv(j):
        return remote(w_rows(1, j), w_rows(1, j), wxs.at[0], wxr.at[j], (sp, mate))

    def w_forward(j):
        w_recv(j).wait_recv()
        yy, zz = y + (1, -1)[j % 2], z + (1, -1)[j // 2 % 2]
        for dev in (at(zz, yy), at(z, yy), at(zz, y)):
            remote(w_rows(1, j), w_rows(1, j), wfs.at[0], wfr.at[j // 4], (dev, me)).start()

    def w_rest(c):
        ref = w.at[1, c, 0:3 * quarter, :]
        return remote(ref, ref, wfs.at[0], wfr.at[c], (sp, partner))

    def c_send():
        return remote(crow.at[0], crow.at[1], cs.at[0], cr.at[0], (sp, mate))

    def ycopy(s, k, to):
        src = esend.at[s, k, pl.ds(pl.multiple_of(to * qr, qr), qr), :]
        return remote(src, ybuf.at[s, y * 2 + half], ys.at[0], yr.at[s], (at(z, to), (me, mate)[k]))

    def zcopy(s, to):
        return remote(zsnd.at[s], zbuf.at[s, z], zs.at[to], zr.at[s, z], (to * ny + y, me))

    def zrecv(s, frm):
        ref = zbuf.at[s, frm]
        return remote(ref, ref, zs.at[frm], zr.at[s, frm], (frm * ny + y, me))

    def mcopy(s, k, to):
        src = msnd.at[s, to * 2 + (half, 1 - half)[k]]
        dst = mbuf.at[s, k, pl.ds(pl.multiple_of(y * qr, qr), qr), :]
        return remote(src, dst, ms.at[0], mr.at[s], (at(z, to), (me, mate)[k]))

    def acopy(s, to):
        src = gsend.at[s, pl.ds(pl.multiple_of(to * rows, rows), rows), :]
        dst = gat.at[s, :, pl.ds(pl.multiple_of(dl * 2 * HD, 2 * HD), 2 * HD)]
        return remote(src, dst, as_.at[0], ar.at[s], (sp, half * 4 + to))

    def whole(ref, send, recv):
        return remote(ref, ref, send, recv, (sp, partner))

    part = 16

    def norm_own(s):
        raw_loads[s].wait()

        @pl.loop(0, rows // part)
        def _(c):
            v = raw[s, pl.ds(pl.multiple_of(c * part, part), part), :].astype(F32)
            scale = lax.rsqrt(jnp.mean(v * v, axis=-1, keepdims=True) + RMS_EPS)
            at_ = pl.multiple_of(dl * rows + c * part, part)
            tok[s, pl.ds(at_, part), :] = (v * scale * gain[...]).astype(BF16)

    gain_load.wait()
    norm_own(0)
    ng_load.wait()
    crow[0, pl.ds(1, 7), :] = jnp.full((7, HD), ld_ref[0], F32)

    pl.semaphore_wait(barrier, len(peers))
    own_send(0).start()
    pass_send(0, 0).start()
    for dev in near:
        pl.semaphore_signal(ready_a, inc=1, device_id=dev, device_id_type=MESH)
    for c in range(2):
        w_loads[c].wait()
        for j in range(4 * c, 4 * c + 4):
            w_send(j).start()
    c_send().start()
    for s in range(1, nseq):
        norm_own(s)
        if s == 1:
            own_send(s).start()
        pass_send(s, 0).start()

    i_col = lax.broadcasted_iota(jnp.int32, (BLOCK, HD), 0).astype(F32)
    i_row = lax.broadcasted_iota(jnp.int32, (BLOCK, HD), 1).astype(F32)

    def decay(k, count):
        return jnp.exp(crow[k, pl.ds(1, 1), :] * count)

    def head_tables(k):
        ld = crow[k, pl.ds(1, 1), :]
        dist = i_col - i_row
        dmat[k] = jnp.where(dist >= 0, jnp.exp(ld * jnp.maximum(dist, 0.0)), 0.0)
        qsc[k] = jnp.exp(ld * (i_col + 1.0))
        ksc[k] = jnp.exp(ld * (BLOCK - 1.0 - i_col))

    head_tables(0)
    tab_load.wait()
    sign = jnp.where(i_row < HD // 2, -1.0, 1.0)
    for b in range(blocks):
        start = sp * nchip + half * blocks + b
        cb = tabs[2, pl.ds(start, 1), :]
        sb = tabs[3, pl.ds(start, 1), :]
        ctab[b] = tabs[0] * cb - tabs[1] * sb
        stab[b] = (tabs[1] * cb + tabs[0] * sb) * sign

    def rotate(u, b):
        return u * ctab[b] + pltpu.roll(u, HD // 2, 1) * stab[b]

    def tokens_of(s, b0, nb):
        return tok[s, pl.ds(pl.multiple_of(b0 * BLOCK, BLOCK), nb * BLOCK), :]

    def block_at(b):
        return pl.ds(pl.multiple_of(b * BLOCK, BLOCK), BLOCK)

    def keys(s, k, b0, nb):
        proj = jnp.dot(tokens_of(s, b0, nb), w[k, 0], preferred_element_type=F32).astype(BF16)
        for i in range(nb):
            b = b0 + i
            here = block_at(b)
            p = proj[i * BLOCK:(i + 1) * BLOCK]
            kk = (rotate(p[:, :HD].astype(F32), b) * HD ** -0.5).astype(BF16)
            v = p[:, HD:]
            kbuf[s, k, here, :] = kk
            vbuf[s, k, here, :] = v
            ks = (kk.astype(F32) * ksc[k]).astype(BF16)
            smat[s, k, b] = lax.dot_general(ks, v, (((0,), (0,)), ((), ())), preferred_element_type=F32)

    def queries(s, k, b0, nb):
        proj = jnp.dot(tokens_of(s, b0, nb), w[k, 1], preferred_element_type=F32).astype(BF16)
        for i in range(nb):
            b = b0 + i
            here = block_at(b)
            p = proj[i * BLOCK:(i + 1) * BLOCK]
            q = rotate(p[:, :HD].astype(F32), b).astype(BF16)
            g = p[:, HD:].astype(F32)
            scores = lax.dot_general(q, kbuf[s, k, here, :], (((1,), (1,)), ((), ())), preferred_element_type=F32)
            weights = (scores * dmat[k]).astype(BF16)
            acc[s, k, here, :] = jnp.dot(weights, vbuf[s, k, here, :], preferred_element_type=F32)
            qs[s, k, here, :] = (q.astype(F32) * qsc[k]).astype(BF16)
            gs[s, k, here, :] = crow[k, pl.ds(0, 1), :] * (g * jax.nn.sigmoid(g))

    def state_out(s):
        for k in range(2):
            esend[s, k] = (smat[s, k, 0] * decay(k, float(BLOCK)) + smat[s, k, 1]).astype(BF16)
        ybuf[s, y * 2 + half] = esend[s, 0, pl.ds(pl.multiple_of(y * qr, qr), qr), :]
        for to in range(ny):
            ycopy(s, 1, (y + to) % ny).start()
            if to:
                ycopy(s, 0, (y + to) % ny).start()

    def state_row(s):
        whole(ybuf.at[s, pl.ds(0, 2 * ny - 1)], ys.at[0], yr.at[s]).wait_recv()
        step = decay(0, float(span))
        total = ybuf[s, 0].astype(F32)
        for k in range(1, 2 * ny):
            total = total * step + ybuf[s, k].astype(F32)
        zsnd[s] = total.astype(BF16)

        @pl.loop(z + 1, nz)
        def _(to):
            zcopy(s, to).start()

    def state_back(s):
        step = decay(0, float(span))
        row_step = decay(0, float(span * 2 * ny))

        def add(frm, total):
            zrecv(s, frm).wait_recv()
            return total * row_step + zbuf[s, frm].astype(F32)

        carried = lax.fori_loop(0, z, add, jnp.zeros((qr, HD), F32))
        for k in range(2 * ny):
            msnd[s, k] = carried.astype(BF16)
            if k < 2 * ny - 1:
                carried = carried * step + ybuf[s, k].astype(F32)
        mbuf[s, 0, pl.ds(pl.multiple_of(y * qr, qr), qr), :] = msnd[s, y * 2 + half]
        for to in range(ny):
            mcopy(s, 1, (y + to) % ny).start()
            if to:
                mcopy(s, 0, (y + to) % ny).start()

    def read_out(s):
        whole(ybuf.at[s, pl.ds(0, 2 * ny - 1)], ms.at[0], mr.at[s]).wait_recv()
        for k in range(2):
            memory = mbuf[s, k]
            for b in range(blocks):
                here = pl.ds(b * BLOCK, BLOCK)
                if b:
                    memory = (smat[s, k, 0] + memory.astype(F32) * decay(k, float(BLOCK))).astype(BF16)
                kept = acc[s, k, here, :] + jnp.dot(qs[s, k, here, :], memory, preferred_element_type=F32)
                kept = kept - jnp.mean(kept, axis=-1, keepdims=True)
                spread = jnp.mean(kept * kept, axis=-1, keepdims=True)
                kept = kept * lax.rsqrt(spread + GROUP_EPS) * gs[s, k, here, :]
                gsend[s, here, k * HD:(k + 1) * HD] = kept.astype(BF16)
        for k in range(1, 4):
            acopy(s, (dl + k) % 4).start()
        own = gsend[s, pl.ds(pl.multiple_of(dl * rows, rows), rows), :]
        gat[s, :, pl.ds(pl.multiple_of(dl * 2 * HD, 2 * HD), 2 * HD)] = own

    def mix(s):
        whole(gat.at[s, :, 0:6 * HD], as_.at[0], ar.at[s]).wait_recv()
        osc[...] = jnp.dot(gat[s], oww[...], preferred_element_type=F32)

        @pl.loop(0, rows // part)
        def _(c):
            here = pl.ds(pl.multiple_of(c * part, part), part)
            v = osc[here, :]
            scale = lax.rsqrt(jnp.mean(v * v, axis=-1, keepdims=True) + RMS_EPS)
            out_ref[s, here, :] = (v * scale * pg[...]).astype(BF16)

    @pl.loop(0, nseq)
    def _(s):
        pass_recv(s, 0).wait_recv()
        keys(s, 0, mine, 1)
        queries(s, 0, mine, 1)

    pl.semaphore_wait(ready_a, len(near))
    for dev in ((at(z - 2, y), me), (at(z + 2, y), me)):
        pl.semaphore_signal(ready_b, inc=1, device_id=dev, device_id_type=MESH)

    def take_pair(s):
        own_recv(s).wait_recv()
        pass_send(s, 1).start()
        if s + 2 < nseq:
            own_send(s + 2).start()

    for j in range(3):
        w_forward(j)
    take_pair(0)
    w_forward(3)
    pass_recv(0, 1).wait_recv()
    keys(0, 0, theirs, 1)
    w_forward(4)
    queries(0, 0, theirs, 1)
    w_forward(5)
    whole(crow.at[1], cs.at[0], cr.at[0]).wait_recv()
    head_tables(1)
    w_rest(0).wait_recv()
    w_forward(6)
    keys(0, 1, 0, 2)
    state_out(0)
    take_pair(1)
    w_forward(7)
    pass_recv(1, 1).wait_recv()
    keys(1, 0, theirs, 1)
    keys(1, 1, 0, 2)
    state_out(1)
    keys(2, 1, mine, 1)
    keys(3, 1, mine, 1)
    queries(1, 0, theirs, 1)
    take_pair(2)
    w_rest(1).wait_recv()
    queries(0, 1, 0, 2)
    pass_recv(2, 1).wait_recv()
    keys(2, 0, theirs, 1)
    keys(2, 1, theirs, 1)
    state_out(2)
    pl.semaphore_wait(ready_b, 2)
    state_row(0)
    state_row(1)
    queries(1, 1, 0, 2)
    take_pair(3)
    queries(2, 0, theirs, 1)
    pass_recv(3, 1).wait_recv()
    keys(3, 0, theirs, 1)
    keys(3, 1, theirs, 1)
    state_out(3)
    state_row(2)
    queries(2, 1, 0, 2)
    state_back(0)
    state_back(1)
    queries(3, 0, theirs, 1)
    queries(3, 1, 0, 2)
    state_row(3)
    state_back(2)
    read_out(0)
    read_out(1)
    state_back(3)
    ow_load.wait()
    pg_load.wait()
    read_out(2)
    mix(0)
    mix(1)
    read_out(3)
    mix(2)
    mix(3)

    whole(raw, xs.at[0], xr.at[0]).wait_send()
    whole(tok.at[:, 0:2 * rows, :], ps.at[0], pr.at[0, 0]).wait_send()
    whole(w.at[1, :, 0:quarter, :], wxs.at[0], wxr.at[0]).wait_send()
    whole(w.at[1, :, 0:3 * quarter, :], wfs.at[0], wfr.at[0]).wait_send()
    whole(crow.at[0], cs.at[0], cr.at[0]).wait_send()
    whole(ybuf.at[:, pl.ds(0, 2 * ny - 1)], ys.at[0], yr.at[0]).wait_send()
    whole(ybuf.at[:, pl.ds(0, 2 * ny - 1)], ms.at[0], mr.at[0]).wait_send()
    whole(gat.at[:, :, 0:6 * HD], as_.at[0], ar.at[0]).wait_send()

    @pl.loop(z + 1, nz)
    def _(to):
        whole(zsnd, zs.at[to], zr.at[0, to]).wait_send()


def body(nz, ny, tokens, in_gain, wq, wk, wv, wg, log_decay, norm_gain, out_weight, post_gain):
    nseq, rows, width = tokens.shape
    ntp = 8
    stretch = rows * ntp
    half = stretch // 2
    tables = jnp.asarray(np.stack(rotary_tables(BLOCK)))
    qr = HD // ny
    vmem, hbm, smem = (pl.BlockSpec(memory_space=m) for m in (pltpu.VMEM, pl.ANY, pltpu.SMEM))
    dma = pltpu.SemaphoreType.DMA
    signal = pltpu.SemaphoreType.REGULAR
    scratch = [
        pltpu.VMEM((nseq, rows, width), BF16),
        pltpu.VMEM((nseq, half, width), BF16),
        pltpu.VMEM((2, 2, width, 2 * HD), BF16),
        pltpu.VMEM(out_weight.shape, BF16),
        pltpu.VMEM((1, width), F32),
        pltpu.VMEM((1, width), F32),
        pltpu.VMEM(tables.shape, F32),
        pltpu.VMEM((2, 8, HD), F32),
        pltpu.VMEM((2, BLOCK, HD), F32),
        pltpu.VMEM((2, BLOCK, HD), F32),
        pltpu.VMEM((2, BLOCK, HD), F32),
        pltpu.VMEM((2, BLOCK, HD), F32),
        pltpu.VMEM((2, BLOCK, HD), F32),
        pltpu.VMEM((nseq, 2, half, HD), BF16),
        pltpu.VMEM((nseq, 2, half, HD), BF16),
        pltpu.VMEM((nseq, 2, half, HD), BF16),
        pltpu.VMEM((nseq, 2, half, HD), F32),
        pltpu.VMEM((nseq, 2, half, HD), F32),
        pltpu.VMEM((nseq, 2, 2, HD, HD), F32),
        pltpu.VMEM((nseq, 2, HD, HD), BF16),
        pltpu.VMEM((nseq, 2 * ny, qr, HD), BF16),
        pltpu.VMEM((nseq, qr, HD), BF16),
        pltpu.VMEM((nseq, nz, qr, HD), BF16),
        pltpu.VMEM((nseq, 2 * ny, qr, HD), BF16),
        pltpu.VMEM((nseq, 2, HD, HD), BF16),
        pltpu.VMEM((nseq, half, 2 * HD), BF16),
        pltpu.VMEM((nseq, rows, ntp * HD), BF16),
        pltpu.VMEM((rows, width), F32),
        dma((11,)),
        dma((1,)), dma((nseq,)), dma((1,)), dma((nseq, 2)), dma((1,)), dma((8,)), dma((1,)), dma((2,)),
        dma((1,)), dma((1,)), dma((1,)), dma((nseq,)), dma((nz,)), dma((nseq, nz)), dma((1,)), dma((nseq,)),
        dma((1,)), dma((nseq,)), signal, signal,
    ]
    return pl.pallas_call(
        functools.partial(kernel, nz, ny),
        out_shape=jax.ShapeDtypeStruct(tokens.shape, BF16),
        in_specs=[hbm] * 6 + [smem] + [hbm] * 4,
        out_specs=vmem,
        scratch_shapes=scratch,
        name="retention",
        compiler_params=pltpu.CompilerParams(
            collective_id=0, has_side_effects=True, vmem_limit_bytes=60 * 1024 * 1024
        ),
    )(
        tokens, in_gain.reshape(1, -1), wq, wk, wv, wg, log_decay, norm_gain.reshape(1, -1), out_weight,
        post_gain.reshape(1, -1), tables,
    )


def solution(mesh):
    both = ("sp", "tp")
    nz = mesh.shape["sp"] // NY
    return jax.shard_map(
        functools.partial(body, nz, NY),
        mesh=mesh,
        in_specs=(
            P(None, both, None), P(), P(None, "tp"), P(None, "tp"), P(None, "tp"), P(None, "tp"), P("tp"), P("tp"),
            P(), P(),
        ),
        out_specs=P(None, both, None),
        check_vma=False,
    )
```

```python
import functools

import jax
import jax.numpy as jnp
import numpy as np
from jax import lax
from jax.experimental import pallas as pl
from jax.experimental.pallas import tpu as pltpu
from jax.sharding import PartitionSpec as P

MESH = pl.DeviceIdType.MESH
F32 = jnp.float32
BF16 = jnp.bfloat16
HD = 128
BLOCK = 128
NY = 4
RMS_EPS = 1e-06
GROUP_EPS = 1e-05
ROPE_BASE = 10000.0


def rotary_tables(blocks):
    half = HD // 2
    rate = ROPE_BASE ** (-np.arange(half, dtype=np.float64) / half)
    rate = np.concatenate([rate, rate])
    inside = np.arange(BLOCK, dtype=np.float64)[:, None] * rate
    starts = BLOCK * np.arange(blocks, dtype=np.float64)[:, None] * rate
    tables = (np.cos(inside), np.sin(inside), np.cos(starts), np.sin(starts))
    return [t.astype(np.float32) for t in tables]


def row_scale(read, width):
    total = jnp.square(read(0))
    for c in range(1, width // HD):
        total += jnp.square(read(c))
    return lax.rsqrt(jnp.sum(total, axis=-1, keepdims=True) * (1.0 / width) + RMS_EPS)


def kernel(
    nz, ny, tok_hbm, gain_hbm, wq, wk, wv, wg, ld_ref, ng_hbm, ow, tab_hbm, gat, oww,
    raw, tok, w, gain, tabs, crow, ctab, stab, dmat, qsc, ksc, kbuf, vbuf, qs, acc, gs, smat, esend, ybuf,
    zsnd, zbuf, msnd, mbuf, gsend, lsem, xs, xr, ps, pr, wxs, wxr, wfs, wfr, cs, cr, ys, yr, zs, zr, ms, mr, as_, ar,
    ready_a, ready_b,
):
    nseq, rows, width = raw.shape
    ntp = 8
    nchip = ntp // 2
    blocks = 2
    span = blocks * BLOCK
    qr = HD // ny
    quarter = width // 4
    chunk = quarter // 4
    sp = lax.axis_index("sp")
    me = lax.axis_index("tp")
    z, y = sp // ny, sp % ny
    chip, core = me // 2, me % 2
    partner = chip * 2 + 1 - core
    half, dl = chip // 2, me % 4
    mine, theirs = chip % 2, 1 - chip % 2
    pair_same = (half * 2 + theirs) * 2 + core
    pair_other = (half * 2 + theirs) * 2 + 1 - core
    mate = (nchip - 1 - chip) * 2 + core

    def at(zz, yy):
        return (zz + nz) % nz * ny + (yy + ny) % ny

    barrier = pltpu.get_barrier_semaphore()
    near = [(at(z, y + k), me) for k in range(1, ny)] + [(at(z - 1, y), me), (at(z + 1, y), me), (sp, mate)]
    peers = [(sp, partner), (sp, pair_same), (sp, pair_other)] + near
    for dev in peers:
        pl.semaphore_signal(barrier, inc=1, device_id=dev, device_id_type=MESH)

    raw_loads = [pltpu.make_async_copy(tok_hbm.at[s], raw.at[s], lsem.at[s]) for s in range(nseq)]
    gain_load = pltpu.make_async_copy(gain_hbm, gain, lsem.at[4])
    tab_load = pltpu.make_async_copy(tab_hbm, tabs, lsem.at[5])
    ng_load = pltpu.make_async_copy(ng_hbm, crow.at[0, pl.ds(0, 1)], lsem.at[6])
    w_loads = [pltpu.make_async_copy(w.at[0, c], w.at[0, c], lsem.at[8 + c]) for c in range(2)]
    ow_load = pltpu.make_async_copy(oww, oww, lsem.at[10])
    gain_load.start()
    for load in raw_loads:
        load.start()
    ng_load.start()
    for j, src in enumerate((wk, wv, wq, wg)):
        cols = j % 2 * HD
        pltpu.make_async_copy(src, w.at[0, j // 2, :, cols:cols + HD], lsem.at[8 + j // 2]).start()
    tab_load.start()
    for d in range(4):
        first = half * 4 + d
        second = (nchip - 1 - first // 2) * 2 + d % 2
        for i, h in enumerate((first, second)):
            src = ow.at[pl.ds(pl.multiple_of(h * HD, HD), HD), :]
            pltpu.make_async_copy(src, oww.at[(2 * d + i) * HD:(2 * d + i + 1) * HD, :], lsem.at[10]).start()

    def remote(src, dst, send, recv, dev):
        return pltpu.make_async_remote_copy(
            src_ref=src, dst_ref=dst, send_sem=send, recv_sem=recv, device_id=dev, device_id_type=MESH
        )

    def part_of(s, d):
        return tok.at[s, pl.ds(pl.multiple_of(d * rows, rows), rows), :]

    def own_send(s):
        ref = part_of(s, dl)
        return remote(ref, ref, xs.at[0], xr.at[s], (sp, pair_same))

    def own_recv(s):
        ref = part_of(s, theirs * 2 + core)
        return remote(ref, ref, xs.at[0], xr.at[s], (sp, pair_same))

    def pass_send(s, i):
        ref = part_of(s, (mine, theirs)[i] * 2 + core)
        return remote(ref, ref, ps.at[0], pr.at[s, i], (sp, partner))

    def pass_recv(s, i):
        ref = part_of(s, (mine, theirs)[i] * 2 + 1 - core)
        return remote(ref, ref, ps.at[0], pr.at[s, i], (sp, partner))

    my_quarter = (y % 2) * 2 + z % 2

    def w_rows(k, j):
        at_ = pl.multiple_of(my_quarter * quarter + j % 4 * chunk, chunk)
        return w.at[k, j // 4, pl.ds(at_, chunk), :]

    def w_send(j):
        return remote(w_rows(0, j), w_rows(1, j), wxs.at[0], wxr.at[j], (sp, mate))

    def w_recv(j):
        return remote(w_rows(1, j), w_rows(1, j), wxs.at[0], wxr.at[j], (sp, mate))

    def w_forward(j):
        w_recv(j).wait_recv()
        yy, zz = y + (1, -1)[j % 2], z + (1, -1)[j // 2 % 2]
        for dev in (at(zz, yy), at(z, yy), at(zz, y)):
            remote(w_rows(1, j), w_rows(1, j), wfs.at[0], wfr.at[j // 4], (dev, me)).start()

    def w_rest(c):
        ref = w.at[1, c, 0:3 * quarter, :]
        return remote(ref, ref, wfs.at[0], wfr.at[c], (sp, partner))

    def c_send():
        return remote(crow.at[0], crow.at[1], cs.at[0], cr.at[0], (sp, mate))

    def ycopy(s, k, to):
        src = esend.at[s, k, pl.ds(pl.multiple_of(to * qr, qr), qr), :]
        return remote(src, ybuf.at[s, y * 2 + half], ys.at[0], yr.at[s], (at(z, to), (me, mate)[k]))

    def zcopy(s, to):
        return remote(zsnd.at[s], zbuf.at[s, z], zs.at[to], zr.at[s, z], (to * ny + y, me))

    def zrecv(s, frm):
        ref = zbuf.at[s, frm]
        return remote(ref, ref, zs.at[frm], zr.at[s, frm], (frm * ny + y, me))

    def mcopy(s, k, to):
        src = msnd.at[s, to * 2 + (half, 1 - half)[k]]
        dst = mbuf.at[s, k, pl.ds(pl.multiple_of(y * qr, qr), qr), :]
        return remote(src, dst, ms.at[0], mr.at[s], (at(z, to), (me, mate)[k]))

    def acopy(s, to):
        src = gsend.at[s, pl.ds(pl.multiple_of(to * rows, rows), rows), :]
        dst = gat.at[s, :, pl.ds(pl.multiple_of(dl * 2 * HD, 2 * HD), 2 * HD)]
        return remote(src, dst, as_.at[0], ar.at[0], (sp, half * 4 + to))

    def whole(ref, send, recv):
        return remote(ref, ref, send, recv, (sp, partner))

    def norm_own(s):
        raw_loads[s].wait()
        scale = row_scale(lambda c: raw[s, :, c * HD:(c + 1) * HD].astype(F32), width)
        here = pl.ds(pl.multiple_of(dl * rows, rows), rows)
        for c in range(width // HD):
            cols = slice(c * HD, (c + 1) * HD)
            v = raw[s, :, cols].astype(F32)
            tok[s, here, cols] = (v * scale * gain[:, cols]).astype(BF16)

    gain_load.wait()
    norm_own(0)
    ng_load.wait()
    crow[0, pl.ds(1, 7), :] = jnp.full((7, HD), ld_ref[0], F32)

    pl.semaphore_wait(barrier, len(peers))
    own_send(0).start()
    pass_send(0, 0).start()
    for dev in near:
        pl.semaphore_signal(ready_a, inc=1, device_id=dev, device_id_type=MESH)
    c_send().start()
    for c in range(2):
        w_loads[c].wait()
        for j in range(4 * c, 4 * c + 4):
            w_send(j).start()
    for s in range(1, nseq):
        norm_own(s)
        if s == 1:
            own_send(s).start()
        pass_send(s, 0).start()

    i_col = lax.broadcasted_iota(jnp.int32, (BLOCK, HD), 0).astype(F32)
    i_row = lax.broadcasted_iota(jnp.int32, (BLOCK, HD), 1).astype(F32)

    def decay(k, count):
        return jnp.exp(crow[k, pl.ds(1, 1), :] * count)

    def head_tables(k):
        ld = crow[k, pl.ds(1, 1), :]
        dist = i_col - i_row
        dmat[k] = jnp.where(dist >= 0, jnp.exp(ld * jnp.maximum(dist, 0.0)), 0.0)
        qsc[k] = jnp.exp(ld * (i_col + 1.0))
        ksc[k] = jnp.exp(ld * (BLOCK - 1.0 - i_col))

    head_tables(0)
    tab_load.wait()
    sign = jnp.where(i_row < HD // 2, -1.0, 1.0)
    for b in range(blocks):
        start = sp * nchip + half * blocks + b
        cb = tabs[2, pl.ds(start, 1), :]
        sb = tabs[3, pl.ds(start, 1), :]
        ctab[b] = tabs[0] * cb - tabs[1] * sb
        stab[b] = (tabs[1] * cb + tabs[0] * sb) * sign

    def rotate(u, b):
        return u * ctab[b] + pltpu.roll(u, HD // 2, 1) * stab[b]

    def tokens_of(s, b0, nb):
        return tok[s, pl.ds(pl.multiple_of(b0 * BLOCK, BLOCK), nb * BLOCK), :]

    def block_at(b):
        return pl.ds(pl.multiple_of(b * BLOCK, BLOCK), BLOCK)

    def keys(s, k, b0, nb):
        proj = jnp.dot(tokens_of(s, b0, nb), w[k, 0], preferred_element_type=F32).astype(BF16)
        for i in range(nb):
            b = b0 + i
            here = block_at(b)
            p = proj[i * BLOCK:(i + 1) * BLOCK]
            kk = (rotate(p[:, :HD].astype(F32), b) * HD ** -0.5).astype(BF16)
            v = p[:, HD:]
            kbuf[s, k, here, :] = kk
            vbuf[s, k, here, :] = v
            ks = (kk.astype(F32) * ksc[k]).astype(BF16)
            smat[s, k, b] = lax.dot_general(ks, v, (((0,), (0,)), ((), ())), preferred_element_type=F32)

    def queries(s, k, b0, nb):
        proj = jnp.dot(tokens_of(s, b0, nb), w[k, 1], preferred_element_type=F32).astype(BF16)
        for i in range(nb):
            b = b0 + i
            here = block_at(b)
            p = proj[i * BLOCK:(i + 1) * BLOCK]
            q = rotate(p[:, :HD].astype(F32), b).astype(BF16)
            g = p[:, HD:].astype(F32)
            scores = lax.dot_general(q, kbuf[s, k, here, :], (((1,), (1,)), ((), ())), preferred_element_type=F32)
            weights = (scores * dmat[k]).astype(BF16)
            acc[s, k, here, :] = jnp.dot(weights, vbuf[s, k, here, :], preferred_element_type=F32)
            qs[s, k, here, :] = (q.astype(F32) * qsc[k]).astype(BF16)
            gs[s, k, here, :] = crow[k, pl.ds(0, 1), :] * (g * jax.nn.sigmoid(g))

    def state_out(s):
        for k in range(2):
            esend[s, k] = (smat[s, k, 0] * decay(k, float(BLOCK)) + smat[s, k, 1]).astype(BF16)
        ybuf[s, y * 2 + half] = esend[s, 0, pl.ds(pl.multiple_of(y * qr, qr), qr), :]
        for to in range(ny):
            ycopy(s, 1, (y + to) % ny).start()
            if to:
                ycopy(s, 0, (y + to) % ny).start()

    def state_row(s):
        whole(ybuf.at[s, pl.ds(0, 2 * ny - 1)], ys.at[0], yr.at[s]).wait_recv()
        step = decay(0, float(span))
        total = ybuf[s, 0].astype(F32)
        for k in range(1, 2 * ny):
            total = total * step + ybuf[s, k].astype(F32)
        zsnd[s] = total.astype(BF16)

        @pl.loop(z + 1, nz)
        def _(to):
            zcopy(s, to).start()

    def state_back(s):
        step = decay(0, float(span))
        row_step = decay(0, float(span * 2 * ny))

        def add(frm, total):
            zrecv(s, frm).wait_recv()
            return total * row_step + zbuf[s, frm].astype(F32)

        carried = lax.fori_loop(0, z, add, jnp.zeros((qr, HD), F32))
        for k in range(2 * ny):
            msnd[s, k] = carried.astype(BF16)
            if k < 2 * ny - 1:
                carried = carried * step + ybuf[s, k].astype(F32)
        mbuf[s, 0, pl.ds(pl.multiple_of(y * qr, qr), qr), :] = msnd[s, y * 2 + half]
        for to in range(ny):
            mcopy(s, 1, (y + to) % ny).start()
            if to:
                mcopy(s, 0, (y + to) % ny).start()

    def read_out(s):
        whole(ybuf.at[s, pl.ds(0, 2 * ny - 1)], ms.at[0], mr.at[s]).wait_recv()
        for k in range(2):
            memory = mbuf[s, k]
            for b in range(blocks):
                here = pl.ds(b * BLOCK, BLOCK)
                if b:
                    memory = (smat[s, k, 0] + memory.astype(F32) * decay(k, float(BLOCK))).astype(BF16)
                kept = acc[s, k, here, :] + jnp.dot(qs[s, k, here, :], memory, preferred_element_type=F32)
                kept = kept - jnp.mean(kept, axis=-1, keepdims=True)
                spread = jnp.mean(kept * kept, axis=-1, keepdims=True)
                kept = kept * lax.rsqrt(spread + GROUP_EPS) * gs[s, k, here, :]
                gsend[s, here, k * HD:(k + 1) * HD] = kept.astype(BF16)
        for k in range(1, 4):
            acopy(s, (dl + k) % 4).start()
        own = gsend[s, pl.ds(pl.multiple_of(dl * rows, rows), rows), :]
        gat[s, :, pl.ds(pl.multiple_of(dl * 2 * HD, 2 * HD), 2 * HD)] = own

    @pl.loop(0, nseq)
    def _(s):
        pass_recv(s, 0).wait_recv()
        keys(s, 0, mine, 1)
        queries(s, 0, mine, 1)

    pl.semaphore_wait(ready_a, len(near))
    for dev in ((at(z - 2, y), me), (at(z + 2, y), me)):
        pl.semaphore_signal(ready_b, inc=1, device_id=dev, device_id_type=MESH)

    def take_pair(s):
        own_recv(s).wait_recv()
        pass_send(s, 1).start()

    w_forward(0)
    own_send(2).start()
    w_forward(1)
    w_forward(2)
    take_pair(0)
    own_send(3).start()
    w_forward(3)
    pass_recv(0, 1).wait_recv()
    keys(0, 0, theirs, 1)
    w_forward(4)
    queries(0, 0, theirs, 1)
    w_forward(5)
    whole(crow.at[1], cs.at[0], cr.at[0]).wait_recv()
    head_tables(1)
    w_rest(0).wait_recv()
    w_forward(6)
    keys(0, 1, 0, 2)
    state_out(0)
    take_pair(1)
    w_forward(7)
    pass_recv(1, 1).wait_recv()
    keys(1, 0, theirs, 1)
    keys(1, 1, 0, 2)
    state_out(1)
    keys(2, 1, mine, 1)
    keys(3, 1, mine, 1)
    queries(1, 0, theirs, 1)
    take_pair(2)
    pass_recv(2, 1).wait_recv()
    keys(2, 0, theirs, 1)
    keys(2, 1, theirs, 1)
    state_out(2)
    pl.semaphore_wait(ready_b, 2)
    state_row(0)
    state_row(1)
    w_rest(1).wait_recv()
    queries(0, 1, 0, 2)
    take_pair(3)
    queries(1, 1, 0, 2)
    pass_recv(3, 1).wait_recv()
    keys(3, 0, theirs, 1)
    keys(3, 1, theirs, 1)
    state_out(3)
    queries(2, 0, theirs, 1)
    queries(2, 1, 0, 2)
    state_row(2)
    queries(3, 0, theirs, 1)
    queries(3, 1, 0, 2)
    state_row(3)
    for s in range(nseq):
        state_back(s)
    for s in range(nseq):
        read_out(s)
    ow_load.wait()
    whole(gat.at[:, :, 0:6 * HD], as_.at[0], ar.at[0]).wait_recv()

    whole(raw, xs.at[0], xr.at[0]).wait_send()
    whole(tok.at[:, 0:2 * rows, :], ps.at[0], pr.at[0, 0]).wait_send()
    whole(w.at[1, :, 0:quarter, :], wxs.at[0], wxr.at[0]).wait_send()
    whole(w.at[1, :, 0:3 * quarter, :], wfs.at[0], wfr.at[0]).wait_send()
    whole(crow.at[0], cs.at[0], cr.at[0]).wait_send()
    whole(ybuf.at[:, pl.ds(0, 2 * ny - 1)], ys.at[0], yr.at[0]).wait_send()
    whole(ybuf.at[:, pl.ds(0, 2 * ny - 1)], ms.at[0], mr.at[0]).wait_send()
    whole(gat.at[:, :, 0:6 * HD], as_.at[0], ar.at[0]).wait_send()

    @pl.loop(z + 1, nz)
    def _(to):
        whole(zsnd, zs.at[to], zr.at[0, to]).wait_send()


def mix_kernel(gat, oww, pg, out_ref, osc):
    osc[...] = jnp.dot(gat[...], oww[...], preferred_element_type=F32)
    width = osc.shape[1]
    scale = row_scale(lambda c: osc[:, c * HD:(c + 1) * HD], width)
    for c in range(width // HD):
        cols = slice(c * HD, (c + 1) * HD)
        out_ref[:, cols] = (osc[:, cols] * scale * pg[:, cols]).astype(BF16)


def body(nz, ny, tokens, in_gain, wq, wk, wv, wg, log_decay, norm_gain, out_weight, post_gain):
    nseq, rows, width = tokens.shape
    ntp = 8
    stretch = rows * ntp
    half = stretch // 2
    tables = jnp.asarray(np.stack(rotary_tables(BLOCK)))
    qr = HD // ny
    vmem, hbm, smem = (pl.BlockSpec(memory_space=m) for m in (pltpu.VMEM, pltpu.HBM, pltpu.SMEM))
    dma = pltpu.SemaphoreType.DMA
    signal = pltpu.SemaphoreType.REGULAR
    scratch = [
        pltpu.VMEM((nseq, rows, width), BF16),
        pltpu.VMEM((nseq, half, width), BF16),
        pltpu.VMEM((2, 2, width, 2 * HD), BF16),
        pltpu.VMEM((1, width), F32),
        pltpu.VMEM(tables.shape, F32),
        pltpu.VMEM((2, 8, HD), F32),
        pltpu.VMEM((2, BLOCK, HD), F32),
        pltpu.VMEM((2, BLOCK, HD), F32),
        pltpu.VMEM((2, BLOCK, HD), F32),
        pltpu.VMEM((2, BLOCK, HD), F32),
        pltpu.VMEM((2, BLOCK, HD), F32),
        pltpu.VMEM((nseq, 2, half, HD), BF16),
        pltpu.VMEM((nseq, 2, half, HD), BF16),
        pltpu.VMEM((nseq, 2, half, HD), BF16),
        pltpu.VMEM((nseq, 2, half, HD), F32),
        pltpu.VMEM((nseq, 2, half, HD), F32),
        pltpu.VMEM((nseq, 2, 2, HD, HD), F32),
        pltpu.VMEM((nseq, 2, HD, HD), BF16),
        pltpu.VMEM((nseq, 2 * ny, qr, HD), BF16),
        pltpu.VMEM((nseq, qr, HD), BF16),
        pltpu.VMEM((nseq, nz, qr, HD), BF16),
        pltpu.VMEM((nseq, 2 * ny, qr, HD), BF16),
        pltpu.VMEM((nseq, 2, HD, HD), BF16),
        pltpu.VMEM((nseq, half, 2 * HD), BF16),
        dma((11,)),
        dma((1,)), dma((nseq,)), dma((1,)), dma((nseq, 2)), dma((1,)), dma((8,)), dma((1,)), dma((2,)),
        dma((1,)), dma((1,)), dma((1,)), dma((nseq,)), dma((nz,)), dma((nseq, nz)), dma((1,)), dma((nseq,)),
        dma((1,)), dma((1,)), signal, signal,
    ]
    gathered, weight = pl.pallas_call(
        functools.partial(kernel, nz, ny),
        out_shape=[pltpu.VMEM((nseq, rows, ntp * HD), BF16), pltpu.VMEM(out_weight.shape, BF16)],
        in_specs=[hbm] * 6 + [smem] + [hbm] * 3,
        out_specs=[vmem, vmem],
        scratch_shapes=scratch,
        name="retention",
        compiler_params=pltpu.CompilerParams(
            collective_id=0, has_side_effects=True, vmem_limit_bytes=62_300_000
        ),
    )(
        tokens, in_gain.reshape(1, -1), wq, wk, wv, wg, log_decay, norm_gain.reshape(1, -1), out_weight, tables,
    )
    every = nseq * rows
    step = every // 2
    mixed = pl.pallas_call(
        mix_kernel,
        out_shape=jax.ShapeDtypeStruct((every, width), BF16),
        grid=(every // step,),
        in_specs=[
            pl.BlockSpec((step, ntp * HD), lambda i: (i, 0)),
            pl.BlockSpec(out_weight.shape, lambda i: (0, 0)),
            pl.BlockSpec((1, width), lambda i: (0, 0)),
        ],
        out_specs=pl.BlockSpec((step, width), lambda i: (i, 0)),
        scratch_shapes=[pltpu.VMEM((step, width), F32)],
        name="mix",
        compiler_params=pltpu.CompilerParams(vmem_limit_bytes=16 * 1024 * 1024),
    )(gathered.reshape(every, ntp * HD), weight, post_gain.reshape(1, -1))
    return mixed.reshape(tokens.shape)


def solution(mesh):
    both = ("sp", "tp")
    nz = mesh.shape["sp"] // NY
    return jax.shard_map(
        functools.partial(body, nz, NY),
        mesh=mesh,
        in_specs=(
            P(None, both, None), P(), P(None, "tp"), P(None, "tp"), P(None, "tp"), P(None, "tp"), P("tp"), P("tp"),
            P(), P(),
        ),
        out_specs=P(None, both, None),
        check_vma=False,
    )
```

```python
import functools

import jax
import jax.numpy as jnp
import numpy as np
from jax import lax
from jax.experimental import pallas as pl
from jax.experimental.pallas import tpu as pltpu
from jax.sharding import PartitionSpec as P

MESH = pl.DeviceIdType.MESH
F32 = jnp.float32
BF16 = jnp.bfloat16
HD = 128
BLOCK = 128
NY = 4
VMEM_LIMIT = 62_000_000
RMS_EPS = 1e-06
GROUP_EPS = 1e-05
ROPE_BASE = 10000.0


def rotary_tables(blocks):
    half = HD // 2
    rate = ROPE_BASE ** (-np.arange(half, dtype=np.float64) / half)
    rate = np.concatenate([rate, rate])
    inside = np.arange(BLOCK, dtype=np.float64)[:, None] * rate
    starts = BLOCK * np.arange(blocks, dtype=np.float64)[:, None] * rate
    tables = (np.cos(inside), np.sin(inside), np.cos(starts), np.sin(starts))
    return [t.astype(np.float32) for t in tables]


def row_scale(read, width):
    total = jnp.square(read(0))
    for c in range(1, width // HD):
        total += jnp.square(read(c))
    return lax.rsqrt(jnp.sum(total, axis=-1, keepdims=True) * (1.0 / width) + RMS_EPS)


def scale_rows(osc, pg, out, start, count):
    width = osc.shape[1]
    here = pl.ds(start, count)
    scale = row_scale(lambda c: osc[here, c * HD:(c + 1) * HD], width)
    for c in range(width // HD):
        cols = slice(c * HD, (c + 1) * HD)
        out[here, cols] = (osc[here, cols] * scale * pg[:, cols]).astype(BF16)


def kernel(
    nz, ny, tok_hbm, gain_hbm, wq, wk, wv, wg, ld_ref, ng_hbm, ow, pg_hbm, tab_hbm,
    gat_late, oww, mixed, raw, tok, w, gain, pg, tabs, crow, ctab, stab, dmat, qsc, ksc, kbuf, vbuf, qs, acc, gs, smat, esend, ybuf,
    zsnd, zbuf, msnd, mbuf, gsend, gat_early, osc, lsem, xs, xr, ps, pr, wxs, wxr, wfs, wfr, cs, cr, ys, yr, zs, zr, ms, mr, as_, ar,
    ready_a, ready_b,
):
    nseq, rows, width = raw.shape
    ntp = 8
    nchip = ntp // 2
    blocks = 2
    span = blocks * BLOCK
    qr = HD // ny
    quarter = width // 4
    chunk = quarter // 4
    sp = lax.axis_index("sp")
    me = lax.axis_index("tp")
    z, y = sp // ny, sp % ny
    chip, core = me // 2, me % 2
    partner = chip * 2 + 1 - core
    half, dl = chip // 2, me % 4
    mine, theirs = chip % 2, 1 - chip % 2
    pair_same = (half * 2 + theirs) * 2 + core
    pair_other = (half * 2 + theirs) * 2 + 1 - core
    mate = (nchip - 1 - chip) * 2 + core
    owners = (chip * 2 + 1, (nchip - 1 - chip) * 2 + 1)

    def at(zz, yy):
        return (zz + nz) % nz * ny + (yy + ny) % ny

    barrier = pltpu.get_barrier_semaphore()
    near = [(at(z, y + k), me) for k in range(1, ny)] + [(at(z - 1, y), me), (at(z + 1, y), me), (sp, mate)]
    near = near + [(sp, partner)]
    peers = [(sp, pair_same), (sp, pair_other)] + near
    for dev in peers:
        pl.semaphore_signal(barrier, inc=1, device_id=dev, device_id_type=MESH)

    raw_loads = [pltpu.make_async_copy(tok_hbm.at[s], raw.at[s], lsem.at[s]) for s in range(nseq)]
    gain_load = pltpu.make_async_copy(gain_hbm, gain, lsem.at[4])
    tab_load = pltpu.make_async_copy(tab_hbm, tabs, lsem.at[5])
    pg_load = pltpu.make_async_copy(pg_hbm, pg, lsem.at[7])
    ng_load = pltpu.make_async_copy(ng_hbm, crow.at[0, pl.ds(0, 1)], lsem.at[6])
    w_loads = [pltpu.make_async_copy(w.at[0, c], w.at[0, c], lsem.at[8 + c]) for c in range(2)]
    ow_load = pltpu.make_async_copy(oww, oww, lsem.at[10])
    raw_loads[0].start()
    gain_load.start()
    ng_load.start()
    for load in raw_loads[1:]:
        load.start()
    for j, src in enumerate((wk, wv, wq, wg)):
        cols = j % 2 * HD
        pltpu.make_async_copy(src, w.at[0, j // 2, :, cols:cols + HD], lsem.at[8 + j // 2]).start()
    tab_load.start()
    pg_load.start()
    for d in range(4):
        first = half * 4 + d
        second = (nchip - 1 - first // 2) * 2 + d % 2
        for i, h in enumerate((first, second)):
            src = ow.at[pl.ds(pl.multiple_of(h * HD, HD), HD), :]
            pltpu.make_async_copy(src, oww.at[(2 * d + i) * HD:(2 * d + i + 1) * HD, :], lsem.at[10]).start()

    def remote(src, dst, send, recv, dev):
        return pltpu.make_async_remote_copy(
            src_ref=src, dst_ref=dst, send_sem=send, recv_sem=recv, device_id=dev, device_id_type=MESH
        )

    def part_of(s, d):
        return tok.at[s, pl.ds(pl.multiple_of(d * rows, rows), rows), :]

    def own_send(s):
        ref = part_of(s, dl)
        return remote(ref, ref, xs.at[0], xr.at[s], (sp, pair_same))

    def own_recv(s):
        ref = part_of(s, theirs * 2 + core)
        return remote(ref, ref, xs.at[0], xr.at[s], (sp, pair_same))

    def pass_send(s, i):
        ref = part_of(s, (mine, theirs)[i] * 2 + core)
        return remote(ref, ref, ps.at[0], pr.at[s, i], (sp, partner))

    def pass_recv(s, i):
        ref = part_of(s, (mine, theirs)[i] * 2 + 1 - core)
        return remote(ref, ref, ps.at[0], pr.at[s, i], (sp, partner))

    my_quarter = (y % 2) * 2 + z % 2

    def w_rows(k, j):
        at_ = pl.multiple_of(my_quarter * quarter + j % 4 * chunk, chunk)
        return w.at[k, j // 4, pl.ds(at_, chunk), :]

    def w_send(j):
        return remote(w_rows(0, j), w_rows(1, j), wxs.at[0], wxr.at[j], (sp, mate))

    def w_recv(j):
        return remote(w_rows(1, j), w_rows(1, j), wxs.at[0], wxr.at[j], (sp, mate))

    def w_forward(j):
        w_recv(j).wait_recv()
        yy, zz = y + (1, -1)[j % 2], z + (1, -1)[j // 2 % 2]
        for dev in (at(zz, yy), at(z, yy), at(zz, y)):
            remote(w_rows(1, j), w_rows(1, j), wfs.at[0], wfr.at[j // 4], (dev, me)).start()

    def w_rest(c):
        ref = w.at[1, c, 0:3 * quarter, :]
        return remote(ref, ref, wfs.at[0], wfr.at[c], (sp, partner))

    def c_send(i):
        return remote(crow.at[0], crow.at[1 + i], cs.at[0], cr.at[i], (sp, (mate, partner)[i]))

    def ycopy(s, k, to):
        src = esend.at[s, k, pl.ds(pl.multiple_of(to * qr, qr), qr), :]
        dst = ybuf.at[s, core * 2 * ny + y * 2 + half]
        return remote(src, dst, ys.at[0], yr.at[s], (at(z, to), owners[k]))

    def zcopy(s, to):
        return remote(zsnd.at[s], zbuf.at[s, z], zs.at[to], zr.at[s, z], (to * ny + y, me))

    def zrecv(s, frm):
        ref = zbuf.at[s, frm]
        return remote(ref, ref, zs.at[frm], zr.at[s, frm], (frm * ny + y, me))

    def mcopy(s, i, k, to):
        src = msnd.at[s, i * 2 * ny + to * 2 + (half, 1 - half)[k]]
        dst = mbuf.at[s, k, pl.ds(pl.multiple_of(y * qr, qr), qr), :]
        return remote(src, dst, ms.at[0], mr.at[s], (at(z, to), owners[k] - 1 + i))

    def gat_of(s):
        return (gat_early, gat_late)[s // 2].at[pl.ds(s % 2 * rows, rows), :]

    def acopy(s, to):
        src = gsend.at[s, pl.ds(pl.multiple_of(to * rows, rows), rows), :]
        dst = gat_of(s).at[:, pl.ds(pl.multiple_of(dl * 2 * HD, 2 * HD), 2 * HD)]
        return remote(src, dst, as_.at[0], ar.at[s // 2], (sp, half * 4 + to))

    def whole(ref, send, recv):
        return remote(ref, ref, send, recv, (sp, partner))

    def norm_own(s):
        raw_loads[s].wait()
        scale = row_scale(lambda c: raw[s, :, c * HD:(c + 1) * HD].astype(F32), width)
        here = pl.ds(pl.multiple_of(dl * rows, rows), rows)
        for c in range(width // HD):
            cols = slice(c * HD, (c + 1) * HD)
            v = raw[s, :, cols].astype(F32)
            tok[s, here, cols] = (v * scale * gain[:, cols]).astype(BF16)

    gain_load.wait()
    norm_own(0)
    ng_load.wait()
    crow[0, pl.ds(1, 7), :] = jnp.full((7, HD), ld_ref[0], F32)

    pl.semaphore_wait(barrier, len(peers))
    own_send(0).start()
    pass_send(0, 0).start()
    for dev in near:
        pl.semaphore_signal(ready_a, inc=1, device_id=dev, device_id_type=MESH)
    c_send(0).start()
    c_send(1).start()
    for c in range(2):
        w_loads[c].wait()
        for j in range(4 * c, 4 * c + 4):
            w_send(j).start()
    for s in range(1, nseq):
        norm_own(s)
        if s == 1:
            own_send(s).start()
        pass_send(s, 0).start()

    i_col = lax.broadcasted_iota(jnp.int32, (BLOCK, HD), 0).astype(F32)
    i_row = lax.broadcasted_iota(jnp.int32, (BLOCK, HD), 1).astype(F32)

    def decay(k, count):
        return jnp.exp(crow[k, pl.ds(1, 1), :] * count)

    def head_tables(k):
        ld = crow[k, pl.ds(1, 1), :]
        dist = i_col - i_row
        dmat[k] = jnp.where(dist >= 0, jnp.exp(ld * jnp.maximum(dist, 0.0)), 0.0)
        qsc[k] = jnp.exp(ld * (i_col + 1.0))
        ksc[k] = jnp.exp(ld * (BLOCK - 1.0 - i_col))

    head_tables(0)
    tab_load.wait()
    sign = jnp.where(i_row < HD // 2, -1.0, 1.0)
    for b in range(blocks):
        start = sp * nchip + half * blocks + b
        cb = tabs[2, pl.ds(start, 1), :]
        sb = tabs[3, pl.ds(start, 1), :]
        ctab[b] = tabs[0] * cb - tabs[1] * sb
        stab[b] = (tabs[1] * cb + tabs[0] * sb) * sign

    def rotate(u, b):
        return u * ctab[b] + pltpu.roll(u, HD // 2, 1) * stab[b]

    def tokens_of(s, b0, nb):
        return tok[s, pl.ds(pl.multiple_of(b0 * BLOCK, BLOCK), nb * BLOCK), :]

    def block_at(b):
        return pl.ds(pl.multiple_of(b * BLOCK, BLOCK), BLOCK)

    def keys(s, k, b0, nb):
        proj = jnp.dot(tokens_of(s, b0, nb), w[k, 0], preferred_element_type=F32).astype(BF16)
        for i in range(nb):
            b = b0 + i
            here = block_at(b)
            p = proj[i * BLOCK:(i + 1) * BLOCK]
            kk = (rotate(p[:, :HD].astype(F32), b) * HD ** -0.5).astype(BF16)
            v = p[:, HD:]
            kbuf[s, k, here, :] = kk
            vbuf[s, k, here, :] = v
            ks = (kk.astype(F32) * ksc[k]).astype(BF16)
            smat[s, k, b] = lax.dot_general(ks, v, (((0,), (0,)), ((), ())), preferred_element_type=F32)

    def queries(s, k, b0, nb):
        proj = jnp.dot(tokens_of(s, b0, nb), w[k, 1], preferred_element_type=F32).astype(BF16)
        for i in range(nb):
            b = b0 + i
            here = block_at(b)
            p = proj[i * BLOCK:(i + 1) * BLOCK]
            q = rotate(p[:, :HD].astype(F32), b).astype(BF16)
            g = p[:, HD:].astype(F32)
            scores = lax.dot_general(q, kbuf[s, k, here, :], (((1,), (1,)), ((), ())), preferred_element_type=F32)
            weights = (scores * dmat[k]).astype(BF16)
            acc[s, k, here, :] = jnp.dot(weights, vbuf[s, k, here, :], preferred_element_type=F32)
            qs[s, k, here, :] = (q.astype(F32) * qsc[k]).astype(BF16)
            gs[s, k, here, :] = crow[k, pl.ds(0, 1), :] * (g * jax.nn.sigmoid(g))

    far_first = [(1, ny // 2)]
    for to in range(1, ny):
        if to != ny // 2:
            far_first.append((1, to))
    far_first += [(0, ny // 2), (1, 0)]
    for to in range(1, ny):
        if to != ny // 2:
            far_first.append((0, to))

    def state_out(s):
        for k in range(2):
            esend[s, k] = (smat[s, k, 0] * decay(k, float(BLOCK)) + smat[s, k, 1]).astype(BF16)
        for k, to in far_first:
            ycopy(s, k, (y + to) % ny).start()

        @pl.when(core == 0)
        def _():
            ycopy(s, 0, y).start()

        @pl.when(core == 1)
        def _():
            kept = esend[s, 0, pl.ds(pl.multiple_of(y * qr, qr), qr), :]
            ybuf[s, 2 * ny + y * 2 + half] = kept

    def owned_decay(i, count):
        return decay((2, 0)[i], count)

    def state_row(s):
        @pl.when(core == 1)
        def _():
            whole(ybuf.at[s, pl.ds(0, 4 * ny - 1)], ys.at[0], yr.at[s]).wait_recv()
            for i in range(2):
                step = owned_decay(i, float(span))
                total = ybuf[s, i * 2 * ny].astype(F32)
                for k in range(1, 2 * ny):
                    total = total * step + ybuf[s, i * 2 * ny + k].astype(F32)
                zsnd[s, i] = total.astype(BF16)

            @pl.loop(0, nz - 1 - z)
            def _(k):
                zcopy(s, nz - 1 - k).start()

    def state_back(s):
        @pl.when(core == 1)
        def _():
            steps = [owned_decay(i, float(span)) for i in range(2)]
            row_steps = [owned_decay(i, float(span * 2 * ny)) for i in range(2)]

            def add(frm, totals):
                zrecv(s, frm).wait_recv()
                return tuple(totals[i] * row_steps[i] + zbuf[s, frm, i].astype(F32) for i in range(2))

            zero = jnp.zeros((qr, HD), F32)
            carried = lax.fori_loop(0, z, add, (zero, zero))
            for i in range(2):
                total = carried[i]
                for k in range(2 * ny):
                    msnd[s, i * 2 * ny + k] = total.astype(BF16)
                    if k < 2 * ny - 1:
                        total = total * steps[i] + ybuf[s, i * 2 * ny + k].astype(F32)
            for k, to in far_first:
                for i in range(2):
                    mcopy(s, i, k, (y + to) % ny).start()
            mcopy(s, 0, 0, y).start()
            mbuf[s, 0, pl.ds(pl.multiple_of(y * qr, qr), qr), :] = msnd[s, 2 * ny + y * 2 + half]

    def read_out(s):
        @pl.when(core == 0)
        def _():
            whole(ybuf.at[s, pl.ds(0, 2 * ny)], ms.at[0], mr.at[s]).wait_recv()

        @pl.when(core == 1)
        def _():
            whole(ybuf.at[s, pl.ds(0, 2 * ny - 1)], ms.at[0], mr.at[s]).wait_recv()

        for k in range(2):
            memory = mbuf[s, k]
            for b in range(blocks):
                here = pl.ds(b * BLOCK, BLOCK)
                if b:
                    memory = (smat[s, k, 0] + memory.astype(F32) * decay(k, float(BLOCK))).astype(BF16)
                kept = acc[s, k, here, :] + jnp.dot(qs[s, k, here, :], memory, preferred_element_type=F32)
                kept = kept - jnp.mean(kept, axis=-1, keepdims=True)
                spread = jnp.mean(kept * kept, axis=-1, keepdims=True)
                kept = kept * lax.rsqrt(spread + GROUP_EPS) * gs[s, k, here, :]
                gsend[s, here, k * HD:(k + 1) * HD] = kept.astype(BF16)
        for k in range(1, 4):
            acopy(s, (dl + k) % 4).start()
        own = gsend[s, pl.ds(pl.multiple_of(dl * rows, rows), rows), :]
        gat_of(s)[:, pl.ds(pl.multiple_of(dl * 2 * HD, 2 * HD), 2 * HD)] = own

    @pl.loop(0, nseq)
    def _(s):
        pass_recv(s, 0).wait_recv()
        keys(s, 0, mine, 1)
        queries(s, 0, mine, 1)

    pl.semaphore_wait(ready_a, len(near))
    far = ((at(z - 2, y), me), (at(z + 2, y), me), (sp, partner))
    for dev in far:
        pl.semaphore_signal(ready_b, inc=1, device_id=dev, device_id_type=MESH)

    def take_pair(s):
        own_recv(s).wait_recv()
        pass_send(s, 1).start()

    w_forward(0)
    own_send(2).start()
    w_forward(1)
    w_forward(2)
    take_pair(0)
    own_send(3).start()
    w_forward(3)
    pass_recv(0, 1).wait_recv()
    keys(0, 0, theirs, 1)
    w_forward(4)
    queries(0, 0, theirs, 1)
    w_forward(5)
    for i in range(2):
        whole(crow.at[1 + i], cs.at[0], cr.at[i]).wait_recv()
    head_tables(1)
    take_pair(1)
    w_forward(6)
    pass_recv(1, 1).wait_recv()
    keys(1, 0, theirs, 1)
    w_forward(7)
    pl.semaphore_wait(ready_b, len(far))
    w_rest(0).wait_recv()
    keys(0, 1, 0, 2)
    state_out(0)
    keys(1, 1, 0, 2)
    state_out(1)
    keys(2, 1, mine, 1)
    keys(3, 1, mine, 1)
    take_pair(2)
    queries(1, 0, theirs, 1)
    pass_recv(2, 1).wait_recv()
    keys(2, 0, theirs, 1)
    keys(2, 1, theirs, 1)
    state_out(2)
    state_row(0)
    state_row(1)
    queries(2, 0, theirs, 1)
    take_pair(3)
    w_rest(1).wait_recv()
    queries(0, 1, 0, 2)
    pass_recv(3, 1).wait_recv()
    keys(3, 0, theirs, 1)
    keys(3, 1, theirs, 1)
    state_out(3)
    queries(1, 1, 0, 2)
    state_row(2)
    state_back(0)
    state_back(1)
    queries(2, 1, 0, 2)
    queries(3, 0, theirs, 1)
    state_row(3)
    state_back(2)
    state_back(3)
    queries(3, 1, 0, 2)
    for s in range(nseq):
        read_out(s)
    ow_load.wait()
    pg_load.wait()
    whole(gat_early.at[:, 0:6 * HD], as_.at[0], ar.at[0]).wait_recv()
    osc[...] = jnp.dot(gat_early[...], oww[...], preferred_element_type=F32)
    scale_rows(osc, pg, mixed, 0, 2 * rows)
    whole(gat_late.at[:, 0:6 * HD], as_.at[0], ar.at[1]).wait_recv()

    whole(raw, xs.at[0], xr.at[0]).wait_send()
    whole(tok.at[:, 0:2 * rows, :], ps.at[0], pr.at[0, 0]).wait_send()
    whole(w.at[1, :, 0:quarter, :], wxs.at[0], wxr.at[0]).wait_send()
    whole(w.at[1, :, 0:3 * quarter, :], wfs.at[0], wfr.at[0]).wait_send()
    whole(crow.at[0:2], cs.at[0], cr.at[0]).wait_send()
    whole(gsend.at[:, pl.ds(0, 3 * rows), :], as_.at[0], ar.at[0]).wait_send()

    @pl.when(core == 0)
    def _():
        whole(ybuf.at[:, pl.ds(0, 2 * ny)], ys.at[0], yr.at[0]).wait_send()

    @pl.when(core == 1)
    def _():
        whole(ybuf.at[:, pl.ds(0, 2 * ny - 1)], ys.at[0], yr.at[0]).wait_send()
        whole(ybuf.at[:, pl.ds(0, 4 * ny - 1)], ms.at[0], mr.at[0]).wait_send()

        @pl.loop(z + 1, nz)
        def _(to):
            whole(zsnd, zs.at[to], zr.at[0, to]).wait_send()


def mix_kernel(gat, oww, mixed, pg, out_ref, osc, late, sem):
    done = mixed.shape[0]
    first = pltpu.make_async_copy(mixed, out_ref.at[pl.ds(0, done), :], sem.at[0])
    first.start()
    osc[...] = jnp.dot(gat[...], oww[...], preferred_element_type=F32)
    part = late.shape[0] // 2
    copies = [first]
    for i in range(2):
        here = pl.ds(i * part, part)
        scale_rows(osc, pg, late, i * part, part)
        copies.append(pltpu.make_async_copy(late.at[here], out_ref.at[pl.ds(done + i * part, part), :], sem.at[1 + i]))
        copies[-1].start()
    for copy in copies:
        copy.wait()


def body(nz, ny, tokens, in_gain, wq, wk, wv, wg, log_decay, norm_gain, out_weight, post_gain):
    nseq, rows, width = tokens.shape
    ntp = 8
    stretch = rows * ntp
    half = stretch // 2
    tables = jnp.asarray(np.stack(rotary_tables(BLOCK)))
    qr = HD // ny
    vmem, hbm, smem = (pl.BlockSpec(memory_space=m) for m in (pltpu.VMEM, pltpu.HBM, pltpu.SMEM))
    dma = pltpu.SemaphoreType.DMA
    signal = pltpu.SemaphoreType.REGULAR
    scratch = [
        pltpu.VMEM((nseq, rows, width), BF16),
        pltpu.VMEM((nseq, half, width), BF16),
        pltpu.VMEM((2, 2, width, 2 * HD), BF16),
        pltpu.VMEM((1, width), F32),
        pltpu.VMEM((1, width), F32),
        pltpu.VMEM(tables.shape, F32),
        pltpu.VMEM((3, 8, HD), F32),
        pltpu.VMEM((2, BLOCK, HD), F32),
        pltpu.VMEM((2, BLOCK, HD), F32),
        pltpu.VMEM((2, BLOCK, HD), F32),
        pltpu.VMEM((2, BLOCK, HD), F32),
        pltpu.VMEM((2, BLOCK, HD), F32),
        pltpu.VMEM((nseq, 2, half, HD), BF16),
        pltpu.VMEM((nseq, 2, half, HD), BF16),
        pltpu.VMEM((nseq, 2, half, HD), BF16),
        pltpu.VMEM((nseq, 2, half, HD), F32),
        pltpu.VMEM((nseq, 2, half, HD), F32),
        pltpu.VMEM((nseq, 2, 2, HD, HD), F32),
        pltpu.VMEM((nseq, 2, HD, HD), BF16),
        pltpu.VMEM((nseq, 4 * ny, qr, HD), BF16),
        pltpu.VMEM((nseq, 2, qr, HD), BF16),
        pltpu.VMEM((nseq, nz, 2, qr, HD), BF16),
        pltpu.VMEM((nseq, 4 * ny, qr, HD), BF16),
        pltpu.VMEM((nseq, 2, HD, HD), BF16),
        pltpu.VMEM((nseq, half, 2 * HD), BF16),
        pltpu.VMEM((2 * rows, ntp * HD), BF16),
        pltpu.VMEM((2 * rows, width), F32),
        dma((11,)),
        dma((1,)), dma((nseq,)), dma((1,)), dma((nseq, 2)), dma((1,)), dma((8,)), dma((1,)), dma((2,)),
        dma((1,)), dma((2,)), dma((1,)), dma((nseq,)), dma((nz,)), dma((nseq, nz)), dma((1,)), dma((nseq,)),
        dma((1,)), dma((2,)), signal, signal,
    ]
    late = 2 * rows
    gain = post_gain.reshape(1, -1)
    gathered, weight, early = pl.pallas_call(
        functools.partial(kernel, nz, ny),
        out_shape=[
            pltpu.VMEM((late, ntp * HD), BF16), pltpu.VMEM(out_weight.shape, BF16), pltpu.VMEM((late, width), BF16)
        ],
        in_specs=[hbm] * 6 + [smem] + [hbm] * 4,
        out_specs=[vmem] * 3,
        scratch_shapes=scratch,
        name="retention",
        compiler_params=pltpu.CompilerParams(
            collective_id=0, has_side_effects=True, vmem_limit_bytes=VMEM_LIMIT
        ),
    )(
        tokens, in_gain.reshape(1, -1), wq, wk, wv, wg, log_decay, norm_gain.reshape(1, -1), out_weight, gain, tables,
    )
    mixed = pl.pallas_call(
        mix_kernel,
        out_shape=jax.ShapeDtypeStruct((nseq * rows, width), BF16),
        in_specs=[vmem] * 4,
        out_specs=hbm,
        scratch_shapes=[pltpu.VMEM((late, width), F32), pltpu.VMEM((late, width), BF16), dma((3,))],
        name="mix",
        compiler_params=pltpu.CompilerParams(vmem_limit_bytes=16 * 1024 * 1024),
    )(gathered, weight, early, gain)
    return mixed.reshape(tokens.shape)


def solution(mesh):
    both = ("sp", "tp")
    nz = mesh.shape["sp"] // NY
    return jax.shard_map(
        functools.partial(body, nz, NY),
        mesh=mesh,
        in_specs=(
            P(None, both, None), P(), P(None, "tp"), P(None, "tp"), P(None, "tp"), P(None, "tp"), P("tp"), P("tp"),
            P(), P(),
        ),
        out_specs=P(None, both, None),
        check_vma=False,
    )
```

```python
import functools

import jax
import jax.numpy as jnp
import numpy as np
from jax import lax
from jax.experimental import pallas as pl
from jax.experimental.pallas import tpu as pltpu
from jax.sharding import PartitionSpec as P

MESH = pl.DeviceIdType.MESH
F32 = jnp.float32
BF16 = jnp.bfloat16
HD = 128
BLOCK = 128
NY = 4
VMEM_LIMIT = 62_000_000
RMS_EPS = 1e-06
GROUP_EPS = 1e-05
ROPE_BASE = 10000.0


def rotary_tables(blocks):
    half = HD // 2
    rate = ROPE_BASE ** (-np.arange(half, dtype=np.float64) / half)
    rate = np.concatenate([rate, rate])
    inside = np.arange(BLOCK, dtype=np.float64)[:, None] * rate
    starts = BLOCK * np.arange(blocks, dtype=np.float64)[:, None] * rate
    tables = (np.cos(inside), np.sin(inside), np.cos(starts), np.sin(starts))
    return [t.astype(np.float32) for t in tables]


def row_scale(read, width):
    total = jnp.square(read(0))
    for c in range(1, width // HD):
        total += jnp.square(read(c))
    return lax.rsqrt(jnp.sum(total, axis=-1, keepdims=True) * (1.0 / width) + RMS_EPS)


def scale_rows(osc, pg, out, start, count):
    width = osc.shape[1]
    here = pl.ds(start, count)
    scale = row_scale(lambda c: osc[here, c * HD:(c + 1) * HD], width)
    for c in range(width // HD):
        cols = slice(c * HD, (c + 1) * HD)
        out[here, cols] = (osc[here, cols] * scale * pg[:, cols]).astype(BF16)


def kernel(
    nz, ny, tok_hbm, gain_hbm, wq, wk, wv, wg, ld_ref, ng_hbm, ow, pg_hbm, tab_hbm,
    gat_late, oww, mixed, raw, tok, w, gain, pg, tabs, crow, ctab, stab, dmat, qsc, ksc, kbuf, vbuf, qs, acc, gs, smat, esend, ybuf,
    zsnd, zbuf, msnd, mbuf, gsend, gat_early, osc, lsem, xs, xr, ps, pr, wxs, wxr, wfs, wfr, cs, cr, ys, yr, zs, zr, ms, mr, as_, ar,
    ready_a, ready_b, ready_c,
):
    nseq, rows, width = raw.shape
    ntp = 8
    nchip = ntp // 2
    blocks = 2
    span = blocks * BLOCK
    qr = HD // ny
    quarter = width // 4
    chunk = quarter // 4
    sp = lax.axis_index("sp")
    me = lax.axis_index("tp")
    z, y = sp // ny, sp % ny
    chip, core = me // 2, me % 2
    partner = chip * 2 + 1 - core
    half, dl = chip // 2, me % 4
    mine, theirs = chip % 2, 1 - chip % 2
    pair_same = (half * 2 + theirs) * 2 + core
    pair_other = (half * 2 + theirs) * 2 + 1 - core
    mate = (nchip - 1 - chip) * 2 + core
    owners = (chip * 2 + 1, (nchip - 1 - chip) * 2 + 1)

    def at(zz, yy):
        return (zz + nz) % nz * ny + (yy + ny) % ny

    barrier = pltpu.get_barrier_semaphore()
    plane = [(at(z, y + k), me) for k in range(1, ny)] + [(sp, mate), (sp, partner)]
    beside = [(at(z - 1, y), me), (at(z + 1, y), me)]
    beyond = [(at(z - 2, y), me), (at(z + 2, y), me)]
    peers = [(sp, pair_same), (sp, pair_other)] + plane
    even, odd = z % 2 == 0, z % 2 == 1

    def tell(sem, devs):
        for dev in devs:
            pl.semaphore_signal(sem, inc=1, device_id=dev, device_id_type=MESH)

    tell(barrier, peers)

    @pl.when(even)
    def _():
        tell(barrier, beside)

    raw_loads = [pltpu.make_async_copy(tok_hbm.at[s], raw.at[s], lsem.at[s]) for s in range(nseq)]
    gain_load = pltpu.make_async_copy(gain_hbm, gain, lsem.at[4])
    tab_load = pltpu.make_async_copy(tab_hbm, tabs, lsem.at[5])
    pg_load = pltpu.make_async_copy(pg_hbm, pg, lsem.at[7])
    ng_load = pltpu.make_async_copy(ng_hbm, crow.at[0, pl.ds(0, 1)], lsem.at[6])
    w_loads = [pltpu.make_async_copy(w.at[0, c], w.at[0, c], lsem.at[8 + c]) for c in range(2)]
    ow_load = pltpu.make_async_copy(oww, oww, lsem.at[10])
    raw_loads[0].start()
    gain_load.start()
    ng_load.start()
    for load in raw_loads[1:]:
        load.start()
    for j, src in enumerate((wk, wv, wq, wg)):
        cols = j % 2 * HD
        pltpu.make_async_copy(src, w.at[0, j // 2, :, cols:cols + HD], lsem.at[8 + j // 2]).start()
    tab_load.start()
    pg_load.start()
    for d in range(4):
        first = half * 4 + d
        second = (nchip - 1 - first // 2) * 2 + d % 2
        for i, h in enumerate((first, second)):
            src = ow.at[pl.ds(pl.multiple_of(h * HD, HD), HD), :]
            pltpu.make_async_copy(src, oww.at[(2 * d + i) * HD:(2 * d + i + 1) * HD, :], lsem.at[10]).start()

    def remote(src, dst, send, recv, dev):
        return pltpu.make_async_remote_copy(
            src_ref=src, dst_ref=dst, send_sem=send, recv_sem=recv, device_id=dev, device_id_type=MESH
        )

    def part_of(s, d):
        return tok.at[s, pl.ds(pl.multiple_of(d * rows, rows), rows), :]

    def own_send(s):
        ref = part_of(s, dl)
        return remote(ref, ref, xs.at[0], xr.at[s], (sp, pair_same))

    def own_recv(s):
        ref = part_of(s, theirs * 2 + core)
        return remote(ref, ref, xs.at[0], xr.at[s], (sp, pair_same))

    def pass_send(s, i):
        ref = part_of(s, (mine, theirs)[i] * 2 + core)
        return remote(ref, ref, ps.at[0], pr.at[s, i], (sp, partner))

    def pass_recv(s, i):
        ref = part_of(s, (mine, theirs)[i] * 2 + 1 - core)
        return remote(ref, ref, ps.at[0], pr.at[s, i], (sp, partner))

    my_quarter = (y % 2) * 2 + z % 2

    def w_rows(k, j):
        at_ = pl.multiple_of(my_quarter * quarter + j % 4 * chunk, chunk)
        return w.at[k, j // 4, pl.ds(at_, chunk), :]

    def w_send(j):
        return remote(w_rows(0, j), w_rows(1, j), wxs.at[0], wxr.at[j], (sp, mate))

    def w_recv(j):
        return remote(w_rows(1, j), w_rows(1, j), wxs.at[0], wxr.at[j], (sp, mate))

    def w_forward(j):
        w_recv(j).wait_recv()
        yy, zz = y + (1, -1)[j % 2], z + (1, -1)[j // 2 % 2]
        for dev in (at(zz, yy), at(z, yy), at(zz, y)):
            remote(w_rows(1, j), w_rows(1, j), wfs.at[0], wfr.at[j // 4], (dev, me)).start()

    def w_rest(c):
        ref = w.at[1, c, 0:3 * quarter, :]
        return remote(ref, ref, wfs.at[0], wfr.at[c], (sp, partner))

    def c_send(i):
        return remote(crow.at[0], crow.at[1 + i], cs.at[0], cr.at[i], (sp, (mate, partner)[i]))

    def ycopy(s, k, to):
        src = esend.at[s, k, pl.ds(pl.multiple_of(to * qr, qr), qr), :]
        dst = ybuf.at[s, core * 2 * ny + y * 2 + half]
        return remote(src, dst, ys.at[0], yr.at[s], (at(z, to), owners[k]))

    def zcopy(s, to):
        return remote(zsnd.at[s], zbuf.at[s, z], zs.at[to], zr.at[s, z], (to * ny + y, me))

    def zrecv(s, frm):
        ref = zbuf.at[s, frm]
        return remote(ref, ref, zs.at[frm], zr.at[s, frm], (frm * ny + y, me))

    def mcopy(s, i, k, to):
        src = msnd.at[s, i * 2 * ny + to * 2 + (half, 1 - half)[k]]
        dst = mbuf.at[s, k, pl.ds(pl.multiple_of(y * qr, qr), qr), :]
        return remote(src, dst, ms.at[0], mr.at[s], (at(z, to), owners[k] - 1 + i))

    def gat_of(s):
        return (gat_early, gat_late)[s // 2].at[pl.ds(s % 2 * rows, rows), :]

    def acopy(s, to):
        src = gsend.at[s, pl.ds(pl.multiple_of(to * rows, rows), rows), :]
        dst = gat_of(s).at[:, pl.ds(pl.multiple_of(dl * 2 * HD, 2 * HD), 2 * HD)]
        return remote(src, dst, as_.at[0], ar.at[s // 2], (sp, half * 4 + to))

    def whole(ref, send, recv):
        return remote(ref, ref, send, recv, (sp, partner))

    def norm_own(s):
        raw_loads[s].wait()
        scale = row_scale(lambda c: raw[s, :, c * HD:(c + 1) * HD].astype(F32), width)
        here = pl.ds(pl.multiple_of(dl * rows, rows), rows)
        for c in range(width // HD):
            cols = slice(c * HD, (c + 1) * HD)
            v = raw[s, :, cols].astype(F32)
            tok[s, here, cols] = (v * scale * gain[:, cols]).astype(BF16)

    gain_load.wait()
    norm_own(0)
    ng_load.wait()
    crow[0, pl.ds(1, 7), :] = jnp.full((7, HD), ld_ref[0], F32)

    @pl.when(even)
    def _():
        pl.semaphore_wait(barrier, len(peers))

    @pl.when(odd)
    def _():
        pl.semaphore_wait(barrier, len(peers) + 2)

    own_send(0).start()
    pass_send(0, 0).start()
    tell(ready_a, plane)

    @pl.when(odd)
    def _():
        tell(ready_a, beside)

    c_send(0).start()
    c_send(1).start()
    for c in range(2):
        w_loads[c].wait()
        for j in range(4 * c, 4 * c + 4):
            w_send(j).start()
    for s in range(1, nseq):
        norm_own(s)
        if s == 1:
            own_send(s).start()
        pass_send(s, 0).start()

    i_col = lax.broadcasted_iota(jnp.int32, (BLOCK, HD), 0).astype(F32)
    i_row = lax.broadcasted_iota(jnp.int32, (BLOCK, HD), 1).astype(F32)

    def decay(k, count):
        return jnp.exp(crow[k, pl.ds(1, 1), :] * count)

    def head_tables(k):
        ld = crow[k, pl.ds(1, 1), :]
        dist = i_col - i_row
        dmat[k] = jnp.where(dist >= 0, jnp.exp(ld * jnp.maximum(dist, 0.0)), 0.0)
        qsc[k] = jnp.exp(ld * (i_col + 1.0))
        ksc[k] = jnp.exp(ld * (BLOCK - 1.0 - i_col))

    head_tables(0)
    tab_load.wait()
    sign = jnp.where(i_row < HD // 2, -1.0, 1.0)
    for b in range(blocks):
        start = sp * nchip + half * blocks + b
        cb = tabs[2, pl.ds(start, 1), :]
        sb = tabs[3, pl.ds(start, 1), :]
        ctab[b] = tabs[0] * cb - tabs[1] * sb
        stab[b] = (tabs[1] * cb + tabs[0] * sb) * sign

    def rotate(u, b):
        return u * ctab[b] + pltpu.roll(u, HD // 2, 1) * stab[b]

    def tokens_of(s, b0, nb):
        return tok[s, pl.ds(pl.multiple_of(b0 * BLOCK, BLOCK), nb * BLOCK), :]

    def block_at(b):
        return pl.ds(pl.multiple_of(b * BLOCK, BLOCK), BLOCK)

    def keys(s, k, b0, nb):
        proj = jnp.dot(tokens_of(s, b0, nb), w[k, 0], preferred_element_type=F32).astype(BF16)
        for i in range(nb):
            b = b0 + i
            here = block_at(b)
            p = proj[i * BLOCK:(i + 1) * BLOCK]
            kk = (rotate(p[:, :HD].astype(F32), b) * HD ** -0.5).astype(BF16)
            v = p[:, HD:]
            kbuf[s, k, here, :] = kk
            vbuf[s, k, here, :] = v
            ks = (kk.astype(F32) * ksc[k]).astype(BF16)
            smat[s, k, b] = lax.dot_general(ks, v, (((0,), (0,)), ((), ())), preferred_element_type=F32)

    def queries(s, k, b0, nb):
        proj = jnp.dot(tokens_of(s, b0, nb), w[k, 1], preferred_element_type=F32).astype(BF16)
        for i in range(nb):
            b = b0 + i
            here = block_at(b)
            p = proj[i * BLOCK:(i + 1) * BLOCK]
            q = rotate(p[:, :HD].astype(F32), b).astype(BF16)
            g = p[:, HD:].astype(F32)
            scores = lax.dot_general(q, kbuf[s, k, here, :], (((1,), (1,)), ((), ())), preferred_element_type=F32)
            weights = (scores * dmat[k]).astype(BF16)
            acc[s, k, here, :] = jnp.dot(weights, vbuf[s, k, here, :], preferred_element_type=F32)
            qs[s, k, here, :] = (q.astype(F32) * qsc[k]).astype(BF16)
            gs[s, k, here, :] = crow[k, pl.ds(0, 1), :] * (g * jax.nn.sigmoid(g))

    far_first = [(1, ny // 2)]
    for to in range(1, ny):
        if to != ny // 2:
            far_first.append((1, to))
    far_first += [(0, ny // 2), (1, 0)]
    for to in range(1, ny):
        if to != ny // 2:
            far_first.append((0, to))

    def state_out(s):
        for k in range(2):
            esend[s, k] = (smat[s, k, 0] * decay(k, float(BLOCK)) + smat[s, k, 1]).astype(BF16)
        for k, to in far_first:
            ycopy(s, k, (y + to) % ny).start()

        @pl.when(core == 0)
        def _():
            ycopy(s, 0, y).start()

        @pl.when(core == 1)
        def _():
            kept = esend[s, 0, pl.ds(pl.multiple_of(y * qr, qr), qr), :]
            ybuf[s, 2 * ny + y * 2 + half] = kept

    def owned_decay(i, count):
        return decay((2, 0)[i], count)

    def state_row(s):
        @pl.when(core == 1)
        def _():
            whole(ybuf.at[s, pl.ds(0, 4 * ny - 1)], ys.at[0], yr.at[s]).wait_recv()
            for i in range(2):
                step = owned_decay(i, float(span))
                total = ybuf[s, i * 2 * ny].astype(F32)
                for k in range(1, 2 * ny):
                    total = total * step + ybuf[s, i * 2 * ny + k].astype(F32)
                zsnd[s, i] = total.astype(BF16)

            @pl.loop(0, nz - 1 - z)
            def _(k):
                zcopy(s, nz - 1 - k).start()

    def state_back(s):
        @pl.when(core == 1)
        def _():
            steps = [owned_decay(i, float(span)) for i in range(2)]
            row_steps = [owned_decay(i, float(span * 2 * ny)) for i in range(2)]

            def add(frm, totals):
                zrecv(s, frm).wait_recv()
                return tuple(totals[i] * row_steps[i] + zbuf[s, frm, i].astype(F32) for i in range(2))

            zero = jnp.zeros((qr, HD), F32)
            carried = lax.fori_loop(0, z, add, (zero, zero))
            for i in range(2):
                total = carried[i]
                for k in range(2 * ny):
                    msnd[s, i * 2 * ny + k] = total.astype(BF16)
                    if k < 2 * ny - 1:
                        total = total * steps[i] + ybuf[s, i * 2 * ny + k].astype(F32)
            for k, to in far_first:
                for i in range(2):
                    mcopy(s, i, k, (y + to) % ny).start()
            mcopy(s, 0, 0, y).start()
            mbuf[s, 0, pl.ds(pl.multiple_of(y * qr, qr), qr), :] = msnd[s, 2 * ny + y * 2 + half]

    def read_out(s):
        @pl.when(core == 0)
        def _():
            whole(ybuf.at[s, pl.ds(0, 2 * ny)], ms.at[0], mr.at[s]).wait_recv()

        @pl.when(core == 1)
        def _():
            whole(ybuf.at[s, pl.ds(0, 2 * ny - 1)], ms.at[0], mr.at[s]).wait_recv()

        for k in range(2):
            memory = mbuf[s, k]
            for b in range(blocks):
                here = pl.ds(b * BLOCK, BLOCK)
                if b:
                    memory = (smat[s, k, 0] + memory.astype(F32) * decay(k, float(BLOCK))).astype(BF16)
                kept = acc[s, k, here, :] + jnp.dot(qs[s, k, here, :], memory, preferred_element_type=F32)
                kept = kept - jnp.mean(kept, axis=-1, keepdims=True)
                spread = jnp.mean(kept * kept, axis=-1, keepdims=True)
                kept = kept * lax.rsqrt(spread + GROUP_EPS) * gs[s, k, here, :]
                gsend[s, here, k * HD:(k + 1) * HD] = kept.astype(BF16)
        for k in range(1, 4):
            acopy(s, (dl + k) % 4).start()
        own = gsend[s, pl.ds(pl.multiple_of(dl * rows, rows), rows), :]
        gat_of(s)[:, pl.ds(pl.multiple_of(dl * 2 * HD, 2 * HD), 2 * HD)] = own

    @pl.loop(0, nseq)
    def _(s):
        pass_recv(s, 0).wait_recv()
        keys(s, 0, mine, 1)
        queries(s, 0, mine, 1)

    @pl.when(even)
    def _():
        pl.semaphore_wait(ready_a, len(plane) + 2)
        tell(ready_b, beyond)

    @pl.when(odd)
    def _():
        pl.semaphore_wait(ready_a, len(plane))

    tell(ready_b, [(sp, partner)])

    def take_pair(s):
        own_recv(s).wait_recv()
        pass_send(s, 1).start()

    w_forward(0)
    own_send(2).start()
    w_forward(1)
    w_forward(2)
    take_pair(0)
    own_send(3).start()
    w_forward(3)
    pass_recv(0, 1).wait_recv()
    keys(0, 0, theirs, 1)
    w_forward(4)
    queries(0, 0, theirs, 1)
    w_forward(5)
    for i in range(2):
        whole(crow.at[1 + i], cs.at[0], cr.at[i]).wait_recv()
    head_tables(1)
    take_pair(1)
    w_forward(6)
    pass_recv(1, 1).wait_recv()
    keys(1, 0, theirs, 1)
    w_forward(7)
    @pl.when(even)
    def _():
        pl.semaphore_wait(ready_b, 3)
        tell(ready_c, beside)

    @pl.when(odd)
    def _():
        pl.semaphore_wait(ready_b, 1)

    w_rest(0).wait_recv()
    keys(0, 1, 0, 2)
    state_out(0)
    keys(1, 1, 0, 2)
    state_out(1)
    keys(2, 1, mine, 1)
    keys(3, 1, mine, 1)
    take_pair(2)
    queries(1, 0, theirs, 1)
    pass_recv(2, 1).wait_recv()
    keys(2, 0, theirs, 1)
    keys(2, 1, theirs, 1)
    state_out(2)
    @pl.when(odd)
    def _():
        pl.semaphore_wait(ready_c, 2)

    state_row(0)
    state_row(1)
    queries(2, 0, theirs, 1)
    take_pair(3)
    w_rest(1).wait_recv()
    queries(0, 1, 0, 2)
    pass_recv(3, 1).wait_recv()
    keys(3, 0, theirs, 1)
    keys(3, 1, theirs, 1)
    state_out(3)
    queries(1, 1, 0, 2)
    state_row(2)
    state_back(0)
    state_back(1)
    queries(2, 1, 0, 2)
    queries(3, 0, theirs, 1)
    state_row(3)
    state_back(2)
    state_back(3)
    queries(3, 1, 0, 2)
    for s in range(nseq):
        read_out(s)
    ow_load.wait()
    pg_load.wait()
    whole(gat_early.at[:, 0:6 * HD], as_.at[0], ar.at[0]).wait_recv()
    osc[...] = jnp.dot(gat_early[...], oww[...], preferred_element_type=F32)
    scale_rows(osc, pg, mixed, 0, 2 * rows)
    whole(gat_late.at[:, 0:6 * HD], as_.at[0], ar.at[1]).wait_recv()

    whole(raw, xs.at[0], xr.at[0]).wait_send()
    whole(tok.at[:, 0:2 * rows, :], ps.at[0], pr.at[0, 0]).wait_send()
    whole(w.at[1, :, 0:quarter, :], wxs.at[0], wxr.at[0]).wait_send()
    whole(w.at[1, :, 0:3 * quarter, :], wfs.at[0], wfr.at[0]).wait_send()
    whole(crow.at[0:2], cs.at[0], cr.at[0]).wait_send()
    whole(gsend.at[:, pl.ds(0, 3 * rows), :], as_.at[0], ar.at[0]).wait_send()

    @pl.when(core == 0)
    def _():
        whole(ybuf.at[:, pl.ds(0, 2 * ny)], ys.at[0], yr.at[0]).wait_send()

    @pl.when(core == 1)
    def _():
        whole(ybuf.at[:, pl.ds(0, 2 * ny - 1)], ys.at[0], yr.at[0]).wait_send()
        whole(ybuf.at[:, pl.ds(0, 4 * ny - 1)], ms.at[0], mr.at[0]).wait_send()

        @pl.loop(z + 1, nz)
        def _(to):
            whole(zsnd, zs.at[to], zr.at[0, to]).wait_send()


def mix_kernel(gat, oww, mixed, pg, out_ref, osc, late, sem):
    done = mixed.shape[0]
    first = pltpu.make_async_copy(mixed, out_ref.at[pl.ds(0, done), :], sem.at[0])
    first.start()
    osc[...] = jnp.dot(gat[...], oww[...], preferred_element_type=F32)
    part = late.shape[0] // 2
    copies = [first]
    for i in range(2):
        here = pl.ds(i * part, part)
        scale_rows(osc, pg, late, i * part, part)
        copies.append(pltpu.make_async_copy(late.at[here], out_ref.at[pl.ds(done + i * part, part), :], sem.at[1 + i]))
        copies[-1].start()
    for copy in copies:
        copy.wait()


def body(nz, ny, tokens, in_gain, wq, wk, wv, wg, log_decay, norm_gain, out_weight, post_gain):
    nseq, rows, width = tokens.shape
    ntp = 8
    stretch = rows * ntp
    half = stretch // 2
    tables = jnp.asarray(np.stack(rotary_tables(BLOCK)))
    qr = HD // ny
    vmem, hbm, smem = (pl.BlockSpec(memory_space=m) for m in (pltpu.VMEM, pltpu.HBM, pltpu.SMEM))
    dma = pltpu.SemaphoreType.DMA
    signal = pltpu.SemaphoreType.REGULAR
    scratch = [
        pltpu.VMEM((nseq, rows, width), BF16),
        pltpu.VMEM((nseq, half, width), BF16),
        pltpu.VMEM((2, 2, width, 2 * HD), BF16),
        pltpu.VMEM((1, width), F32),
        pltpu.VMEM((1, width), F32),
        pltpu.VMEM(tables.shape, F32),
        pltpu.VMEM((3, 8, HD), F32),
        pltpu.VMEM((2, BLOCK, HD), F32),
        pltpu.VMEM((2, BLOCK, HD), F32),
        pltpu.VMEM((2, BLOCK, HD), F32),
        pltpu.VMEM((2, BLOCK, HD), F32),
        pltpu.VMEM((2, BLOCK, HD), F32),
        pltpu.VMEM((nseq, 2, half, HD), BF16),
        pltpu.VMEM((nseq, 2, half, HD), BF16),
        pltpu.VMEM((nseq, 2, half, HD), BF16),
        pltpu.VMEM((nseq, 2, half, HD), F32),
        pltpu.VMEM((nseq, 2, half, HD), F32),
        pltpu.VMEM((nseq, 2, 2, HD, HD), F32),
        pltpu.VMEM((nseq, 2, HD, HD), BF16),
        pltpu.VMEM((nseq, 4 * ny, qr, HD), BF16),
        pltpu.VMEM((nseq, 2, qr, HD), BF16),
        pltpu.VMEM((nseq, nz, 2, qr, HD), BF16),
        pltpu.VMEM((nseq, 4 * ny, qr, HD), BF16),
        pltpu.VMEM((nseq, 2, HD, HD), BF16),
        pltpu.VMEM((nseq, half, 2 * HD), BF16),
        pltpu.VMEM((2 * rows, ntp * HD), BF16),
        pltpu.VMEM((2 * rows, width), F32),
        dma((11,)),
        dma((1,)), dma((nseq,)), dma((1,)), dma((nseq, 2)), dma((1,)), dma((8,)), dma((1,)), dma((2,)),
        dma((1,)), dma((2,)), dma((1,)), dma((nseq,)), dma((nz,)), dma((nseq, nz)), dma((1,)), dma((nseq,)),
        dma((1,)), dma((2,)), signal, signal, signal,
    ]
    late = 2 * rows
    gain = post_gain.reshape(1, -1)
    gathered, weight, early = pl.pallas_call(
        functools.partial(kernel, nz, ny),
        out_shape=[
            pltpu.VMEM((late, ntp * HD), BF16), pltpu.VMEM(out_weight.shape, BF16), pltpu.VMEM((late, width), BF16)
        ],
        in_specs=[hbm] * 6 + [smem] + [hbm] * 4,
        out_specs=[vmem] * 3,
        scratch_shapes=scratch,
        name="retention",
        compiler_params=pltpu.CompilerParams(
            collective_id=0, has_side_effects=True, vmem_limit_bytes=VMEM_LIMIT
        ),
    )(
        tokens, in_gain.reshape(1, -1), wq, wk, wv, wg, log_decay, norm_gain.reshape(1, -1), out_weight, gain, tables,
    )
    mixed = pl.pallas_call(
        mix_kernel,
        out_shape=jax.ShapeDtypeStruct((nseq * rows, width), BF16),
        in_specs=[vmem] * 4,
        out_specs=hbm,
        scratch_shapes=[pltpu.VMEM((late, width), F32), pltpu.VMEM((late, width), BF16), dma((3,))],
        name="mix",
        compiler_params=pltpu.CompilerParams(vmem_limit_bytes=16 * 1024 * 1024),
    )(gathered, weight, early, gain)
    return mixed.reshape(tokens.shape)


def solution(mesh):
    both = ("sp", "tp")
    nz = mesh.shape["sp"] // NY
    return jax.shard_map(
        functools.partial(body, nz, NY),
        mesh=mesh,
        in_specs=(
            P(None, both, None), P(), P(None, "tp"), P(None, "tp"), P(None, "tp"), P(None, "tp"), P("tp"), P("tp"),
            P(), P(),
        ),
        out_specs=P(None, both, None),
        check_vma=False,
    )
```

```python
import functools

import jax
import jax.numpy as jnp
import numpy as np
from jax import lax
from jax.experimental import pallas as pl
from jax.experimental.pallas import tpu as pltpu
from jax.sharding import PartitionSpec as P

MESH = pl.DeviceIdType.MESH
F32 = jnp.float32
BF16 = jnp.bfloat16
HD = 128
BLOCK = 128
NY = 4
VMEM_LIMIT = 62_000_000
RMS_EPS = 1e-06
GROUP_EPS = 1e-05
ROPE_BASE = 10000.0


def rotary_tables(blocks):
    half = HD // 2
    rate = ROPE_BASE ** (-np.arange(half, dtype=np.float64) / half)
    rate = np.concatenate([rate, rate])
    inside = np.arange(BLOCK, dtype=np.float64)[:, None] * rate
    starts = BLOCK * np.arange(blocks, dtype=np.float64)[:, None] * rate
    tables = (np.cos(inside), np.sin(inside), np.cos(starts), np.sin(starts))
    return [t.astype(np.float32) for t in tables]


def row_scale(read, width):
    total = jnp.square(read(0))
    for c in range(1, width // HD):
        total += jnp.square(read(c))
    return lax.rsqrt(jnp.sum(total, axis=-1, keepdims=True) * (1.0 / width) + RMS_EPS)


def scale_rows(osc, pg, out, start, count):
    width = osc.shape[1]
    here = pl.ds(start, count)
    scale = row_scale(lambda c: osc[here, c * HD:(c + 1) * HD], width)
    for c in range(width // HD):
        cols = slice(c * HD, (c + 1) * HD)
        out[here, cols] = (osc[here, cols] * scale * pg[:, cols]).astype(BF16)


def kernel(
    nz, ny, tok_hbm, gain_hbm, wq, wk, wv, wg, ld_ref, ng_hbm, ow, pg_hbm, tab_hbm,
    gat_late, oww, mixed, raw, tok, w, gain, pg, tabs, crow, ctab, stab, dmat, qsc, ksc, kbuf, vbuf, qs, acc, gs, smat, esend, ybuf,
    zsnd, zbuf, msnd, mbuf, gsend, gat_early, osc, lsem, xs, xr, ps, pr, wxs, wxr, wfs, wfr, cs, cr, ys, yr, zs, zr, ms, mr, as_, ar,
    ready_a, ready_b, ready_c,
):
    nseq, rows, width = raw.shape
    ntp = 8
    nchip = ntp // 2
    blocks = 2
    span = blocks * BLOCK
    qr = HD // ny
    quarter = width // 4
    chunk = quarter // 4
    sp = lax.axis_index("sp")
    me = lax.axis_index("tp")
    z, y = sp // ny, sp % ny
    chip, core = me // 2, me % 2
    partner = chip * 2 + 1 - core
    half, dl = chip // 2, me % 4
    mine, theirs = chip % 2, 1 - chip % 2
    pair_same = (half * 2 + theirs) * 2 + core
    pair_other = (half * 2 + theirs) * 2 + 1 - core
    mate = (nchip - 1 - chip) * 2 + core
    owners = (chip * 2 + 1, (nchip - 1 - chip) * 2 + 1)

    def at(zz, yy):
        return (zz + nz) % nz * ny + (yy + ny) % ny

    barrier = pltpu.get_barrier_semaphore()
    plane = [(at(z, y + k), me) for k in range(1, ny)] + [(sp, mate), (sp, partner)]
    beside = [(at(z - 1, y), me), (at(z + 1, y), me)]
    beyond = [(at(z - 2, y), me), (at(z + 2, y), me)]
    peers = [(sp, pair_same), (sp, pair_other)] + plane
    even, odd = z % 2 == 0, z % 2 == 1

    def tell(sem, devs):
        for dev in devs:
            pl.semaphore_signal(sem, inc=1, device_id=dev, device_id_type=MESH)

    tell(barrier, peers)

    @pl.when(even)
    def _():
        tell(barrier, beside)

    raw_loads = [pltpu.make_async_copy(tok_hbm.at[s], raw.at[s], lsem.at[s]) for s in range(nseq)]
    gain_load = pltpu.make_async_copy(gain_hbm, gain, lsem.at[4])
    tab_load = pltpu.make_async_copy(tab_hbm, tabs, lsem.at[5])
    pg_load = pltpu.make_async_copy(pg_hbm, pg, lsem.at[7])
    ng_load = pltpu.make_async_copy(ng_hbm, crow.at[0, pl.ds(0, 1)], lsem.at[6])
    w_loads = [pltpu.make_async_copy(w.at[0, c], w.at[0, c], lsem.at[8 + c]) for c in range(2)]
    ow_load = pltpu.make_async_copy(oww, oww, lsem.at[10])
    raw_loads[0].start()
    gain_load.start()
    ng_load.start()
    for load in raw_loads[1:]:
        load.start()
    for j, src in enumerate((wk, wv, wq, wg)):
        cols = j % 2 * HD
        pltpu.make_async_copy(src, w.at[0, j // 2, :, cols:cols + HD], lsem.at[8 + j // 2]).start()
    tab_load.start()
    pg_load.start()
    for d in range(4):
        first = half * 4 + d
        second = (nchip - 1 - first // 2) * 2 + d % 2
        for i, h in enumerate((first, second)):
            src = ow.at[pl.ds(pl.multiple_of(h * HD, HD), HD), :]
            pltpu.make_async_copy(src, oww.at[(2 * d + i) * HD:(2 * d + i + 1) * HD, :], lsem.at[10]).start()

    def remote(src, dst, send, recv, dev):
        return pltpu.make_async_remote_copy(
            src_ref=src, dst_ref=dst, send_sem=send, recv_sem=recv, device_id=dev, device_id_type=MESH
        )

    def part_of(s, d):
        return tok.at[s, pl.ds(pl.multiple_of(d * rows, rows), rows), :]

    def own_send(s):
        ref = part_of(s, dl)
        return remote(ref, ref, xs.at[0], xr.at[s], (sp, pair_same))

    def own_recv(s):
        ref = part_of(s, theirs * 2 + core)
        return remote(ref, ref, xs.at[0], xr.at[s], (sp, pair_same))

    def pass_send(s, i):
        ref = part_of(s, (mine, theirs)[i] * 2 + core)
        return remote(ref, ref, ps.at[0], pr.at[s, i], (sp, partner))

    def pass_recv(s, i):
        ref = part_of(s, (mine, theirs)[i] * 2 + 1 - core)
        return remote(ref, ref, ps.at[0], pr.at[s, i], (sp, partner))

    my_quarter = (y % 2) * 2 + z % 2

    def w_rows(k, j):
        at_ = pl.multiple_of(my_quarter * quarter + j % 4 * chunk, chunk)
        return w.at[k, j // 4, pl.ds(at_, chunk), :]

    def w_send(j):
        return remote(w_rows(0, j), w_rows(1, j), wxs.at[0], wxr.at[j], (sp, mate))

    def w_recv(j):
        return remote(w_rows(1, j), w_rows(1, j), wxs.at[0], wxr.at[j], (sp, mate))

    def w_forward(j):
        w_recv(j).wait_recv()
        yy, zz = y + (1, -1)[j % 2], z + (1, -1)[j // 2 % 2]
        for dev in (at(zz, yy), at(z, yy), at(zz, y)):
            remote(w_rows(1, j), w_rows(1, j), wfs.at[0], wfr.at[j // 4], (dev, me)).start()

    def w_rest(c):
        ref = w.at[1, c, 0:3 * quarter, :]
        return remote(ref, ref, wfs.at[0], wfr.at[c], (sp, partner))

    def c_send(i):
        return remote(crow.at[0], crow.at[1 + i], cs.at[0], cr.at[i], (sp, (mate, partner)[i]))

    def ycopy(s, k, to):
        src = esend.at[s, k, pl.ds(pl.multiple_of(to * qr, qr), qr), :]
        dst = ybuf.at[s, core * 2 * ny + y * 2 + half]
        return remote(src, dst, ys.at[0], yr.at[s], (at(z, to), owners[k]))

    def zcopy(s, to):
        return remote(zsnd.at[s], zbuf.at[s, z], zs.at[0], zr.at[s], (to * ny + y, me))

    def mcopy(s, i, k, to):
        src = msnd.at[s, i * 2 * ny + to * 2 + (half, 1 - half)[k]]
        dst = mbuf.at[s, k, pl.ds(pl.multiple_of(y * qr, qr), qr), :]
        return remote(src, dst, ms.at[0], mr.at[s], (at(z, to), owners[k] - 1 + i))

    def gat_of(s):
        return (gat_early, gat_late)[s // 2].at[pl.ds(s % 2 * rows, rows), :]

    def acopy(s, to):
        src = gsend.at[s, pl.ds(pl.multiple_of(to * rows, rows), rows), :]
        dst = gat_of(s).at[:, pl.ds(pl.multiple_of(dl * 2 * HD, 2 * HD), 2 * HD)]
        return remote(src, dst, as_.at[0], ar.at[s // 2], (sp, half * 4 + to))

    def whole(ref, send, recv):
        return remote(ref, ref, send, recv, (sp, partner))

    def norm_own(s):
        raw_loads[s].wait()
        scale = row_scale(lambda c: raw[s, :, c * HD:(c + 1) * HD].astype(F32), width)
        here = pl.ds(pl.multiple_of(dl * rows, rows), rows)
        for c in range(width // HD):
            cols = slice(c * HD, (c + 1) * HD)
            v = raw[s, :, cols].astype(F32)
            tok[s, here, cols] = (v * scale * gain[:, cols]).astype(BF16)

    gain_load.wait()
    norm_own(0)
    ng_load.wait()
    crow[0, pl.ds(1, 7), :] = jnp.full((7, HD), ld_ref[0], F32)

    @pl.when(even)
    def _():
        pl.semaphore_wait(barrier, len(peers))

    @pl.when(odd)
    def _():
        pl.semaphore_wait(barrier, len(peers) + 2)

    own_send(0).start()
    pass_send(0, 0).start()
    tell(ready_a, plane)

    @pl.when(odd)
    def _():
        tell(ready_a, beside)

    c_send(0).start()
    c_send(1).start()
    for c in range(2):
        w_loads[c].wait()
        for j in range(4 * c, 4 * c + 4):
            w_send(j).start()
    for s in range(1, nseq):
        norm_own(s)
        if s == 1:
            own_send(s).start()
        pass_send(s, 0).start()

    i_col = lax.broadcasted_iota(jnp.int32, (BLOCK, HD), 0).astype(F32)
    i_row = lax.broadcasted_iota(jnp.int32, (BLOCK, HD), 1).astype(F32)

    def decay(k, count):
        return jnp.exp(crow[k, pl.ds(1, 1), :] * count)

    def head_tables(k):
        ld = crow[k, pl.ds(1, 1), :]
        dist = i_col - i_row
        dmat[k] = jnp.where(dist >= 0, jnp.exp(ld * jnp.maximum(dist, 0.0)), 0.0)
        qsc[k] = jnp.exp(ld * (i_col + 1.0))
        ksc[k] = jnp.exp(ld * (BLOCK - 1.0 - i_col))

    head_tables(0)
    tab_load.wait()
    sign = jnp.where(i_row < HD // 2, -1.0, 1.0)
    for b in range(blocks):
        start = sp * nchip + half * blocks + b
        cb = tabs[2, pl.ds(start, 1), :]
        sb = tabs[3, pl.ds(start, 1), :]
        ctab[b] = tabs[0] * cb - tabs[1] * sb
        stab[b] = (tabs[1] * cb + tabs[0] * sb) * sign

    def rotate(u, b):
        return u * ctab[b] + pltpu.roll(u, HD // 2, 1) * stab[b]

    def tokens_of(s, b0, nb):
        return tok[s, pl.ds(pl.multiple_of(b0 * BLOCK, BLOCK), nb * BLOCK), :]

    def block_at(b):
        return pl.ds(pl.multiple_of(b * BLOCK, BLOCK), BLOCK)

    def keys(s, k, b0, nb):
        proj = jnp.dot(tokens_of(s, b0, nb), w[k, 0], preferred_element_type=F32).astype(BF16)
        for i in range(nb):
            b = b0 + i
            here = block_at(b)
            p = proj[i * BLOCK:(i + 1) * BLOCK]
            kk = (rotate(p[:, :HD].astype(F32), b) * HD ** -0.5).astype(BF16)
            v = p[:, HD:]
            kbuf[s, k, here, :] = kk
            vbuf[s, k, here, :] = v
            ks = (kk.astype(F32) * ksc[k]).astype(BF16)
            smat[s, k, b] = lax.dot_general(ks, v, (((0,), (0,)), ((), ())), preferred_element_type=F32)

    def queries(s, k, b0, nb):
        proj = jnp.dot(tokens_of(s, b0, nb), w[k, 1], preferred_element_type=F32).astype(BF16)
        for i in range(nb):
            b = b0 + i
            here = block_at(b)
            p = proj[i * BLOCK:(i + 1) * BLOCK]
            q = rotate(p[:, :HD].astype(F32), b).astype(BF16)
            g = p[:, HD:].astype(F32)
            scores = lax.dot_general(q, kbuf[s, k, here, :], (((1,), (1,)), ((), ())), preferred_element_type=F32)
            weights = (scores * dmat[k]).astype(BF16)
            acc[s, k, here, :] = jnp.dot(weights, vbuf[s, k, here, :], preferred_element_type=F32)
            qs[s, k, here, :] = (q.astype(F32) * qsc[k]).astype(BF16)
            gs[s, k, here, :] = crow[k, pl.ds(0, 1), :] * (g * jax.nn.sigmoid(g))

    far_first = [(1, ny // 2)]
    for to in range(1, ny):
        if to != ny // 2:
            far_first.append((1, to))
    far_first += [(0, ny // 2), (1, 0)]
    for to in range(1, ny):
        if to != ny // 2:
            far_first.append((0, to))

    def state_out(s):
        for k in range(2):
            esend[s, k] = (smat[s, k, 0] * decay(k, float(BLOCK)) + smat[s, k, 1]).astype(BF16)
        for k, to in far_first:
            ycopy(s, k, (y + to) % ny).start()

        @pl.when(core == 0)
        def _():
            ycopy(s, 0, y).start()

        @pl.when(core == 1)
        def _():
            kept = esend[s, 0, pl.ds(pl.multiple_of(y * qr, qr), qr), :]
            ybuf[s, 2 * ny + y * 2 + half] = kept

    def owned_decay(i, count):
        return decay((2, 0)[i], count)

    def state_row(s):
        @pl.when(core == 1)
        def _():
            whole(ybuf.at[s, pl.ds(0, 4 * ny - 1)], ys.at[0], yr.at[s]).wait_recv()
            for i in range(2):
                step = owned_decay(i, float(span))
                total = ybuf[s, i * 2 * ny].astype(F32)
                for k in range(1, 2 * ny):
                    total = total * step + ybuf[s, i * 2 * ny + k].astype(F32)
                zsnd[s, i] = total.astype(BF16)

            @pl.loop(0, nz - 1 - z)
            def _(k):
                zcopy(s, nz - 1 - k).start()

    def state_back(s):
        @pl.when(core == 1)
        def _():
            steps = [owned_decay(i, float(span)) for i in range(2)]
            row_steps = [owned_decay(i, float(span * 2 * ny)) for i in range(2)]

            for count in range(1, nz):
                @pl.when(z == count)
                def _():
                    whole(zbuf.at[s, pl.ds(0, count)], zs.at[0], zr.at[s]).wait_recv()

            def add(frm, totals):
                return tuple(totals[i] * row_steps[i] + zbuf[s, frm, i].astype(F32) for i in range(2))

            zero = jnp.zeros((qr, HD), F32)
            carried = lax.fori_loop(0, z, add, (zero, zero))
            for i in range(2):
                total = carried[i]
                for k in range(2 * ny):
                    msnd[s, i * 2 * ny + k] = total.astype(BF16)
                    if k < 2 * ny - 1:
                        total = total * steps[i] + ybuf[s, i * 2 * ny + k].astype(F32)
            for k, to in far_first:
                for i in range(2):
                    mcopy(s, i, k, (y + to) % ny).start()
            mcopy(s, 0, 0, y).start()
            mbuf[s, 0, pl.ds(pl.multiple_of(y * qr, qr), qr), :] = msnd[s, 2 * ny + y * 2 + half]

    def read_out(s):
        @pl.when(core == 0)
        def _():
            whole(ybuf.at[s, pl.ds(0, 2 * ny)], ms.at[0], mr.at[s]).wait_recv()

        @pl.when(core == 1)
        def _():
            whole(ybuf.at[s, pl.ds(0, 2 * ny - 1)], ms.at[0], mr.at[s]).wait_recv()

        for k in range(2):
            memory = mbuf[s, k]
            for b in range(blocks):
                here = pl.ds(b * BLOCK, BLOCK)
                if b:
                    memory = (smat[s, k, 0] + memory.astype(F32) * decay(k, float(BLOCK))).astype(BF16)
                kept = acc[s, k, here, :] + jnp.dot(qs[s, k, here, :], memory, preferred_element_type=F32)
                kept = kept - jnp.mean(kept, axis=-1, keepdims=True)
                spread = jnp.mean(kept * kept, axis=-1, keepdims=True)
                kept = kept * lax.rsqrt(spread + GROUP_EPS) * gs[s, k, here, :]
                gsend[s, here, k * HD:(k + 1) * HD] = kept.astype(BF16)
        for to in (theirs * 2 + core, theirs * 2 + 1 - core, mine * 2 + 1 - core):
            acopy(s, to).start()
        own = gsend[s, pl.ds(pl.multiple_of(dl * rows, rows), rows), :]
        gat_of(s)[:, pl.ds(pl.multiple_of(dl * 2 * HD, 2 * HD), 2 * HD)] = own

    @pl.loop(0, nseq)
    def _(s):
        pass_recv(s, 0).wait_recv()
        keys(s, 0, mine, 1)
        queries(s, 0, mine, 1)

    @pl.when(even)
    def _():
        pl.semaphore_wait(ready_a, len(plane) + 2)
        tell(ready_b, beyond)

    @pl.when(odd)
    def _():
        pl.semaphore_wait(ready_a, len(plane))

    tell(ready_b, [(sp, partner)])

    def take_pair(s):
        own_recv(s).wait_recv()
        pass_send(s, 1).start()

    w_forward(0)
    own_send(2).start()
    w_forward(1)
    w_forward(2)
    take_pair(0)
    own_send(3).start()
    w_forward(3)
    pass_recv(0, 1).wait_recv()
    keys(0, 0, theirs, 1)
    w_forward(4)
    queries(0, 0, theirs, 1)
    w_forward(5)
    for i in range(2):
        whole(crow.at[1 + i], cs.at[0], cr.at[i]).wait_recv()
    head_tables(1)
    take_pair(1)
    w_forward(6)
    pass_recv(1, 1).wait_recv()
    keys(1, 0, theirs, 1)
    w_forward(7)
    @pl.when(even)
    def _():
        pl.semaphore_wait(ready_b, 3)
        tell(ready_c, beside)

    @pl.when(odd)
    def _():
        pl.semaphore_wait(ready_b, 1)

    w_rest(0).wait_recv()
    keys(0, 1, 0, 2)
    state_out(0)
    keys(1, 1, 0, 2)
    state_out(1)
    keys(2, 1, mine, 1)
    keys(3, 1, mine, 1)
    take_pair(2)
    queries(1, 0, theirs, 1)
    pass_recv(2, 1).wait_recv()
    keys(2, 0, theirs, 1)
    keys(2, 1, theirs, 1)
    state_out(2)
    @pl.when(odd)
    def _():
        pl.semaphore_wait(ready_c, 2)

    state_row(0)
    state_row(1)
    queries(2, 0, theirs, 1)
    take_pair(3)
    w_rest(1).wait_recv()
    queries(0, 1, 0, 2)
    pass_recv(3, 1).wait_recv()
    keys(3, 0, theirs, 1)
    keys(3, 1, theirs, 1)
    state_out(3)
    queries(1, 1, 0, 2)
    state_row(2)
    state_back(0)
    state_back(1)
    queries(2, 1, 0, 2)
    queries(3, 0, theirs, 1)
    state_row(3)
    state_back(2)
    queries(3, 1, 0, 2)
    state_back(3)
    read_out(0)
    read_out(1)
    read_out(2)
    ow_load.wait()
    pg_load.wait()
    read_out(3)
    whole(gat_early.at[:, 0:6 * HD], as_.at[0], ar.at[0]).wait_recv()
    osc[...] = jnp.dot(gat_early[...], oww[...], preferred_element_type=F32)
    scale_rows(osc, pg, mixed, 0, 2 * rows)
    whole(gat_late.at[:, 0:6 * HD], as_.at[0], ar.at[1]).wait_recv()

    whole(raw, xs.at[0], xr.at[0]).wait_send()
    whole(tok.at[:, 0:2 * rows, :], ps.at[0], pr.at[0, 0]).wait_send()
    whole(w.at[1, :, 0:quarter, :], wxs.at[0], wxr.at[0]).wait_send()
    whole(w.at[1, :, 0:3 * quarter, :], wfs.at[0], wfr.at[0]).wait_send()
    whole(crow.at[0:2], cs.at[0], cr.at[0]).wait_send()
    whole(gsend.at[:, pl.ds(0, 3 * rows), :], as_.at[0], ar.at[0]).wait_send()

    @pl.when(core == 0)
    def _():
        whole(ybuf.at[:, pl.ds(0, 2 * ny)], ys.at[0], yr.at[0]).wait_send()

    @pl.when(core == 1)
    def _():
        whole(ybuf.at[:, pl.ds(0, 2 * ny - 1)], ys.at[0], yr.at[0]).wait_send()
        whole(ybuf.at[:, pl.ds(0, 4 * ny - 1)], ms.at[0], mr.at[0]).wait_send()

        for count in range(1, nz):
            @pl.when(z == nz - 1 - count)
            def _():
                whole(zbuf.at[:, pl.ds(0, count)], zs.at[0], zr.at[0]).wait_send()


def mix_kernel(gat, oww, mixed, pg, out_ref, osc, late, sem):
    done = mixed.shape[0]
    first = pltpu.make_async_copy(mixed, out_ref.at[pl.ds(0, done), :], sem.at[0])
    first.start()
    osc[...] = jnp.dot(gat[...], oww[...], preferred_element_type=F32)
    part = late.shape[0] // 2
    copies = [first]
    for i in range(2):
        here = pl.ds(i * part, part)
        scale_rows(osc, pg, late, i * part, part)
        copies.append(pltpu.make_async_copy(late.at[here], out_ref.at[pl.ds(done + i * part, part), :], sem.at[1 + i]))
        copies[-1].start()
    for copy in copies:
        copy.wait()


def body(nz, ny, tokens, in_gain, wq, wk, wv, wg, log_decay, norm_gain, out_weight, post_gain):
    nseq, rows, width = tokens.shape
    ntp = 8
    stretch = rows * ntp
    half = stretch // 2
    tables = jnp.asarray(np.stack(rotary_tables(BLOCK)))
    qr = HD // ny
    vmem, hbm, smem = (pl.BlockSpec(memory_space=m) for m in (pltpu.VMEM, pltpu.HBM, pltpu.SMEM))
    dma = pltpu.SemaphoreType.DMA
    signal = pltpu.SemaphoreType.REGULAR
    scratch = [
        pltpu.VMEM((nseq, rows, width), BF16),
        pltpu.VMEM((nseq, half, width), BF16),
        pltpu.VMEM((2, 2, width, 2 * HD), BF16),
        pltpu.VMEM((1, width), F32),
        pltpu.VMEM((1, width), F32),
        pltpu.VMEM(tables.shape, F32),
        pltpu.VMEM((3, 8, HD), F32),
        pltpu.VMEM((2, BLOCK, HD), F32),
        pltpu.VMEM((2, BLOCK, HD), F32),
        pltpu.VMEM((2, BLOCK, HD), F32),
        pltpu.VMEM((2, BLOCK, HD), F32),
        pltpu.VMEM((2, BLOCK, HD), F32),
        pltpu.VMEM((nseq, 2, half, HD), BF16),
        pltpu.VMEM((nseq, 2, half, HD), BF16),
        pltpu.VMEM((nseq, 2, half, HD), BF16),
        pltpu.VMEM((nseq, 2, half, HD), F32),
        pltpu.VMEM((nseq, 2, half, HD), F32),
        pltpu.VMEM((nseq, 2, 2, HD, HD), F32),
        pltpu.VMEM((nseq, 2, HD, HD), BF16),
        pltpu.VMEM((nseq, 4 * ny, qr, HD), BF16),
        pltpu.VMEM((nseq, 2, qr, HD), BF16),
        pltpu.VMEM((nseq, nz, 2, qr, HD), BF16),
        pltpu.VMEM((nseq, 4 * ny, qr, HD), BF16),
        pltpu.VMEM((nseq, 2, HD, HD), BF16),
        pltpu.VMEM((nseq, half, 2 * HD), BF16),
        pltpu.VMEM((2 * rows, ntp * HD), BF16),
        pltpu.VMEM((2 * rows, width), F32),
        dma((11,)),
        dma((1,)), dma((nseq,)), dma((1,)), dma((nseq, 2)), dma((1,)), dma((8,)), dma((1,)), dma((2,)),
        dma((1,)), dma((2,)), dma((1,)), dma((nseq,)), dma((1,)), dma((nseq,)), dma((1,)), dma((nseq,)),
        dma((1,)), dma((2,)), signal, signal, signal,
    ]
    late = 2 * rows
    gain = post_gain.reshape(1, -1)
    gathered, weight, early = pl.pallas_call(
        functools.partial(kernel, nz, ny),
        out_shape=[
            pltpu.VMEM((late, ntp * HD), BF16), pltpu.VMEM(out_weight.shape, BF16), pltpu.VMEM((late, width), BF16)
        ],
        in_specs=[hbm] * 6 + [smem] + [hbm] * 4,
        out_specs=[vmem] * 3,
        scratch_shapes=scratch,
        name="retention",
        compiler_params=pltpu.CompilerParams(
            collective_id=0, has_side_effects=True, vmem_limit_bytes=VMEM_LIMIT
        ),
    )(
        tokens, in_gain.reshape(1, -1), wq, wk, wv, wg, log_decay, norm_gain.reshape(1, -1), out_weight, gain, tables,
    )
    mixed = pl.pallas_call(
        mix_kernel,
        out_shape=jax.ShapeDtypeStruct((nseq * rows, width), BF16),
        in_specs=[vmem] * 4,
        out_specs=hbm,
        scratch_shapes=[pltpu.VMEM((late, width), F32), pltpu.VMEM((late, width), BF16), dma((3,))],
        name="mix",
        compiler_params=pltpu.CompilerParams(vmem_limit_bytes=16 * 1024 * 1024),
    )(gathered, weight, early, gain)
    return mixed.reshape(tokens.shape)


def solution(mesh):
    both = ("sp", "tp")
    nz = mesh.shape["sp"] // NY
    return jax.shard_map(
        functools.partial(body, nz, NY),
        mesh=mesh,
        in_specs=(
            P(None, both, None), P(), P(None, "tp"), P(None, "tp"), P(None, "tp"), P(None, "tp"), P("tp"), P("tp"),
            P(), P(),
        ),
        out_specs=P(None, both, None),
        check_vma=False,
    )
```

```python
import functools

import jax
import jax.numpy as jnp
import numpy as np
from jax import lax
from jax.experimental import pallas as pl
from jax.experimental.pallas import tpu as pltpu
from jax.sharding import PartitionSpec as P

MESH = pl.DeviceIdType.MESH
F32 = jnp.float32
BF16 = jnp.bfloat16
HD = 128
BLOCK = 128
NY = 4
VMEM_LIMIT = 62_000_000
RMS_EPS = 1e-06
GROUP_EPS = 1e-05
ROPE_BASE = 10000.0


def rotary_tables(blocks):
    half = HD // 2
    rate = ROPE_BASE ** (-np.arange(half, dtype=np.float64) / half)
    rate = np.concatenate([rate, rate])
    inside = np.arange(BLOCK, dtype=np.float64)[:, None] * rate
    starts = BLOCK * np.arange(blocks, dtype=np.float64)[:, None] * rate
    tables = (np.cos(inside), np.sin(inside), np.cos(starts), np.sin(starts))
    return [t.astype(np.float32) for t in tables]


def row_scale(read, width):
    total = jnp.square(read(0))
    for c in range(1, width // HD):
        total += jnp.square(read(c))
    return lax.rsqrt(jnp.sum(total, axis=-1, keepdims=True) * (1.0 / width) + RMS_EPS)


def scale_rows(osc, pg, out, start, count):
    width = osc.shape[1]
    here = pl.ds(start, count)
    scale = row_scale(lambda c: osc[here, c * HD:(c + 1) * HD], width)
    for c in range(width // HD):
        cols = slice(c * HD, (c + 1) * HD)
        out[here, cols] = (osc[here, cols] * scale * pg[:, cols]).astype(BF16)


def kernel(
    nz, ny, tok_hbm, gain_hbm, wq, wk, wv, wg, ld_ref, ng_hbm, ow, pg_hbm, tab_hbm,
    gat_late, oww, mixed, raw, tok, w, gain, pg, tabs, crow, ctab, stab, dmat, qsc, ksc, kbuf, vbuf, qs, acc, gs, smat, esend, ybuf,
    zsnd, zbuf, msnd, mbuf, gsend, gat_early, osc, lsem, xs, xr, ps, pr, wxs, wxr, wfs, wfr, cs, cr, ys, yr, zs, zr, ms, mr, as_, ar,
    ready_a, ready_b, ready_c,
):
    nseq, rows, width = raw.shape
    ntp = 8
    nchip = ntp // 2
    blocks = 2
    span = blocks * BLOCK
    qr = HD // ny
    quarter = width // 4
    chunk = quarter // 4
    sp = lax.axis_index("sp")
    me = lax.axis_index("tp")
    z, y = sp // ny, sp % ny
    chip, core = me // 2, me % 2
    partner = chip * 2 + 1 - core
    half, dl = chip // 2, me % 4
    mine, theirs = chip % 2, 1 - chip % 2
    pair_same = (half * 2 + theirs) * 2 + core
    pair_other = (half * 2 + theirs) * 2 + 1 - core
    mate = (nchip - 1 - chip) * 2 + core
    owners = (chip * 2 + 1, (nchip - 1 - chip) * 2 + 1)

    def at(zz, yy):
        return (zz + nz) % nz * ny + (yy + ny) % ny

    barrier = pltpu.get_barrier_semaphore()
    plane = [(at(z, y + k), me) for k in range(1, ny)] + [(sp, mate), (sp, partner)]
    beside = [(at(z - 1, y), me), (at(z + 1, y), me)]
    beyond = [(at(z - 2, y), me), (at(z + 2, y), me)]
    peers = [(sp, pair_same), (sp, pair_other)] + plane
    even, odd = z % 2 == 0, z % 2 == 1

    def tell(sem, devs):
        for dev in devs:
            pl.semaphore_signal(sem, inc=1, device_id=dev, device_id_type=MESH)

    tell(barrier, peers)

    @pl.when(even)
    def _():
        tell(barrier, beside)

    raw_loads = [pltpu.make_async_copy(tok_hbm.at[s], raw.at[s], lsem.at[s]) for s in range(nseq)]
    gain_load = pltpu.make_async_copy(gain_hbm, gain, lsem.at[4])
    tab_load = pltpu.make_async_copy(tab_hbm, tabs, lsem.at[5])
    pg_load = pltpu.make_async_copy(pg_hbm, pg, lsem.at[7])
    ng_load = pltpu.make_async_copy(ng_hbm, crow.at[0, pl.ds(0, 1)], lsem.at[6])
    w_loads = [pltpu.make_async_copy(w.at[0, c], w.at[0, c], lsem.at[8 + c]) for c in range(2)]
    ow_load = pltpu.make_async_copy(oww, oww, lsem.at[10])
    raw_loads[0].start()
    gain_load.start()
    ng_load.start()
    for load in raw_loads[1:]:
        load.start()
    for j, src in enumerate((wk, wv, wq, wg)):
        cols = j % 2 * HD
        pltpu.make_async_copy(src, w.at[0, j // 2, :, cols:cols + HD], lsem.at[8 + j // 2]).start()
    tab_load.start()
    pg_load.start()
    for d in range(4):
        first = half * 4 + d
        second = (nchip - 1 - first // 2) * 2 + d % 2
        for i, h in enumerate((first, second)):
            src = ow.at[pl.ds(pl.multiple_of(h * HD, HD), HD), :]
            pltpu.make_async_copy(src, oww.at[(2 * d + i) * HD:(2 * d + i + 1) * HD, :], lsem.at[10]).start()

    def remote(src, dst, send, recv, dev):
        return pltpu.make_async_remote_copy(
            src_ref=src, dst_ref=dst, send_sem=send, recv_sem=recv, device_id=dev, device_id_type=MESH
        )

    def part_of(s, d):
        return tok.at[s, pl.ds(pl.multiple_of(d * rows, rows), rows), :]

    def own_send(s):
        ref = part_of(s, dl)
        return remote(ref, ref, xs.at[0], xr.at[s], (sp, pair_same))

    def own_recv(s):
        ref = part_of(s, theirs * 2 + core)
        return remote(ref, ref, xs.at[0], xr.at[s], (sp, pair_same))

    def pass_send(s, i):
        ref = part_of(s, (mine, theirs)[i] * 2 + core)
        return remote(ref, ref, ps.at[0], pr.at[s, i], (sp, partner))

    def pass_recv(s, i):
        ref = part_of(s, (mine, theirs)[i] * 2 + 1 - core)
        return remote(ref, ref, ps.at[0], pr.at[s, i], (sp, partner))

    my_quarter = (y % 2) * 2 + z % 2

    def w_rows(k, j):
        at_ = pl.multiple_of(my_quarter * quarter + j % 4 * chunk, chunk)
        return w.at[k, j // 4, pl.ds(at_, chunk), :]

    def w_send(j):
        return remote(w_rows(0, j), w_rows(1, j), wxs.at[0], wxr.at[j], (sp, mate))

    def w_recv(j):
        return remote(w_rows(1, j), w_rows(1, j), wxs.at[0], wxr.at[j], (sp, mate))

    def w_forward(j):
        w_recv(j).wait_recv()
        yy, zz = y + (1, -1)[j % 2], z + (1, -1)[j // 2 % 2]
        for dev in (at(zz, yy), at(z, yy), at(zz, y)):
            remote(w_rows(1, j), w_rows(1, j), wfs.at[0], wfr.at[j // 4], (dev, me)).start()

    def w_rest(c):
        ref = w.at[1, c, 0:3 * quarter, :]
        return remote(ref, ref, wfs.at[0], wfr.at[c], (sp, partner))

    def c_send(i):
        return remote(crow.at[0], crow.at[1 + i], cs.at[0], cr.at[i], (sp, (mate, partner)[i]))

    def ycopy(s, k, to):
        src = esend.at[s, k, pl.ds(pl.multiple_of(to * qr, qr), qr), :]
        dst = ybuf.at[s, core * 2 * ny + y * 2 + half]
        return remote(src, dst, ys.at[0], yr.at[s], (at(z, to), owners[k]))

    def zcopy(s, to):
        return remote(zsnd.at[s], zbuf.at[s, z], zs.at[0], zr.at[s], (to * ny + y, me))

    def mcopy(s, i, k, to):
        src = msnd.at[s, i * 2 * ny + to * 2 + (half, 1 - half)[k]]
        dst = mbuf.at[s, k, pl.ds(pl.multiple_of(y * qr, qr), qr), :]
        return remote(src, dst, ms.at[0], mr.at[s], (at(z, to), owners[k] - 1 + i))

    def gat_of(s):
        return (gat_early, gat_late)[s // 2].at[pl.ds(s % 2 * rows, rows), :]

    def acopy(s, to):
        src = gsend.at[s, pl.ds(pl.multiple_of(to * rows, rows), rows), :]
        dst = gat_of(s).at[:, pl.ds(pl.multiple_of(dl * 2 * HD, 2 * HD), 2 * HD)]
        return remote(src, dst, as_.at[0], ar.at[s // 2], (sp, half * 4 + to))

    def whole(ref, send, recv):
        return remote(ref, ref, send, recv, (sp, partner))

    def norm_own(s):
        raw_loads[s].wait()
        scale = row_scale(lambda c: raw[s, :, c * HD:(c + 1) * HD].astype(F32), width)
        here = pl.ds(pl.multiple_of(dl * rows, rows), rows)
        for c in range(width // HD):
            cols = slice(c * HD, (c + 1) * HD)
            v = raw[s, :, cols].astype(F32)
            tok[s, here, cols] = (v * scale * gain[:, cols]).astype(BF16)

    gain_load.wait()
    norm_own(0)
    ng_load.wait()
    crow[0, pl.ds(1, 7), :] = jnp.full((7, HD), ld_ref[0], F32)

    @pl.when(even)
    def _():
        pl.semaphore_wait(barrier, len(peers))

    @pl.when(odd)
    def _():
        pl.semaphore_wait(barrier, len(peers) + 2)

    own_send(0).start()
    pass_send(0, 0).start()
    tell(ready_a, plane)

    @pl.when(odd)
    def _():
        tell(ready_a, beside)

    c_send(0).start()
    c_send(1).start()
    for c in range(2):
        w_loads[c].wait()
        for j in range(4 * c, 4 * c + 4):
            w_send(j).start()
    for s in range(1, nseq):
        norm_own(s)
        if s == 1:
            own_send(s).start()
        pass_send(s, 0).start()

    i_col = lax.broadcasted_iota(jnp.int32, (BLOCK, HD), 0).astype(F32)
    i_row = lax.broadcasted_iota(jnp.int32, (BLOCK, HD), 1).astype(F32)

    def decay(k, count):
        return jnp.exp(crow[k, pl.ds(1, 1), :] * count)

    def head_tables(k):
        ld = crow[k, pl.ds(1, 1), :]
        dist = i_col - i_row
        dmat[k] = jnp.where(dist >= 0, jnp.exp(ld * jnp.maximum(dist, 0.0)), 0.0)
        qsc[k] = jnp.exp(ld * (i_col + 1.0))
        ksc[k] = jnp.exp(ld * (BLOCK - 1.0 - i_col))

    head_tables(0)
    tab_load.wait()
    sign = jnp.where(i_row < HD // 2, -1.0, 1.0)
    for b in range(blocks):
        start = sp * nchip + half * blocks + b
        cb = tabs[2, pl.ds(start, 1), :]
        sb = tabs[3, pl.ds(start, 1), :]
        ctab[b] = tabs[0] * cb - tabs[1] * sb
        stab[b] = (tabs[1] * cb + tabs[0] * sb) * sign

    def rotate(u, b):
        return u * ctab[b] + pltpu.roll(u, HD // 2, 1) * stab[b]

    def tokens_of(s, b0, nb):
        return tok[s, pl.ds(pl.multiple_of(b0 * BLOCK, BLOCK), nb * BLOCK), :]

    def block_at(b):
        return pl.ds(pl.multiple_of(b * BLOCK, BLOCK), BLOCK)

    def keys(s, k, b0, nb):
        proj = jnp.dot(tokens_of(s, b0, nb), w[k, 0], preferred_element_type=F32).astype(BF16)
        for i in range(nb):
            b = b0 + i
            here = block_at(b)
            p = proj[i * BLOCK:(i + 1) * BLOCK]
            kk = (rotate(p[:, :HD].astype(F32), b) * HD ** -0.5).astype(BF16)
            v = p[:, HD:]
            kbuf[s, k, here, :] = kk
            vbuf[s, k, here, :] = v
            ks = (kk.astype(F32) * ksc[k]).astype(BF16)
            smat[s, k, b] = lax.dot_general(ks, v, (((0,), (0,)), ((), ())), preferred_element_type=F32)

    def queries(s, k, b0, nb):
        proj = jnp.dot(tokens_of(s, b0, nb), w[k, 1], preferred_element_type=F32).astype(BF16)
        for i in range(nb):
            b = b0 + i
            here = block_at(b)
            p = proj[i * BLOCK:(i + 1) * BLOCK]
            q = rotate(p[:, :HD].astype(F32), b).astype(BF16)
            g = p[:, HD:].astype(F32)
            scores = lax.dot_general(q, kbuf[s, k, here, :], (((1,), (1,)), ((), ())), preferred_element_type=F32)
            weights = (scores * dmat[k]).astype(BF16)
            acc[s, k, here, :] = jnp.dot(weights, vbuf[s, k, here, :], preferred_element_type=F32)
            qs[s, k, here, :] = (q.astype(F32) * qsc[k]).astype(BF16)
            gs[s, k, here, :] = crow[k, pl.ds(0, 1), :] * (g * jax.nn.sigmoid(g))

    far_first = [(1, ny // 2)]
    for to in range(1, ny):
        if to != ny // 2:
            far_first.append((1, to))
    far_first += [(0, ny // 2), (1, 0)]
    for to in range(1, ny):
        if to != ny // 2:
            far_first.append((0, to))

    def state_out(s):
        for k in range(2):
            esend[s, k] = (smat[s, k, 0] * decay(k, float(BLOCK)) + smat[s, k, 1]).astype(BF16)
        for k, to in far_first:
            ycopy(s, k, (y + to) % ny).start()

        @pl.when(core == 0)
        def _():
            ycopy(s, 0, y).start()

        @pl.when(core == 1)
        def _():
            kept = esend[s, 0, pl.ds(pl.multiple_of(y * qr, qr), qr), :]
            ybuf[s, 2 * ny + y * 2 + half] = kept

    def owned_decay(i, count):
        return decay((2, 0)[i], count)

    def state_row(s):
        @pl.when(core == 1)
        def _():
            whole(ybuf.at[s, pl.ds(0, 4 * ny - 1)], ys.at[0], yr.at[s]).wait_recv()
            for i in range(2):
                step = owned_decay(i, float(span))
                total = ybuf[s, i * 2 * ny].astype(F32)
                for k in range(1, 2 * ny):
                    total = total * step + ybuf[s, i * 2 * ny + k].astype(F32)
                zsnd[s, i] = total.astype(BF16)

            @pl.loop(0, nz - 1 - z)
            def _(k):
                zcopy(s, nz - 1 - k).start()

    def state_back(s):
        @pl.when(core == 1)
        def _():
            steps = [owned_decay(i, float(span)) for i in range(2)]
            row_steps = [owned_decay(i, float(span * 2 * ny)) for i in range(2)]

            for count in range(1, nz):
                @pl.when(z == count)
                def _():
                    whole(zbuf.at[s, pl.ds(0, count)], zs.at[0], zr.at[s]).wait_recv()

            def add(frm, totals):
                return tuple(totals[i] * row_steps[i] + zbuf[s, frm, i].astype(F32) for i in range(2))

            zero = jnp.zeros((qr, HD), F32)
            carried = lax.fori_loop(0, z, add, (zero, zero))
            for i in range(2):
                total = carried[i]
                for k in range(2 * ny):
                    msnd[s, i * 2 * ny + k] = total.astype(BF16)
                    if k < 2 * ny - 1:
                        total = total * steps[i] + ybuf[s, i * 2 * ny + k].astype(F32)
            for k, to in far_first:
                for i in range(2):
                    mcopy(s, i, k, (y + to) % ny).start()
            mcopy(s, 0, 0, y).start()
            mbuf[s, 0, pl.ds(pl.multiple_of(y * qr, qr), qr), :] = msnd[s, 2 * ny + y * 2 + half]

    def read_out(s):
        @pl.when(core == 0)
        def _():
            whole(ybuf.at[s, pl.ds(0, 2 * ny)], ms.at[0], mr.at[s]).wait_recv()

        @pl.when(core == 1)
        def _():
            whole(ybuf.at[s, pl.ds(0, 2 * ny - 1)], ms.at[0], mr.at[s]).wait_recv()

        for k in range(2):
            memory = mbuf[s, k]
            for b in range(blocks):
                here = pl.ds(b * BLOCK, BLOCK)
                if b:
                    memory = (smat[s, k, 0] + memory.astype(F32) * decay(k, float(BLOCK))).astype(BF16)
                kept = acc[s, k, here, :] + jnp.dot(qs[s, k, here, :], memory, preferred_element_type=F32)
                kept = kept - jnp.mean(kept, axis=-1, keepdims=True)
                spread = jnp.mean(kept * kept, axis=-1, keepdims=True)
                kept = kept * lax.rsqrt(spread + GROUP_EPS) * gs[s, k, here, :]
                gsend[s, here, k * HD:(k + 1) * HD] = kept.astype(BF16)
        for to in (theirs * 2 + core, theirs * 2 + 1 - core, mine * 2 + 1 - core):
            acopy(s, to).start()
        own = gsend[s, pl.ds(pl.multiple_of(dl * rows, rows), rows), :]
        gat_of(s)[:, pl.ds(pl.multiple_of(dl * 2 * HD, 2 * HD), 2 * HD)] = own

    @pl.loop(0, nseq)
    def _(s):
        pass_recv(s, 0).wait_recv()
        keys(s, 0, mine, 1)
        queries(s, 0, mine, 1)

    @pl.when(even)
    def _():
        pl.semaphore_wait(ready_a, len(plane) + 2)
        tell(ready_b, beyond)

    @pl.when(odd)
    def _():
        pl.semaphore_wait(ready_a, len(plane))

    tell(ready_b, [(sp, partner)])

    def take_pair(s):
        own_recv(s).wait_recv()
        pass_send(s, 1).start()

    w_forward(0)
    own_send(2).start()
    w_forward(1)
    w_forward(2)
    take_pair(0)
    @pl.when(core == 0)
    def _():
        own_send(3).start()

    w_forward(3)
    pass_recv(0, 1).wait_recv()
    keys(0, 0, theirs, 1)
    w_forward(4)
    queries(0, 0, theirs, 1)
    w_forward(5)
    for i in range(2):
        whole(crow.at[1 + i], cs.at[0], cr.at[i]).wait_recv()
    head_tables(1)
    take_pair(1)
    w_forward(6)
    pass_recv(1, 1).wait_recv()
    keys(1, 0, theirs, 1)
    w_forward(7)
    @pl.when(even)
    def _():
        pl.semaphore_wait(ready_b, 3)
        tell(ready_c, beside)

    @pl.when(odd)
    def _():
        pl.semaphore_wait(ready_b, 1)

    w_rest(0).wait_recv()
    keys(0, 1, 0, 2)
    state_out(0)

    @pl.when(core == 1)
    def _():
        own_send(3).start()

    keys(1, 1, 0, 2)
    state_out(1)
    keys(2, 1, mine, 1)
    keys(3, 1, mine, 1)
    take_pair(2)
    queries(1, 0, theirs, 1)
    pass_recv(2, 1).wait_recv()
    keys(2, 0, theirs, 1)
    keys(2, 1, theirs, 1)
    state_out(2)
    @pl.when(odd)
    def _():
        pl.semaphore_wait(ready_c, 2)

    state_row(0)
    state_row(1)
    queries(2, 0, theirs, 1)
    take_pair(3)
    w_rest(1).wait_recv()
    queries(0, 1, 0, 2)
    pass_recv(3, 1).wait_recv()
    keys(3, 0, theirs, 1)
    keys(3, 1, theirs, 1)
    state_out(3)
    queries(1, 1, 0, 2)
    state_row(2)
    state_back(0)
    state_back(1)
    queries(2, 1, 0, 2)
    queries(3, 0, theirs, 1)
    state_row(3)
    state_back(2)
    queries(3, 1, 0, 2)
    state_back(3)
    read_out(0)
    read_out(1)
    read_out(2)
    ow_load.wait()
    pg_load.wait()
    read_out(3)
    whole(gat_early.at[:, 0:6 * HD], as_.at[0], ar.at[0]).wait_recv()
    osc[...] = jnp.dot(gat_early[...], oww[...], preferred_element_type=F32)
    scale_rows(osc, pg, mixed, 0, 2 * rows)
    whole(gat_late.at[:, 0:6 * HD], as_.at[0], ar.at[1]).wait_recv()

    whole(raw, xs.at[0], xr.at[0]).wait_send()
    whole(tok.at[:, 0:2 * rows, :], ps.at[0], pr.at[0, 0]).wait_send()
    whole(w.at[1, :, 0:quarter, :], wxs.at[0], wxr.at[0]).wait_send()
    whole(w.at[1, :, 0:3 * quarter, :], wfs.at[0], wfr.at[0]).wait_send()
    whole(crow.at[0:2], cs.at[0], cr.at[0]).wait_send()
    whole(gsend.at[:, pl.ds(0, 3 * rows), :], as_.at[0], ar.at[0]).wait_send()

    @pl.when(core == 0)
    def _():
        whole(ybuf.at[:, pl.ds(0, 2 * ny)], ys.at[0], yr.at[0]).wait_send()

    @pl.when(core == 1)
    def _():
        whole(ybuf.at[:, pl.ds(0, 2 * ny - 1)], ys.at[0], yr.at[0]).wait_send()
        whole(ybuf.at[:, pl.ds(0, 4 * ny - 1)], ms.at[0], mr.at[0]).wait_send()

        for count in range(1, nz):
            @pl.when(z == nz - 1 - count)
            def _():
                whole(zbuf.at[:, pl.ds(0, count)], zs.at[0], zr.at[0]).wait_send()


def mix_kernel(gat, oww, mixed, pg, out_ref, osc, late, sem):
    done = mixed.shape[0]
    first = pltpu.make_async_copy(mixed, out_ref.at[pl.ds(0, done), :], sem.at[0])
    first.start()
    osc[...] = jnp.dot(gat[...], oww[...], preferred_element_type=F32)
    part = late.shape[0] // 2
    copies = [first]
    for i in range(2):
        here = pl.ds(i * part, part)
        scale_rows(osc, pg, late, i * part, part)
        copies.append(pltpu.make_async_copy(late.at[here], out_ref.at[pl.ds(done + i * part, part), :], sem.at[1 + i]))
        copies[-1].start()
    for copy in copies:
        copy.wait()


def body(nz, ny, tokens, in_gain, wq, wk, wv, wg, log_decay, norm_gain, out_weight, post_gain):
    nseq, rows, width = tokens.shape
    ntp = 8
    stretch = rows * ntp
    half = stretch // 2
    tables = jnp.asarray(np.stack(rotary_tables(BLOCK)))
    qr = HD // ny
    vmem, hbm, smem = (pl.BlockSpec(memory_space=m) for m in (pltpu.VMEM, pltpu.HBM, pltpu.SMEM))
    dma = pltpu.SemaphoreType.DMA
    signal = pltpu.SemaphoreType.REGULAR
    scratch = [
        pltpu.VMEM((nseq, rows, width), BF16),
        pltpu.VMEM((nseq, half, width), BF16),
        pltpu.VMEM((2, 2, width, 2 * HD), BF16),
        pltpu.VMEM((1, width), F32),
        pltpu.VMEM((1, width), F32),
        pltpu.VMEM(tables.shape, F32),
        pltpu.VMEM((3, 8, HD), F32),
        pltpu.VMEM((2, BLOCK, HD), F32),
        pltpu.VMEM((2, BLOCK, HD), F32),
        pltpu.VMEM((2, BLOCK, HD), F32),
        pltpu.VMEM((2, BLOCK, HD), F32),
        pltpu.VMEM((2, BLOCK, HD), F32),
        pltpu.VMEM((nseq, 2, half, HD), BF16),
        pltpu.VMEM((nseq, 2, half, HD), BF16),
        pltpu.VMEM((nseq, 2, half, HD), BF16),
        pltpu.VMEM((nseq, 2, half, HD), F32),
        pltpu.VMEM((nseq, 2, half, HD), F32),
        pltpu.VMEM((nseq, 2, 2, HD, HD), F32),
        pltpu.VMEM((nseq, 2, HD, HD), BF16),
        pltpu.VMEM((nseq, 4 * ny, qr, HD), BF16),
        pltpu.VMEM((nseq, 2, qr, HD), BF16),
        pltpu.VMEM((nseq, nz, 2, qr, HD), BF16),
        pltpu.VMEM((nseq, 4 * ny, qr, HD), BF16),
        pltpu.VMEM((nseq, 2, HD, HD), BF16),
        pltpu.VMEM((nseq, half, 2 * HD), BF16),
        pltpu.VMEM((2 * rows, ntp * HD), BF16),
        pltpu.VMEM((2 * rows, width), F32),
        dma((11,)),
        dma((1,)), dma((nseq,)), dma((1,)), dma((nseq, 2)), dma((1,)), dma((8,)), dma((1,)), dma((2,)),
        dma((1,)), dma((2,)), dma((1,)), dma((nseq,)), dma((1,)), dma((nseq,)), dma((1,)), dma((nseq,)),
        dma((1,)), dma((2,)), signal, signal, signal,
    ]
    late = 2 * rows
    gain = post_gain.reshape(1, -1)
    gathered, weight, early = pl.pallas_call(
        functools.partial(kernel, nz, ny),
        out_shape=[
            pltpu.VMEM((late, ntp * HD), BF16), pltpu.VMEM(out_weight.shape, BF16), pltpu.VMEM((late, width), BF16)
        ],
        in_specs=[hbm] * 6 + [smem] + [hbm] * 4,
        out_specs=[vmem] * 3,
        scratch_shapes=scratch,
        name="retention",
        compiler_params=pltpu.CompilerParams(
            collective_id=0, has_side_effects=True, vmem_limit_bytes=VMEM_LIMIT
        ),
    )(
        tokens, in_gain.reshape(1, -1), wq, wk, wv, wg, log_decay, norm_gain.reshape(1, -1), out_weight, gain, tables,
    )
    mixed = pl.pallas_call(
        mix_kernel,
        out_shape=jax.ShapeDtypeStruct((nseq * rows, width), BF16),
        in_specs=[vmem] * 4,
        out_specs=hbm,
        scratch_shapes=[pltpu.VMEM((late, width), F32), pltpu.VMEM((late, width), BF16), dma((3,))],
        name="mix",
        compiler_params=pltpu.CompilerParams(vmem_limit_bytes=16 * 1024 * 1024),
    )(gathered, weight, early, gain)
    return mixed.reshape(tokens.shape)


def solution(mesh):
    both = ("sp", "tp")
    nz = mesh.shape["sp"] // NY
    return jax.shard_map(
        functools.partial(body, nz, NY),
        mesh=mesh,
        in_specs=(
            P(None, both, None), P(), P(None, "tp"), P(None, "tp"), P(None, "tp"), P(None, "tp"), P("tp"), P("tp"),
            P(), P(),
        ),
        out_specs=P(None, both, None),
        check_vma=False,
    )
```

```python
import functools

import jax
import jax.numpy as jnp
import numpy as np
from jax import lax
from jax.experimental import pallas as pl
from jax.experimental.pallas import tpu as pltpu
from jax.sharding import PartitionSpec as P

MESH = pl.DeviceIdType.MESH
F32 = jnp.float32
BF16 = jnp.bfloat16
HD = 128
BLOCK = 128
NY = 4
VMEM_LIMIT = 62_000_000
RMS_EPS = 1e-06
GROUP_EPS = 1e-05
ROPE_BASE = 10000.0


def rotary_tables(blocks):
    half = HD // 2
    rate = ROPE_BASE ** (-np.arange(half, dtype=np.float64) / half)
    rate = np.concatenate([rate, rate])
    inside = np.arange(BLOCK, dtype=np.float64)[:, None] * rate
    starts = BLOCK * np.arange(blocks, dtype=np.float64)[:, None] * rate
    tables = (np.cos(inside), np.sin(inside), np.cos(starts), np.sin(starts))
    return [t.astype(np.float32) for t in tables]


def row_scale(read, width):
    total = jnp.square(read(0))
    for c in range(1, width // HD):
        total += jnp.square(read(c))
    return lax.rsqrt(jnp.sum(total, axis=-1, keepdims=True) * (1.0 / width) + RMS_EPS)


def scale_rows(osc, pg, out, start, count):
    width = osc.shape[1]
    here = pl.ds(start, count)
    scale = row_scale(lambda c: osc[here, c * HD:(c + 1) * HD], width)
    for c in range(width // HD):
        cols = slice(c * HD, (c + 1) * HD)
        out[here, cols] = (osc[here, cols] * scale * pg[:, cols]).astype(BF16)


def kernel(
    nz, ny, tok_hbm, gain_hbm, wq, wk, wv, wg, ld_ref, ng_hbm, ow, pg_hbm, tab_hbm,
    gat_late, oww, mixed, raw, tok, w, gain, pg, tabs, crow, ctab, stab, dmat, qsc, ksc, kbuf, vbuf, qs, acc, gs, smat, esend, ybuf,
    zsnd, zbuf, msnd, mbuf, gsend, gat_early, osc, lsem, xs, xr, ps, pr, wxs, wxr, wfs, wfr, cs, cr, ys, yr, zs, zr, ms, mr, as_, ar,
    ready_a, ready_b, ready_c,
):
    nseq, rows, width = raw.shape
    ntp = 8
    nchip = ntp // 2
    blocks = 2
    span = blocks * BLOCK
    qr = HD // ny
    quarter = width // 4
    chunk = quarter // 4
    sp = lax.axis_index("sp")
    me = lax.axis_index("tp")
    z, y = sp // ny, sp % ny
    chip, core = me // 2, me % 2
    partner = chip * 2 + 1 - core
    half, dl = chip // 2, me % 4
    mine, theirs = chip % 2, 1 - chip % 2
    pair_same = (half * 2 + theirs) * 2 + core
    pair_other = (half * 2 + theirs) * 2 + 1 - core
    mate = (nchip - 1 - chip) * 2 + core
    owners = (chip * 2 + 1, (nchip - 1 - chip) * 2 + 1)

    def at(zz, yy):
        return (zz + nz) % nz * ny + (yy + ny) % ny

    barrier = pltpu.get_barrier_semaphore()
    plane = [(at(z, y + k), me) for k in range(1, ny)] + [(sp, mate), (sp, partner)]
    beside = [(at(z - 1, y), me), (at(z + 1, y), me)]
    beyond = [(at(z - 2, y), me), (at(z + 2, y), me)]
    peers = [(sp, pair_same), (sp, pair_other)] + plane
    even, odd = z % 2 == 0, z % 2 == 1

    def tell(sem, devs):
        for dev in devs:
            pl.semaphore_signal(sem, inc=1, device_id=dev, device_id_type=MESH)

    tell(barrier, peers)

    @pl.when(even)
    def _():
        tell(barrier, beside)

    raw_loads = [pltpu.make_async_copy(tok_hbm.at[s], raw.at[s], lsem.at[s]) for s in range(nseq)]
    gain_load = pltpu.make_async_copy(gain_hbm, gain, lsem.at[4])
    tab_load = pltpu.make_async_copy(tab_hbm, tabs, lsem.at[5])
    pg_load = pltpu.make_async_copy(pg_hbm, pg, lsem.at[7])
    ng_load = pltpu.make_async_copy(ng_hbm, crow.at[0, pl.ds(0, 1)], lsem.at[6])
    w_loads = [pltpu.make_async_copy(w.at[0, c], w.at[0, c], lsem.at[8 + c]) for c in range(2)]
    ow_load = pltpu.make_async_copy(oww, oww, lsem.at[10])
    raw_loads[0].start()
    gain_load.start()
    ng_load.start()
    for load in raw_loads[1:]:
        load.start()
    for j, src in enumerate((wk, wv, wq, wg)):
        cols = j % 2 * HD
        pltpu.make_async_copy(src, w.at[0, j // 2, :, cols:cols + HD], lsem.at[8 + j // 2]).start()
    tab_load.start()
    pg_load.start()
    for d in range(4):
        first = half * 4 + d
        second = (nchip - 1 - first // 2) * 2 + d % 2
        for i, h in enumerate((first, second)):
            src = ow.at[pl.ds(pl.multiple_of(h * HD, HD), HD), :]
            pltpu.make_async_copy(src, oww.at[(2 * d + i) * HD:(2 * d + i + 1) * HD, :], lsem.at[10]).start()

    def remote(src, dst, send, recv, dev):
        return pltpu.make_async_remote_copy(
            src_ref=src, dst_ref=dst, send_sem=send, recv_sem=recv, device_id=dev, device_id_type=MESH
        )

    def part_of(s, d):
        return tok.at[s, pl.ds(pl.multiple_of(d * rows, rows), rows), :]

    def own_send(s):
        ref = part_of(s, dl)
        return remote(ref, ref, xs.at[0], xr.at[s], (sp, pair_same))

    def own_recv(s):
        ref = part_of(s, theirs * 2 + core)
        return remote(ref, ref, xs.at[0], xr.at[s], (sp, pair_same))

    def pass_send(s, i):
        ref = part_of(s, (mine, theirs)[i] * 2 + core)
        return remote(ref, ref, ps.at[0], pr.at[s, i], (sp, partner))

    def pass_recv(s, i):
        ref = part_of(s, (mine, theirs)[i] * 2 + 1 - core)
        return remote(ref, ref, ps.at[0], pr.at[s, i], (sp, partner))

    my_quarter = (y % 2) * 2 + z % 2

    def w_rows(k, j):
        at_ = pl.multiple_of(my_quarter * quarter + j % 4 * chunk, chunk)
        return w.at[k, j // 4, pl.ds(at_, chunk), :]

    def w_send(j):
        return remote(w_rows(0, j), w_rows(1, j), wxs.at[0], wxr.at[j], (sp, mate))

    def w_recv(j):
        return remote(w_rows(1, j), w_rows(1, j), wxs.at[0], wxr.at[j], (sp, mate))

    def w_forward(j):
        w_recv(j).wait_recv()
        yy, zz = y + (1, -1)[j % 2], z + (1, -1)[j // 2 % 2]
        for dev in (at(zz, yy), at(z, yy), at(zz, y)):
            remote(w_rows(1, j), w_rows(1, j), wfs.at[0], wfr.at[j // 4], (dev, me)).start()

    def w_rest(c):
        ref = w.at[1, c, 0:3 * quarter, :]
        return remote(ref, ref, wfs.at[0], wfr.at[c], (sp, partner))

    def c_send(i):
        return remote(crow.at[0], crow.at[1 + i], cs.at[0], cr.at[i], (sp, (mate, partner)[i]))

    def ycopy(s, k, to):
        src = esend.at[s, k, pl.ds(pl.multiple_of(to * qr, qr), qr), :]
        dst = ybuf.at[s, core * 2 * ny + y * 2 + half]
        return remote(src, dst, ys.at[0], yr.at[s], (at(z, to), owners[k]))

    def zcopy(s, to):
        return remote(zsnd.at[s], zbuf.at[s, z], zs.at[0], zr.at[s], (to * ny + y, me))

    def mcopy(s, i, k, to):
        src = msnd.at[s, i * 2 * ny + to * 2 + (half, 1 - half)[k]]
        dst = mbuf.at[s, k, pl.ds(pl.multiple_of(y * qr, qr), qr), :]
        return remote(src, dst, ms.at[0], mr.at[s], (at(z, to), owners[k] - 1 + i))

    def gat_of(s):
        return (gat_early, gat_late)[s // 2].at[pl.ds(s % 2 * rows, rows), :]

    def acopy(s, to):
        src = gsend.at[s, pl.ds(pl.multiple_of(to * rows, rows), rows), :]
        dst = gat_of(s).at[:, pl.ds(pl.multiple_of(dl * 2 * HD, 2 * HD), 2 * HD)]
        return remote(src, dst, as_.at[0], ar.at[s // 2], (sp, half * 4 + to))

    def whole(ref, send, recv):
        return remote(ref, ref, send, recv, (sp, partner))

    def norm_own(s):
        raw_loads[s].wait()
        scale = row_scale(lambda c: raw[s, :, c * HD:(c + 1) * HD].astype(F32), width)
        here = pl.ds(pl.multiple_of(dl * rows, rows), rows)
        for c in range(width // HD):
            cols = slice(c * HD, (c + 1) * HD)
            v = raw[s, :, cols].astype(F32)
            tok[s, here, cols] = (v * scale * gain[:, cols]).astype(BF16)

    gain_load.wait()
    norm_own(0)
    ng_load.wait()
    crow[0, pl.ds(1, 7), :] = jnp.full((7, HD), ld_ref[0], F32)

    @pl.when(even)
    def _():
        pl.semaphore_wait(barrier, len(peers))

    @pl.when(odd)
    def _():
        pl.semaphore_wait(barrier, len(peers) + 2)

    own_send(0).start()
    pass_send(0, 0).start()
    tell(ready_a, plane)

    @pl.when(odd)
    def _():
        tell(ready_a, beside)

    c_send(0).start()
    c_send(1).start()
    for c in range(2):
        w_loads[c].wait()
        for j in range(4 * c, 4 * c + 4):
            w_send(j).start()
    for s in range(1, nseq):
        norm_own(s)
        if s == 1:
            own_send(s).start()
        pass_send(s, 0).start()

    i_col = lax.broadcasted_iota(jnp.int32, (BLOCK, HD), 0).astype(F32)
    i_row = lax.broadcasted_iota(jnp.int32, (BLOCK, HD), 1).astype(F32)

    def decay(k, count):
        return jnp.exp(crow[k, pl.ds(1, 1), :] * count)

    def head_tables(k):
        ld = crow[k, pl.ds(1, 1), :]
        dist = i_col - i_row
        dmat[k] = jnp.where(dist >= 0, jnp.exp(ld * jnp.maximum(dist, 0.0)), 0.0)
        qsc[k] = jnp.exp(ld * (i_col + 1.0))
        ksc[k] = jnp.exp(ld * (BLOCK - 1.0 - i_col))

    head_tables(0)
    tab_load.wait()
    sign = jnp.where(i_row < HD // 2, -1.0, 1.0)
    for b in range(blocks):
        start = sp * nchip + half * blocks + b
        cb = tabs[2, pl.ds(start, 1), :]
        sb = tabs[3, pl.ds(start, 1), :]
        ctab[b] = tabs[0] * cb - tabs[1] * sb
        stab[b] = (tabs[1] * cb + tabs[0] * sb) * sign

    def rotate(u, b):
        return u * ctab[b] + pltpu.roll(u, HD // 2, 1) * stab[b]

    def tokens_of(s, b0, nb):
        return tok[s, pl.ds(pl.multiple_of(b0 * BLOCK, BLOCK), nb * BLOCK), :]

    def block_at(b):
        return pl.ds(pl.multiple_of(b * BLOCK, BLOCK), BLOCK)

    def keys(s, k, b0, nb):
        proj = jnp.dot(tokens_of(s, b0, nb), w[k, 0], preferred_element_type=F32).astype(BF16)
        for i in range(nb):
            b = b0 + i
            here = block_at(b)
            p = proj[i * BLOCK:(i + 1) * BLOCK]
            kk = (rotate(p[:, :HD].astype(F32), b) * HD ** -0.5).astype(BF16)
            v = p[:, HD:]
            kbuf[s, k, here, :] = kk
            vbuf[s, k, here, :] = v
            ks = (kk.astype(F32) * ksc[k]).astype(BF16)
            smat[s, k, b] = lax.dot_general(ks, v, (((0,), (0,)), ((), ())), preferred_element_type=F32)

    def queries(s, k, b0, nb):
        proj = jnp.dot(tokens_of(s, b0, nb), w[k, 1], preferred_element_type=F32).astype(BF16)
        for i in range(nb):
            b = b0 + i
            here = block_at(b)
            p = proj[i * BLOCK:(i + 1) * BLOCK]
            q = rotate(p[:, :HD].astype(F32), b).astype(BF16)
            g = p[:, HD:].astype(F32)
            scores = lax.dot_general(q, kbuf[s, k, here, :], (((1,), (1,)), ((), ())), preferred_element_type=F32)
            weights = (scores * dmat[k]).astype(BF16)
            acc[s, k, here, :] = jnp.dot(weights, vbuf[s, k, here, :], preferred_element_type=F32)
            qs[s, k, here, :] = (q.astype(F32) * qsc[k]).astype(BF16)
            gs[s, k, here, :] = crow[k, pl.ds(0, 1), :] * (g * jax.nn.sigmoid(g))

    far_first = [(1, ny // 2)]
    for to in range(1, ny):
        if to != ny // 2:
            far_first.append((1, to))
    far_first += [(0, ny // 2), (1, 0)]
    for to in range(1, ny):
        if to != ny // 2:
            far_first.append((0, to))

    def state_head(s, k):
        esend[s, k] = (smat[s, k, 0] * decay(k, float(BLOCK)) + smat[s, k, 1]).astype(BF16)
        for head, to in far_first:
            if head == k:
                ycopy(s, k, (y + to) % ny).start()

    def state_out(s, last=False):
        if not last:
            state_head(s, 1)
        state_head(s, 0)

        @pl.when(core == 0)
        def _():
            ycopy(s, 0, y).start()

        @pl.when(core == 1)
        def _():
            kept = esend[s, 0, pl.ds(pl.multiple_of(y * qr, qr), qr), :]
            ybuf[s, 2 * ny + y * 2 + half] = kept

    def owned_decay(i, count):
        return decay((2, 0)[i], count)

    def state_row(s):
        @pl.when(core == 1)
        def _():
            whole(ybuf.at[s, pl.ds(0, 4 * ny - 1)], ys.at[0], yr.at[s]).wait_recv()
            for i in range(2):
                step = owned_decay(i, float(span))
                total = ybuf[s, i * 2 * ny].astype(F32)
                for k in range(1, 2 * ny):
                    total = total * step + ybuf[s, i * 2 * ny + k].astype(F32)
                zsnd[s, i] = total.astype(BF16)

            @pl.loop(0, nz - 1 - z)
            def _(k):
                zcopy(s, nz - 1 - k).start()

    def state_back(s):
        @pl.when(core == 1)
        def _():
            steps = [owned_decay(i, float(span)) for i in range(2)]
            row_steps = [owned_decay(i, float(span * 2 * ny)) for i in range(2)]

            for count in range(1, nz):
                @pl.when(z == count)
                def _():
                    whole(zbuf.at[s, pl.ds(0, count)], zs.at[0], zr.at[s]).wait_recv()

            def add(frm, totals):
                return tuple(totals[i] * row_steps[i] + zbuf[s, frm, i].astype(F32) for i in range(2))

            zero = jnp.zeros((qr, HD), F32)
            carried = lax.fori_loop(0, z, add, (zero, zero))
            for i in range(2):
                total = carried[i]
                for k in range(2 * ny):
                    msnd[s, i * 2 * ny + k] = total.astype(BF16)
                    if k < 2 * ny - 1:
                        total = total * steps[i] + ybuf[s, i * 2 * ny + k].astype(F32)
            for k, to in far_first:
                for i in range(2):
                    mcopy(s, i, k, (y + to) % ny).start()
            mcopy(s, 0, 0, y).start()
            mbuf[s, 0, pl.ds(pl.multiple_of(y * qr, qr), qr), :] = msnd[s, 2 * ny + y * 2 + half]

    def read_out(s):
        @pl.when(core == 0)
        def _():
            whole(ybuf.at[s, pl.ds(0, 2 * ny)], ms.at[0], mr.at[s]).wait_recv()

        @pl.when(core == 1)
        def _():
            whole(ybuf.at[s, pl.ds(0, 2 * ny - 1)], ms.at[0], mr.at[s]).wait_recv()

        for k in range(2):
            memory = mbuf[s, k]
            for b in range(blocks):
                here = pl.ds(b * BLOCK, BLOCK)
                if b:
                    memory = (smat[s, k, 0] + memory.astype(F32) * decay(k, float(BLOCK))).astype(BF16)
                kept = acc[s, k, here, :] + jnp.dot(qs[s, k, here, :], memory, preferred_element_type=F32)
                kept = kept - jnp.mean(kept, axis=-1, keepdims=True)
                spread = jnp.mean(kept * kept, axis=-1, keepdims=True)
                kept = kept * lax.rsqrt(spread + GROUP_EPS) * gs[s, k, here, :]
                gsend[s, here, k * HD:(k + 1) * HD] = kept.astype(BF16)
        for to in (theirs * 2 + core, theirs * 2 + 1 - core, mine * 2 + 1 - core):
            acopy(s, to).start()
        own = gsend[s, pl.ds(pl.multiple_of(dl * rows, rows), rows), :]
        gat_of(s)[:, pl.ds(pl.multiple_of(dl * 2 * HD, 2 * HD), 2 * HD)] = own

    @pl.loop(0, nseq)
    def _(s):
        pass_recv(s, 0).wait_recv()
        keys(s, 0, mine, 1)
        queries(s, 0, mine, 1)

    @pl.when(even)
    def _():
        pl.semaphore_wait(ready_a, len(plane) + 2)
        tell(ready_b, beyond)

    @pl.when(odd)
    def _():
        pl.semaphore_wait(ready_a, len(plane))

    tell(ready_b, [(sp, partner)])

    def take_pair(s):
        own_recv(s).wait_recv()
        pass_send(s, 1).start()

    w_forward(0)
    own_send(2).start()
    w_forward(1)
    w_forward(2)
    take_pair(0)
    own_send(3).start()
    w_forward(3)
    pass_recv(0, 1).wait_recv()
    keys(0, 0, theirs, 1)
    w_forward(4)
    queries(0, 0, theirs, 1)
    w_forward(5)
    for i in range(2):
        whole(crow.at[1 + i], cs.at[0], cr.at[i]).wait_recv()
    head_tables(1)
    take_pair(1)
    w_forward(6)
    pass_recv(1, 1).wait_recv()
    keys(1, 0, theirs, 1)
    w_forward(7)
    @pl.when(even)
    def _():
        pl.semaphore_wait(ready_b, 3)
        tell(ready_c, beside)

    @pl.when(odd)
    def _():
        pl.semaphore_wait(ready_b, 1)

    w_rest(0).wait_recv()
    keys(0, 1, 0, 2)
    state_out(0)
    keys(1, 1, 0, 2)
    state_out(1)
    keys(2, 1, mine, 1)
    keys(3, 1, mine, 1)
    take_pair(2)
    queries(1, 0, theirs, 1)
    pass_recv(2, 1).wait_recv()
    keys(2, 0, theirs, 1)
    keys(2, 1, theirs, 1)
    state_out(2)
    @pl.when(odd)
    def _():
        pl.semaphore_wait(ready_c, 2)

    state_row(0)
    state_row(1)
    queries(2, 0, theirs, 1)
    take_pair(3)
    w_rest(1).wait_recv()
    queries(0, 1, 0, 2)
    pass_recv(3, 1).wait_recv()
    keys(3, 1, theirs, 1)
    state_head(3, 1)
    keys(3, 0, theirs, 1)
    state_out(3, True)
    queries(1, 1, 0, 2)
    state_row(2)
    state_back(0)
    state_back(1)
    queries(2, 1, 0, 2)
    queries(3, 0, theirs, 1)
    state_row(3)
    state_back(2)
    queries(3, 1, 0, 2)
    state_back(3)
    read_out(0)
    read_out(1)
    read_out(2)
    ow_load.wait()
    pg_load.wait()
    read_out(3)
    whole(gat_early.at[:, 0:6 * HD], as_.at[0], ar.at[0]).wait_recv()
    osc[...] = jnp.dot(gat_early[...], oww[...], preferred_element_type=F32)
    scale_rows(osc, pg, mixed, 0, 2 * rows)
    whole(gat_late.at[:, 0:6 * HD], as_.at[0], ar.at[1]).wait_recv()

    whole(raw, xs.at[0], xr.at[0]).wait_send()
    whole(tok.at[:, 0:2 * rows, :], ps.at[0], pr.at[0, 0]).wait_send()
    whole(w.at[1, :, 0:quarter, :], wxs.at[0], wxr.at[0]).wait_send()
    whole(w.at[1, :, 0:3 * quarter, :], wfs.at[0], wfr.at[0]).wait_send()
    whole(crow.at[0:2], cs.at[0], cr.at[0]).wait_send()
    whole(gsend.at[:, pl.ds(0, 3 * rows), :], as_.at[0], ar.at[0]).wait_send()

    @pl.when(core == 0)
    def _():
        whole(ybuf.at[:, pl.ds(0, 2 * ny)], ys.at[0], yr.at[0]).wait_send()

    @pl.when(core == 1)
    def _():
        whole(ybuf.at[:, pl.ds(0, 2 * ny - 1)], ys.at[0], yr.at[0]).wait_send()
        whole(ybuf.at[:, pl.ds(0, 4 * ny - 1)], ms.at[0], mr.at[0]).wait_send()

        for count in range(1, nz):
            @pl.when(z == nz - 1 - count)
            def _():
                whole(zbuf.at[:, pl.ds(0, count)], zs.at[0], zr.at[0]).wait_send()


def mix_kernel(gat, oww, mixed, pg, out_ref, osc, late, sem):
    done = mixed.shape[0]
    first = pltpu.make_async_copy(mixed, out_ref.at[pl.ds(0, done), :], sem.at[0])
    first.start()
    osc[...] = jnp.dot(gat[...], oww[...], preferred_element_type=F32)
    part = late.shape[0] // 2
    copies = [first]
    for i in range(2):
        here = pl.ds(i * part, part)
        scale_rows(osc, pg, late, i * part, part)
        copies.append(pltpu.make_async_copy(late.at[here], out_ref.at[pl.ds(done + i * part, part), :], sem.at[1 + i]))
        copies[-1].start()
    for copy in copies:
        copy.wait()


def body(nz, ny, tokens, in_gain, wq, wk, wv, wg, log_decay, norm_gain, out_weight, post_gain):
    nseq, rows, width = tokens.shape
    ntp = 8
    stretch = rows * ntp
    half = stretch // 2
    tables = jnp.asarray(np.stack(rotary_tables(BLOCK)))
    qr = HD // ny
    vmem, hbm, smem = (pl.BlockSpec(memory_space=m) for m in (pltpu.VMEM, pltpu.HBM, pltpu.SMEM))
    dma = pltpu.SemaphoreType.DMA
    signal = pltpu.SemaphoreType.REGULAR
    scratch = [
        pltpu.VMEM((nseq, rows, width), BF16),
        pltpu.VMEM((nseq, half, width), BF16),
        pltpu.VMEM((2, 2, width, 2 * HD), BF16),
        pltpu.VMEM((1, width), F32),
        pltpu.VMEM((1, width), F32),
        pltpu.VMEM(tables.shape, F32),
        pltpu.VMEM((3, 8, HD), F32),
        pltpu.VMEM((2, BLOCK, HD), F32),
        pltpu.VMEM((2, BLOCK, HD), F32),
        pltpu.VMEM((2, BLOCK, HD), F32),
        pltpu.VMEM((2, BLOCK, HD), F32),
        pltpu.VMEM((2, BLOCK, HD), F32),
        pltpu.VMEM((nseq, 2, half, HD), BF16),
        pltpu.VMEM((nseq, 2, half, HD), BF16),
        pltpu.VMEM((nseq, 2, half, HD), BF16),
        pltpu.VMEM((nseq, 2, half, HD), F32),
        pltpu.VMEM((nseq, 2, half, HD), F32),
        pltpu.VMEM((nseq, 2, 2, HD, HD), F32),
        pltpu.VMEM((nseq, 2, HD, HD), BF16),
        pltpu.VMEM((nseq, 4 * ny, qr, HD), BF16),
        pltpu.VMEM((nseq, 2, qr, HD), BF16),
        pltpu.VMEM((nseq, nz, 2, qr, HD), BF16),
        pltpu.VMEM((nseq, 4 * ny, qr, HD), BF16),
        pltpu.VMEM((nseq, 2, HD, HD), BF16),
        pltpu.VMEM((nseq, half, 2 * HD), BF16),
        pltpu.VMEM((2 * rows, ntp * HD), BF16),
        pltpu.VMEM((2 * rows, width), F32),
        dma((11,)),
        dma((1,)), dma((nseq,)), dma((1,)), dma((nseq, 2)), dma((1,)), dma((8,)), dma((1,)), dma((2,)),
        dma((1,)), dma((2,)), dma((1,)), dma((nseq,)), dma((1,)), dma((nseq,)), dma((1,)), dma((nseq,)),
        dma((1,)), dma((2,)), signal, signal, signal,
    ]
    late = 2 * rows
    gain = post_gain.reshape(1, -1)
    gathered, weight, early = pl.pallas_call(
        functools.partial(kernel, nz, ny),
        out_shape=[
            pltpu.VMEM((late, ntp * HD), BF16), pltpu.VMEM(out_weight.shape, BF16), pltpu.VMEM((late, width), BF16)
        ],
        in_specs=[hbm] * 6 + [smem] + [hbm] * 4,
        out_specs=[vmem] * 3,
        scratch_shapes=scratch,
        name="retention",
        compiler_params=pltpu.CompilerParams(
            collective_id=0, has_side_effects=True, vmem_limit_bytes=VMEM_LIMIT
        ),
    )(
        tokens, in_gain.reshape(1, -1), wq, wk, wv, wg, log_decay, norm_gain.reshape(1, -1), out_weight, gain, tables,
    )
    mixed = pl.pallas_call(
        mix_kernel,
        out_shape=jax.ShapeDtypeStruct((nseq * rows, width), BF16),
        in_specs=[vmem] * 4,
        out_specs=hbm,
        scratch_shapes=[pltpu.VMEM((late, width), F32), pltpu.VMEM((late, width), BF16), dma((3,))],
        name="mix",
        compiler_params=pltpu.CompilerParams(vmem_limit_bytes=16 * 1024 * 1024),
    )(gathered, weight, early, gain)
    return mixed.reshape(tokens.shape)


def solution(mesh):
    both = ("sp", "tp")
    nz = mesh.shape["sp"] // NY
    return jax.shard_map(
        functools.partial(body, nz, NY),
        mesh=mesh,
        in_specs=(
            P(None, both, None), P(), P(None, "tp"), P(None, "tp"), P(None, "tp"), P(None, "tp"), P("tp"), P("tp"),
            P(), P(),
        ),
        out_specs=P(None, both, None),
        check_vma=False,
    )
```
